128 devices in a mesh: sp: 16 (over z, y), tp: 4 (over x), dp: 2 (over core).
Axes of the slice: x: 4, y: 4, z: 4, core: 2. Of those that a mesh axis runs over, the one named last changes fastest.
Arguments:
- latent: bfloat16 [32768, 2048], P(('dp', 'sp', 'tp')), parts along dimension 0, may hold values from -6 to 6
- cond: bfloat16 [4096], P('dp'), parts along dimension 0, may hold values from -6 to 6
- ctx_rows: bfloat16 [2048, 2048], P(('dp', 'sp')), parts along dimension 0, may hold values from -6 to 6
- ctx_cond: bfloat16 [2048], replicated, may hold values from -6 to 6
- mod_weight: bfloat16 [3, 2048, 2048], P(None, 'sp', 'tp'), may hold values from -0.125 to 0.125
- norm_gain: float32 [2048], replicated, may hold values from 0.1 to 1.9
- out_gain: float32 [2048], replicated, may hold values from 0.1 to 1.9
- w_query: bfloat16 [2048, 1024], replicated, may hold values from -16 to 16
- w_key: bfloat16 [2048, 256], replicated, may hold values from -1 to 1
- w_value: bfloat16 [2048, 256], replicated, may hold values from -0.125 to 0.125
- w_out: bfloat16 [1024, 2048], replicated, may hold values from -0.1875 to 0.1875
- sink: float32 [16], replicated, may hold values from 3 to 8
Outputs:
- updated: bfloat16 [32768, 2048], P(('dp', 'sp', 'tp')), parts along dimension 0
The draws below stay inside these ranges and needn't reach their ends.
There are 2 independent parts, one for each index of `dp`. The reference program is written for one: setup_inputs(seed, part) draws one part's arguments, and reference() takes and returns one part's arrays. A program takes and returns all parts, laid end to end along the dimension named above; an argument that names none is the same for every part. Nothing has to cross between parts.
All inputs are finite; a program needn't handle non-finite values.
Results may differ from the reference program's by a relative error of at most 0.0053.
Values may be sent and summed in bfloat16 or wider, within the bound.
No kernel may reach another device: no remote copies, remote signals or barrier semaphores. Data moves between devices by JAX's collectives and lax.ppermute only.
A program may use at most 128 MiB of HBM per device.

```python
import jax
import jax.numpy as jnp
from jax import lax

D = 2048
HEADS = 16
KV_HEADS = 4
HEAD_DIM = 64
WINDOW = 128
SPAN = 128
GRID_W = 64
CTX = 1024
SEQ = 16384


def shared_weights(key):
    base_key = jax.random.fold_in(key, 11)
    first_key, second_key = jax.random.split(base_key, 2)
    key_matrix = jax.random.normal(first_key, (D, KV_HEADS * HEAD_DIM), jnp.float32) * D ** (-0.5)
    key_matrix = jnp.clip(key_matrix, -1.0, 1.0)
    query_matrix = jax.random.normal(second_key, (D, HEADS * HEAD_DIM), jnp.float32) * D ** (-0.5)
    return (key_matrix, query_matrix)


def draw_w_key(key, part):
    return shared_weights(key)[0].astype(jnp.bfloat16)


def draw_w_query(key, part):
    key_matrix, query_matrix = shared_weights(key)
    query_matrix = jnp.clip(query_matrix, -16.0, 16.0)
    return query_matrix.astype(jnp.bfloat16)


def levels(own_key, dims, cuts, least, high):
    def one(axis_at, blocks):
        steps = jax.random.uniform(jax.random.fold_in(jax.random.fold_in(own_key, 6), axis_at), (blocks,), jnp.float32, least / len(cuts), high / len(cuts))
        return jnp.repeat(jnp.exp(steps), dims[axis_at] // blocks).reshape((-1,) + (1,) * (len(dims) - axis_at - 1))

    factor_of = one(*cuts[0])
    for cut in cuts[1:]:
        factor_of = factor_of * one(*cut)
    return factor_of


def gaussian(own_key, dims, scale, most, shards=(), kind=jnp.bfloat16):
    level = levels(own_key, dims, shards, -0.22, 0.18) if shards else 1.0
    result = jax.random.normal(own_key, dims, jnp.float32) * scale * level
    return jnp.minimum(jnp.maximum(result, -most), most).astype(kind)


def setup_inputs(seed: int = 0, part: int = 0) -> dict:
    arg_keys = jax.random.split(jax.random.key(seed), 13)
    part_splits = jax.random.split(jax.random.fold_in(arg_keys[12], part), 13)
    return {
        "latent": gaussian(part_splits[0], (SEQ, D), 1.0, 6.0, ((0, 64),)),
        "cond": gaussian(part_splits[1], (D,), 1.0, 6.0),
        "ctx_rows": gaussian(part_splits[2], (CTX, D), 1.0, 6.0, ((0, 16),)),
        "ctx_cond": gaussian(arg_keys[3], (D,), 1.0, 6.0),
        "mod_weight": gaussian(arg_keys[4], (3, D, D), D ** -0.5, 0.125, ((1, 16), (2, 4))),
        "norm_gain": jnp.clip(1.0 + 0.18 * jax.random.normal(arg_keys[5], (D,), jnp.float32), 0.1, 1.9),
        "out_gain": jnp.clip(1.0 + 0.18 * jax.random.normal(arg_keys[6], (D,), jnp.float32), 0.1, 1.9),
        "w_query": draw_w_query(jax.random.fold_in(arg_keys[12], 71), part),
        "w_key": draw_w_key(jax.random.fold_in(arg_keys[12], 71), part),
        "w_value": gaussian(arg_keys[9], (D, KV_HEADS * HEAD_DIM), D ** -0.5, 0.125),
        "w_out": gaussian(arg_keys[10], (HEADS * HEAD_DIM, D), (HEADS * HEAD_DIM) ** -0.5, 0.1875),
        "sink": jnp.clip(jax.random.uniform(arg_keys[11], (HEADS,), jnp.float32, 3.0, 8.0), 3.0, 8.0),
    }


EPSILON = 1e-06
NEG_BIG = -1e+30

def rope_angles(positions, head_width):
    freq_count = head_width // 4
    inverse = 10000.0 ** (-jnp.arange(freq_count, dtype=jnp.float32) / freq_count)
    grid_row = (positions // GRID_W).astype(jnp.float32)
    grid_col = (positions % GRID_W).astype(jnp.float32)
    angles = jnp.concatenate([grid_row[:, None] * inverse, grid_col[:, None] * inverse], axis=-1)
    return (jnp.cos(angles), jnp.sin(angles))

def rotate(values, cosine, sine_table):
    half_width = values.shape[-1] // 2
    floats = values.astype(jnp.float32)
    first = floats[..., :half_width]
    second = floats[..., half_width:]
    cos_b = cosine[:, None]
    sin_b = sine_table[:, None]
    return jnp.concatenate([first * cos_b - second * sin_b, first * sin_b + second * cos_b], axis=-1).astype(jnp.bfloat16)

def mod_norm(rows, gain, scale_vec, shift_vec):
    floats = rows.astype(jnp.float32)
    normed = floats * lax.rsqrt(lax.optimization_barrier(jnp.mean(floats * floats, axis=-1, keepdims=True)) + EPSILON) * gain
    return (normed * (1.0 + scale_vec) + shift_vec).astype(jnp.bfloat16)

def band_attention(query_rot, query_plain, key_padded, value_padded, key_ctx, value_ctx, sink_group, offset, seq_total):
    length_dev, groups, head_width = query_rot.shape
    blocks = length_dev // SPAN
    query_blocks = query_rot.reshape(blocks, SPAN, groups, head_width).astype(jnp.float32)
    plain_blocks = query_plain.reshape(blocks, SPAN, groups, head_width).astype(jnp.float32)
    key_split = key_padded.reshape(blocks + 2, SPAN, head_width)
    value_split = value_padded.reshape(blocks + 2, SPAN, head_width)
    key_band = jnp.concatenate([key_split[:-2], key_split[1:-1], key_split[2:]], axis=1).astype(jnp.float32)
    value_band = jnp.concatenate([value_split[:-2], value_split[1:-1], value_split[2:]], axis=1).astype(jnp.float32)
    factor = head_width ** (-0.5)
    local = jnp.einsum('nigd,njd->ngij', query_blocks, key_band) * factor
    block_start = offset + jnp.arange(blocks, dtype=jnp.int32) * SPAN
    query_pos = block_start[:, None, None] + jnp.arange(SPAN, dtype=jnp.int32)[None, :, None]
    key_pos = block_start[:, None, None] + jnp.arange(3 * SPAN, dtype=jnp.int32)[None, None, :] - SPAN
    allowed = (jnp.abs(query_pos - key_pos) <= WINDOW) & (key_pos >= 0) & (key_pos < seq_total)
    local = jnp.where(allowed[:, None], local, NEG_BIG)
    context = jnp.einsum('nigd,cd->ngic', plain_blocks, key_ctx.astype(jnp.float32)) * factor
    sink_col = sink_group.astype(jnp.float32)[None, :, None]
    row_max = jnp.maximum(jnp.maximum(lax.optimization_barrier(jnp.max(local, axis=-1)), lax.optimization_barrier(jnp.max(context, axis=-1))), sink_col)
    exp_local = jnp.exp(local - row_max[..., None])
    exp_ctx = jnp.exp(context - row_max[..., None])
    exp_sink = jnp.exp(sink_col - row_max)
    denom = lax.optimization_barrier(jnp.sum(exp_local, axis=-1)) + lax.optimization_barrier(jnp.sum(exp_ctx, axis=-1)) + exp_sink
    weight_local = (exp_local / denom[..., None]).astype(jnp.bfloat16)
    weight_ctx = (exp_ctx / denom[..., None]).astype(jnp.bfloat16)
    mixed = jnp.einsum('ngij,njd->nigd', weight_local.astype(jnp.float32), value_band) + jnp.einsum('ngic,cd->nigd', weight_ctx.astype(jnp.float32), value_ctx.astype(jnp.float32))
    return mixed.astype(jnp.bfloat16).reshape(length_dev, groups * head_width)

def reference(latent, cond, ctx_rows, ctx_cond, mod_weight, norm_gain, out_gain, w_query, w_key, w_value, w_out, sink):
    vectors = jax.nn.silu(jnp.stack([cond, ctx_cond]).astype(jnp.float32)).astype(jnp.bfloat16)
    shift_vec = jnp.dot(vectors, mod_weight[0], preferred_element_type=jnp.float32)
    scale_vec = jnp.dot(vectors, mod_weight[1], preferred_element_type=jnp.float32)
    gate_vec = jnp.dot(vectors[:1], mod_weight[2], preferred_element_type=jnp.float32)[0]
    hidden = mod_norm(latent, norm_gain, scale_vec[0], shift_vec[0])
    ctx_hidden = mod_norm(ctx_rows, norm_gain, scale_vec[1], shift_vec[1])
    query = jnp.dot(hidden, w_query, preferred_element_type=jnp.float32).astype(jnp.bfloat16)
    keys = jnp.dot(hidden, w_key, preferred_element_type=jnp.float32).astype(jnp.bfloat16)
    values = jnp.dot(hidden, w_value, preferred_element_type=jnp.float32).astype(jnp.bfloat16)
    ctx_keys = jnp.dot(ctx_hidden, w_key, preferred_element_type=jnp.float32).astype(jnp.bfloat16)
    ctx_values = jnp.dot(ctx_hidden, w_value, preferred_element_type=jnp.float32).astype(jnp.bfloat16)
    seq_total = latent.shape[0]
    groups = HEADS // KV_HEADS
    cosine, sine_table = rope_angles(jnp.arange(seq_total, dtype=jnp.int32), HEAD_DIM)
    query_heads = query.reshape(seq_total, HEADS, HEAD_DIM)
    query_rot = rotate(query_heads, cosine, sine_table).reshape(seq_total, KV_HEADS, groups, HEAD_DIM)
    query_grid = query_heads.reshape(seq_total, KV_HEADS, groups, HEAD_DIM)
    key_rot = rotate(keys.reshape(seq_total, KV_HEADS, HEAD_DIM), cosine, sine_table)
    value_grid = values.reshape(seq_total, KV_HEADS, HEAD_DIM)
    padding = jnp.zeros((SPAN, KV_HEADS, HEAD_DIM), jnp.bfloat16)
    key_pad = jnp.concatenate([padding, key_rot, padding], axis=0)
    value_pad = jnp.concatenate([padding, value_grid, padding], axis=0)

    def one_head(operands):
        return band_attention(operands[0], operands[1], operands[2], operands[3], operands[4], operands[5], operands[6], 0, seq_total)
    stacked = lax.map(one_head, (jnp.transpose(query_rot, (1, 0, 2, 3)), jnp.transpose(query_grid, (1, 0, 2, 3)), jnp.transpose(key_pad, (1, 0, 2)), jnp.transpose(value_pad, (1, 0, 2)), jnp.transpose(ctx_keys.reshape(CTX, KV_HEADS, HEAD_DIM), (1, 0, 2)), jnp.transpose(ctx_values.reshape(CTX, KV_HEADS, HEAD_DIM), (1, 0, 2)), sink.reshape(KV_HEADS, groups)))
    mixed = jnp.transpose(stacked, (1, 0, 2)).reshape(seq_total, HEADS * HEAD_DIM)
    projected = jnp.dot(mixed, w_out, preferred_element_type=jnp.float32)
    normed = projected * lax.rsqrt(lax.optimization_barrier(jnp.mean(projected * projected, axis=-1, keepdims=True)) + EPSILON) * out_gain
    return (latent.astype(jnp.float32) + gate_vec * normed).astype(jnp.bfloat16)
```

```python
import jax
import jax.numpy as jnp
from jax import lax
from jax.experimental import pallas as pl
from jax.experimental.pallas import tpu as pltpu
from jax.sharding import PartitionSpec as P

HEAD_DIM = 64
WINDOW = 128
GRID_W = 64
EPSILON = 1e-06
NEG_BIG = -1e30
LOG2E = 1.4426950408889634
FACTOR = HEAD_DIM**-0.5 * LOG2E
F32 = jnp.float32
BF16 = jnp.bfloat16
VM = pltpu.MemorySpace.VMEM
SM = pltpu.MemorySpace.SMEM


def vspec(n):
    return [pl.BlockSpec(memory_space=VM)] * n


def dot(a, b):
    return jnp.dot(a, b, preferred_element_type=F32)


def dot_nt(a, b):
    return lax.dot_general(a, b, (((1,), (1,)), ((), ())), preferred_element_type=F32)


def iota(shape, dim):
    return lax.broadcasted_iota(jnp.int32, shape, dim)


def pick(h, cols, transposed):
    if transposed:
        out, inp = iota((cols, 256), 0), iota((cols, 256), 1)
    else:
        out, inp = iota((256, cols), 1), iota((256, cols), 0)
    return (inp == h * HEAD_DIM + (out & (HEAD_DIM - 1))).astype(F32).astype(BF16)


def swap_matrix():
    k, c = iota((256, 256), 0), iota((256, 256), 1)
    low = (c & 63) < 32
    neg = jnp.where(low & (k == c + 32), -1.0, 0.0)
    pos = jnp.where((~low) & (k == c - 32), 1.0, 0.0)
    return (neg + pos).astype(BF16)


def partials_kernel(vec_ref, mod_ref, out_ref):
    v = vec_ref[...]
    parts = [dot(v, mod_ref[i]) for i in range(3)]
    five = (parts[0][0:1], parts[0][1:2], parts[1][0:1], parts[1][1:2], parts[2][0:1])
    zero = jnp.zeros((1, 128), F32)
    rows = []
    for j in range(4):
        cut = [x[:, j * 128 : (j + 1) * 128] for x in five]
        rows.append(jnp.concatenate(cut[:3], axis=1))
        rows.append(jnp.concatenate(cut[3:] + [zero], axis=1))
    block = jnp.concatenate(rows, axis=0).astype(BF16)
    for i in range(out_ref.shape[0]):
        out_ref[i] = block


def normed(x, mult, shift):
    x = x.astype(F32)
    rs = lax.rsqrt(jnp.mean(x * x, axis=-1, keepdims=True) + EPSILON)
    return (x * rs * mult + shift).astype(BF16)


def context_kernel(recv_ref, gain_ref, ctx_ref, wk_ref, wv_ref, kv_ref, vec_ref):
    sums = []
    for t in range(4):
        acc = recv_ref[t].astype(F32)
        for s in range(1, 16):
            acc = acc + recv_ref[s * 4 + t].astype(F32)
        sums.append(acc)

    def vector(v):
        cuts = []
        for t in range(4):
            for j in range(4):
                r, c = 2 * j + v // 3, (v % 3) * 128
                cuts.append(sums[t][r : r + 1, c : c + 128])
        return jnp.concatenate(cuts, axis=1)

    gain = gain_ref[...]
    mult0 = gain * (1.0 + vector(2))
    mult1 = gain * (1.0 + vector(3))
    vec_ref[0:1, :] = mult0
    vec_ref[1:2, :] = vector(0)
    vec_ref[2:3, :] = vector(4)
    vec_ref[3:8, :] = jnp.zeros((5, 2048), F32)
    hidden = normed(ctx_ref[...], mult1, vector(1))
    k = dot(hidden, wk_ref[...]).astype(BF16)
    v = dot(hidden, wv_ref[...]).astype(BF16)
    for i in range(kv_ref.shape[0]):
        kv_ref[i, :, 0:256] = k
        kv_ref[i, :, 256:512] = v


def local_kernel(
    flags_ref, sink_ref, vec_ref, lo_ref, own_ref, hi_ref, wq_ref, wk_ref, wv_ref, cos_ref, sin_ref,
    q_ref, o_ref, l_ref, m_ref, hid_ref, key_ref, val_ref, rot_ref,
):
    mult, shift = vec_ref[0:1, :], vec_ref[1:2, :]
    hid_ref[128:384, :] = normed(own_ref[...], mult, shift)
    hid_ref[0:128, :] = normed(lo_ref[...], mult, shift)
    hid_ref[384:512, :] = normed(hi_ref[...], mult, shift)
    swap = swap_matrix()
    query = dot(hid_ref[128:384, :], wq_ref[...]).astype(BF16)
    q_ref[...] = query
    keys = dot(hid_ref[...], wk_ref[...]).astype(BF16)
    val_ref[...] = dot(hid_ref[...], wv_ref[...]).astype(BF16)
    cos, sin = cos_ref[...], sin_ref[...]
    key_ref[...] = (keys.astype(F32) * cos + dot(keys, swap) * sin).astype(BF16)
    for h in range(4):
        part = query[:, h * 256 : (h + 1) * 256]
        rot_ref[:, h * 256 : (h + 1) * 256] = (
            part.astype(F32) * cos[128:384] + dot(part, swap) * sin[128:384]
        ).astype(BF16)
    lane = iota((128, 256), 1) // HEAD_DIM
    first = iota((128, 128), 1) < HEAD_DIM
    row, col = iota((128, 128), 0), iota((128, 128), 1)
    low_bias = jnp.where(col >= row, 0.0, NEG_BIG)
    high_bias = jnp.where(col <= row, 0.0, NEG_BIG)
    low_edge = low_bias + jnp.where(flags_ref[0] > 0, 0.0, NEG_BIG)
    high_edge = high_bias + jnp.where(flags_ref[1] > 0, 0.0, NEG_BIG)
    ones = jnp.ones((512, 128), BF16)
    for h in range(4):
        kt = dot_nt(pick(h, 256, True), key_ref[...]).astype(BF16)
        va = jnp.concatenate([dot(val_ref[...], pick(h, 128, False)).astype(BF16), ones], axis=1)
        for b in range(2):
            q = rot_ref[b * 128 : (b + 1) * 128, h * 256 : (h + 1) * 256]
            stacked = jnp.concatenate(
                [jnp.where(lane == g, q, jnp.zeros_like(q)) for g in range(4)], axis=0
            )
            s = dot(stacked, kt[:, b * 128 : b * 128 + 384]) * FACTOR
            lb = low_edge if b == 0 else low_bias
            hb = high_edge if b == 1 else high_bias
            os, ls, ms = [], [], []
            for g in range(4):
                sg = s[g * 128 : (g + 1) * 128]
                s0, s1, s2 = sg[:, 0:128] + lb, sg[:, 128:256], sg[:, 256:384] + hb
                sink = sink_ref[h * 4 + g] * LOG2E
                m = jnp.max(jnp.maximum(jnp.maximum(s0, s1), s2), axis=-1, keepdims=True)
                m = jnp.maximum(m, sink)
                p = jnp.concatenate(
                    [jnp.exp2(s0 - m), jnp.exp2(s1 - m), jnp.exp2(s2 - m)], axis=1
                ).astype(BF16)
                o = dot(p, va[b * 128 : b * 128 + 384])
                mb = jnp.broadcast_to(m, (128, 128))
                os.append(o[:, 0:128])
                ls.append(o[:, 128:256] + jnp.exp2(sink - mb))
                ms.append(mb)
            for p2 in range(2):
                at = h * 256 + p2 * 128
                for ref, xs in ((o_ref, os), (l_ref, ls), (m_ref, ms)):
                    ref[b * 128 : (b + 1) * 128, at : at + 128] = jnp.where(
                        first, xs[2 * p2], xs[2 * p2 + 1]
                    )


def final_kernel(
    q_ref, kv_ref, o_ref, l_ref, m_ref, wo_ref, lat_ref, vec_ref, gain_ref, out_ref, mix_ref
):
    lane = iota((256, 256), 1) // HEAD_DIM
    first = iota((256, 128), 1) < HEAD_DIM
    keys = kv_ref[:, 0:256]
    vals = kv_ref[:, 256:512]
    ones = jnp.ones((1024, 128), BF16)
    for h in range(4):
        kt = dot_nt(pick(h, 256, True), keys).astype(BF16)
        va = jnp.concatenate([dot(vals, pick(h, 128, False)).astype(BF16), ones], axis=1)
        q = q_ref[:, h * 256 : (h + 1) * 256]
        for p2 in range(2):
            os, ls, ms = [], [], []
            for g in (2 * p2, 2 * p2 + 1):
                s = dot(jnp.where(lane == g, q, jnp.zeros_like(q)), kt) * FACTOR
                m = jnp.max(s, axis=-1, keepdims=True)
                p = jnp.exp2(s - m).astype(BF16)
                o = dot(p, va)
                os.append(o[:, 0:128])
                ls.append(o[:, 128:256])
                ms.append(jnp.broadcast_to(m, (256, 128)))
            at = h * 256 + p2 * 128
            oc, lc, mc = (jnp.where(first, x[0], x[1]) for x in (os, ls, ms))
            ml = m_ref[:, at : at + 128]
            top = jnp.maximum(ml, mc)
            wl, wc = jnp.exp2(ml - top), jnp.exp2(mc - top)
            num = wl * o_ref[:, at : at + 128] + wc * oc
            den = wl * l_ref[:, at : at + 128] + wc * lc
            mix_ref[:, at : at + 128] = (num / den).astype(BF16)
    projected = dot(mix_ref[...], wo_ref[...])
    rs = lax.rsqrt(jnp.mean(projected * projected, axis=-1, keepdims=True) + EPSILON)
    scale = vec_ref[2:3, :] * gain_ref[...]
    out_ref[...] = (lat_ref[...].astype(F32) + projected * rs * scale).astype(BF16)


def call(kernel, name, outs, scratch=(), specs=None, flops=0, moved=0, limit=32):
    return pl.pallas_call(
        kernel,
        out_shape=[jax.ShapeDtypeStruct(s, d) for s, d in outs],
        in_specs=specs,
        out_specs=vspec(len(outs)),
        scratch_shapes=[pltpu.VMEM(s, d) for s, d in scratch],
        compiler_params=pltpu.CompilerParams(vmem_limit_bytes=limit * 1024 * 1024),
        cost_estimate=pl.CostEstimate(flops=flops, bytes_accessed=moved, transcendentals=0),
        name=name,
    )


def shards(
    latent, cond, ctx_rows, ctx_cond, mod_weight, norm_gain, out_gain,
    w_query, w_key, w_value, w_out, sink,
):
    sp_size = lax.axis_size("sp")
    tp_size = lax.axis_size("tp")
    sp_index = lax.axis_index("sp")
    place = sp_index * tp_size + lax.axis_index("tp")
    both = ("sp", "tp")
    count = sp_size * tp_size
    piece = mod_weight.shape[1]
    rows = latent.shape[0]

    up = [(i, i + 1) for i in range(count - 1)]
    low = lax.ppermute(latent[rows - WINDOW :], both, up)
    high = lax.ppermute(latent[:WINDOW], both, [(b, a) for a, b in up])

    at = sp_index * piece
    raw = jnp.stack(
        [lax.dynamic_slice_in_dim(cond, at, piece), lax.dynamic_slice_in_dim(ctx_cond, at, piece)]
    )
    vectors = jax.nn.silu(raw.astype(F32)).astype(BF16)
    (parts,) = call(
        partials_kernel, "partials", [((count, 8, 384), BF16)], specs=vspec(2), flops=10**6, limit=4
    )(vectors, mod_weight)
    recv = lax.all_to_all(parts, both, 0, 0, tiled=True)
    gain_row = norm_gain.reshape(1, -1)
    kv_send, vecs = call(
        context_kernel,
        "context",
        [((sp_size, 64, 512), BF16), ((8, 2048), F32)],
        specs=vspec(5),
        flops=2 * 10**8,
        limit=12,
    )(recv, gain_row, ctx_rows, w_key, w_value)
    kv_ctx = lax.all_to_all(kv_send, "sp", 0, 0, tiled=True).reshape(sp_size * 64, 512)

    positions = place * rows - WINDOW + jnp.arange(rows + 2 * WINDOW, dtype=jnp.int32)
    freq = 10000.0 ** (-jnp.arange(HEAD_DIM // 4, dtype=F32) / (HEAD_DIM // 4))
    grid_row = (positions // GRID_W).astype(F32)
    grid_col = (positions % GRID_W).astype(F32)
    angles = jnp.concatenate([grid_row[:, None] * freq, grid_col[:, None] * freq], axis=-1)
    cosine, sine = jnp.tile(jnp.cos(angles), (1, 8)), jnp.tile(jnp.sin(angles), (1, 8))
    flags = jnp.stack([place > 0, place < count - 1]).astype(jnp.int32)
    smem = pl.BlockSpec(memory_space=SM)
    wide = (rows, 1024)
    query, o_loc, l_loc, m_loc = call(
        local_kernel,
        "local",
        [(wide, BF16), (wide, F32), (wide, F32), (wide, F32)],
        scratch=[((512, 2048), BF16), ((512, 256), BF16), ((512, 256), BF16), (wide, BF16)],
        specs=[smem, smem] + vspec(9),
        flops=6 * 10**9,
        limit=32,
    )(flags, sink, vecs, low, latent, high, w_query, w_key, w_value, cosine, sine)
    (updated,) = call(
        final_kernel,
        "final",
        [((rows, 2048), BF16)],
        scratch=[(wide, BF16)],
        specs=vspec(9),
        flops=6 * 10**9,
        limit=32,
    )(query, kv_ctx, o_loc, l_loc, m_loc, w_out, latent, vecs, out_gain.reshape(1, -1))
    return updated


def solution(mesh):
    placed = (
        P(("dp", "sp", "tp"), None),
        P("dp"),
        P(("dp", "sp"), None),
        P(),
        P(None, "sp", "tp"),
        P(),
        P(),
        P(),
        P(),
        P(),
        P(),
        P(),
    )
    return jax.shard_map(
        shards, mesh=mesh, in_specs=placed, out_specs=P(("dp", "sp", "tp"), None), check_vma=False
    )
```

```python
import jax
import numpy as np
import jax.numpy as jnp
from jax import lax
from jax.experimental import pallas as pl
from jax.experimental.pallas import tpu as pltpu
from jax.sharding import PartitionSpec as P

HEAD_DIM = 64
WINDOW = 128
GRID_W = 64
EPSILON = 1e-06
NEG_BIG = -1e30
LOG2E = 1.4426950408889634
FACTOR = HEAD_DIM**-0.5 * LOG2E
F32 = jnp.float32
BF16 = jnp.bfloat16
VM = pltpu.MemorySpace.VMEM
HB = pltpu.MemorySpace.HBM
SM = pltpu.MemorySpace.SMEM


def spec(kinds):
    return [pl.BlockSpec(memory_space={"v": VM, "h": HB, "s": SM}[k]) for k in kinds]


def place_of():
    return lax.axis_index("sp") * lax.axis_size("tp") + lax.axis_index("tp")


def dot(a, b):
    return jnp.dot(a, b, preferred_element_type=F32)


def dot_nt(a, b):
    return lax.dot_general(a, b, (((1,), (1,)), ((), ())), preferred_element_type=F32)


def iota(shape, dim):
    return lax.broadcasted_iota(jnp.int32, shape, dim)


def pick(h, cols, transposed):
    if transposed:
        out, inp = iota((cols, 256), 0), iota((cols, 256), 1)
    else:
        out, inp = iota((256, cols), 1), iota((256, cols), 0)
    return (inp == h * HEAD_DIM + (out & (HEAD_DIM - 1))).astype(F32).astype(BF16)


def swap_matrix():
    k, c = iota((256, 256), 0), iota((256, 256), 1)
    low = (c & 63) < 32
    neg = jnp.where(low & (k == c + 32), -1.0, 0.0)
    pos = jnp.where((~low) & (k == c - 32), 1.0, 0.0)
    return (neg + pos).astype(BF16)


def normed(x, mult, shift):
    x = x.astype(F32)
    rs = lax.rsqrt(jnp.mean(x * x, axis=-1, keepdims=True) + EPSILON)
    return (x * rs * mult + shift).astype(BF16)


def entry_kernel(
    cond_ref, cctx_ref, mod_ref, lat_ref, ctx_ref, gain_ref,
    parts_ref, one_ref, two_ref, ng_ref,
    cond_v, cctx_v, mod_v, lat_v, ctx_v, gain_v, block_v, sems,
):
    sp = lax.axis_index("sp")
    odd = place_of() & 1
    copy = pltpu.make_async_copy
    ins = [
        copy(src, dst, sems.at[i])
        for i, (src, dst) in enumerate(
            (
                (cond_ref, cond_v),
                (cctx_ref, cctx_v),
                (mod_ref, mod_v),
                (lat_ref, lat_v),
                (ctx_ref, ctx_v),
                (gain_ref, gain_v),
            )
        )
    ]
    for c in ins:
        c.start()
    ins[0].wait()
    ins[1].wait()
    here = iota((16, 128), 0) == sp
    rows = []
    for ref in (cond_v, cctx_v):
        x = jnp.sum(jnp.where(here, ref[...].astype(F32), 0.0), axis=0, keepdims=True)
        rows.append(x / (1.0 + jnp.exp(-x)))
    v = jnp.concatenate(rows + [jnp.zeros((6, 128), F32)], axis=0).astype(BF16)
    ins[2].wait()
    parts = [dot(v, mod_v[i]) for i in range(3)]
    five = (parts[0][0:1], parts[0][1:2], parts[1][0:1], parts[1][1:2], parts[2][0:1])
    zero = jnp.zeros((1, 128), F32)
    rows = []
    for j in range(4):
        cut = [x[:, j * 128 : (j + 1) * 128] for x in five]
        rows.append(jnp.concatenate(cut[:3], axis=1))
        rows.append(jnp.concatenate(cut[3:] + [zero], axis=1))
    block = jnp.concatenate(rows, axis=0).astype(BF16)
    for i in range(block_v.shape[0]):
        block_v[i] = block
    outs = [copy(block_v, parts_ref, sems.at[6])]
    outs[0].start()
    ins[3].wait()
    outs.append(copy(lat_v.at[pl.ds((1 - odd) * 128, 128)], one_ref, sems.at[7]))
    outs.append(copy(lat_v.at[pl.ds(odd * 128, 128)], two_ref, sems.at[8]))
    outs[1].start()
    outs[2].start()
    ins[4].wait()
    ins[5].wait()
    x = ctx_v[...].astype(F32)
    gain = gain_v[...]
    rs = lax.rsqrt(jnp.mean(x * x, axis=-1, keepdims=True) + EPSILON)
    ng_ref[0:64, :] = x * rs * gain
    ng_ref[64:72, :] = jnp.broadcast_to(gain, (8, 2048))
    for c in outs:
        c.wait()


def context_kernel(recv_ref, ng_ref, wk_ref, wv_ref, send_ref, vec_ref, kv_v, vec_v, sems):
    sums = []
    for t in range(4):
        acc = recv_ref[t].astype(F32)
        for s in range(1, 16):
            acc = acc + recv_ref[s * 4 + t].astype(F32)
        sums.append(acc)

    def vector(v):
        cuts = []
        for t in range(4):
            for j in range(4):
                r, c = 2 * j + v // 3, (v % 3) * 128
                cuts.append(sums[t][r : r + 1, c : c + 128])
        return jnp.concatenate(cuts, axis=1)

    hidden = (ng_ref[0:64, :] * (1.0 + vector(3)) + vector(1)).astype(BF16)
    kv_v[:, 0:256] = dot(hidden, wk_ref[...]).astype(BF16)
    kv_v[:, 256:512] = dot(hidden, wv_ref[...]).astype(BF16)
    copy = pltpu.make_async_copy
    outs = [copy(kv_v, send_ref.at[i], sems.at[i]) for i in range(16)]
    for c in outs:
        c.start()
    vec_v[...] = jnp.zeros((8, 2048), F32)
    vec_v[0:1, :] = ng_ref[64:65, :] * (1.0 + vector(2))
    vec_v[1:2, :] = vector(0)
    vec_v[2:3, :] = vector(4)
    outs.append(copy(vec_v, vec_ref, sems.at[16]))
    outs[16].start()
    for c in outs:
        c.wait()


def softmax_parts(s_list, floor, va, shape):
    m = s_list[0]
    for s in s_list[1:]:
        m = jnp.maximum(m, s)
    m = jnp.max(m, axis=-1, keepdims=True)
    if floor is not None:
        m = jnp.maximum(m, floor)
    p = [jnp.exp2(s - m).astype(BF16) for s in s_list]
    p = p[0] if len(p) == 1 else jnp.concatenate(p, axis=1)
    o = dot(p, va)
    return o[:, 0:128], o[:, 128:256], jnp.broadcast_to(m, shape)


def masked_heads(q, lane):
    return [jnp.where(lane == g, q, jnp.zeros_like(q)) for g in range(4)]


def rotated(x, cos, sin, swap):
    return (x.astype(F32) * cos + dot(x, swap) * sin).astype(BF16)


def own_kernel(
    sink_ref, vec_ref, lat_ref, wq_ref, wk_ref, wv_ref, rowc_ref, rows_ref, colc_ref, cols_ref,
    q_ref, rot_ref, o_ref, l_ref, m_ref,
    vec_v, lat_v, wq_v, hid_v, q_v, sems,
):
    copy = pltpu.make_async_copy
    ins = [copy(vec_ref, vec_v, sems.at[0]), copy(lat_ref, lat_v, sems.at[1])]
    for h in range(4):
        cols = pl.ds(h * 256, 256)
        ins.append(copy(wq_ref.at[:, cols], wq_v.at[h], sems.at[2 + h]))
    for c in ins:
        c.start()
    swap = swap_matrix()
    cos = jnp.concatenate([colc_ref[...] + rowc_ref[r : r + 1, :] for r in range(2, 6)], axis=0)
    sin = jnp.concatenate([cols_ref[...] + rows_ref[r : r + 1, :] for r in range(2, 6)], axis=0)
    ins[0].wait()
    ins[1].wait()
    hid_v[...] = normed(lat_v[...], vec_v[0:1, :], vec_v[1:2, :])
    keys = rotated(dot(hid_v[...], wk_ref[...]).astype(BF16), cos, sin, swap)
    vals = dot(hid_v[...], wv_ref[...]).astype(BF16)
    lane = iota((128, 256), 1) // HEAD_DIM
    first = iota((128, 128), 1) < HEAD_DIM
    row, col = iota((128, 128), 0), iota((128, 128), 1)
    bias = (jnp.where(col <= row, 0.0, NEG_BIG), jnp.where(col >= row, 0.0, NEG_BIG))
    ones = jnp.ones((256, 128), BF16)
    outs = []
    for h in range(4):
        ins[2 + h].wait()
        at = h * 256
        query = dot(hid_v[...], wq_v[h]).astype(BF16)
        q_v[:, at : at + 256] = query
        cols = pl.ds(at, 256)
        outs.append(copy(q_v.at[:, cols], q_ref.at[:, cols], sems.at[6 + h]))
        outs[h].start()
        turned = rotated(query, cos, sin, swap)
        rot_ref[:, at : at + 256] = turned
        kt = dot_nt(pick(h, 256, True), keys).astype(BF16)
        va = jnp.concatenate([dot(vals, pick(h, 128, False)).astype(BF16), ones], axis=1)
        for b in range(2):
            rows = slice(b * 128, b * 128 + 128)
            s = dot(jnp.concatenate(masked_heads(turned[rows], lane), axis=0), kt) * FACTOR
            got = []
            for g in range(4):
                near = s[g * 128 : (g + 1) * 128, b * 128 : b * 128 + 128]
                far = s[g * 128 : (g + 1) * 128, (1 - b) * 128 : (1 - b) * 128 + 128] + bias[b]
                both = [near, far] if b == 0 else [far, near]
                sink = sink_ref[h * 4 + g] * LOG2E
                o, l, m = softmax_parts(both, sink, va, (128, 128))
                got.append((o, l + jnp.exp2(sink - m), m))
            for pair in range(2):
                to = slice(at + pair * 128, at + pair * 128 + 128)
                for ref, x, y in zip((o_ref, l_ref, m_ref), got[2 * pair], got[2 * pair + 1]):
                    ref[rows, to] = jnp.where(first, x, y)
    for c in outs:
        c.wait()


def halo_kernel(
    vec_ref, one_ref, two_ref, wk_ref, wv_ref, rowc_ref, rows_ref, colc_ref, cols_ref,
    rot_ref, o_ref, l_ref, m_ref,
    oo_ref, ll_ref, mm_ref,
    vec_v, raw_v, hid_v, o_v, l_v, m_v, sems,
):
    place = place_of()
    odd = place & 1
    copy = pltpu.make_async_copy
    ins = [
        copy(vec_ref, vec_v, sems.at[0]),
        copy(one_ref, raw_v.at[1 - odd], sems.at[1]),
        copy(two_ref, raw_v.at[odd], sems.at[2]),
    ]
    for c in ins:
        c.start()
    swap = swap_matrix()
    pick_rows = (0, 1, 6, 7)
    cos = jnp.concatenate([colc_ref[...] + rowc_ref[r : r + 1, :] for r in pick_rows], axis=0)
    sin = jnp.concatenate([cols_ref[...] + rows_ref[r : r + 1, :] for r in pick_rows], axis=0)
    for c in ins:
        c.wait()
    for b in range(2):
        hid_v[b * 128 : b * 128 + 128, :] = normed(raw_v[b], vec_v[0:1, :], vec_v[1:2, :])
    keys = rotated(dot(hid_v[...], wk_ref[...]).astype(BF16), cos, sin, swap)
    vals = dot(hid_v[...], wv_ref[...]).astype(BF16)
    lane = iota((128, 256), 1) // HEAD_DIM
    first = iota((128, 128), 1) < HEAD_DIM
    row, col = iota((128, 128), 0), iota((128, 128), 1)
    last = lax.axis_size("sp") * lax.axis_size("tp") - 1
    bias = (
        jnp.where((col >= row) & (place > 0), 0.0, NEG_BIG),
        jnp.where((col <= row) & (place < last), 0.0, NEG_BIG),
    )
    ones = jnp.ones((256, 128), BF16)
    outs = []
    for h in range(4):
        at = h * 256
        kt = dot_nt(pick(h, 256, True), keys).astype(BF16)
        va = jnp.concatenate([dot(vals, pick(h, 128, False)).astype(BF16), ones], axis=1)
        for b in range(2):
            rows = slice(b * 128, b * 128 + 128)
            turned = rot_ref[rows, at : at + 256]
            s = dot(jnp.concatenate(masked_heads(turned, lane), axis=0), kt[:, rows]) * FACTOR
            got = []
            for g in range(4):
                part = s[g * 128 : (g + 1) * 128] + bias[b]
                got.append(softmax_parts([part], None, va[rows], (128, 128)))
            for pair in range(2):
                to = slice(at + pair * 128, at + pair * 128 + 128)
                o, l, m = (
                    jnp.where(first, x, y) for x, y in zip(got[2 * pair], got[2 * pair + 1])
                )
                old = m_ref[rows, to]
                top = jnp.maximum(old, m)
                wo, wn = jnp.exp2(old - top), jnp.exp2(m - top)
                o_v[rows, to] = o_ref[rows, to] * wo + o * wn
                l_v[rows, to] = l_ref[rows, to] * wo + l * wn
                m_v[rows, to] = top
        cols = pl.ds(at, 256)
        for i, (src, dst) in enumerate(((o_v, oo_ref), (l_v, ll_ref), (m_v, mm_ref))):
            outs.append(copy(src.at[:, cols], dst.at[:, cols], sems.at[3 + 3 * h + i]))
            outs[-1].start()
    for c in outs:
        c.wait()


def final_kernel(
    q_ref, kv_ref, o_ref, l_ref, m_ref, wo_ref, lat_ref, vec_ref, gain_ref, out_ref,
    q_v, kv_v, o_v, l_v, m_v, wo_v, lat_v, vec_v, gain_v, mix_v, out_v, sems,
):
    copy = pltpu.make_async_copy
    pairs = (
        (kv_ref, kv_v), (q_ref, q_v), (o_ref, o_v), (l_ref, l_v), (m_ref, m_v),
        (wo_ref, wo_v), (lat_ref, lat_v), (vec_ref, vec_v), (gain_ref, gain_v),
    )
    ins = [copy(src, dst, sems.at[i]) for i, (src, dst) in enumerate(pairs)]
    for c in ins:
        c.start()
    lane = iota((256, 256), 1) // HEAD_DIM
    first = iota((256, 128), 1) < HEAD_DIM
    ones = jnp.ones((1024, 128), BF16)
    ins[0].wait()
    ins[1].wait()
    keys = kv_v[:, 0:256]
    vals = kv_v[:, 256:512]
    for h in range(4):
        kt = dot_nt(pick(h, 256, True), keys).astype(BF16)
        va = jnp.concatenate([dot(vals, pick(h, 128, False)).astype(BF16), ones], axis=1)
        q = q_v[:, h * 256 : (h + 1) * 256]
        for pair in range(2):
            got = []
            for g in (2 * pair, 2 * pair + 1):
                s = dot(jnp.where(lane == g, q, jnp.zeros_like(q)), kt) * FACTOR
                got.append(softmax_parts([s], None, va, (256, 128)))
            if h == 0 and pair == 0:
                for c in ins[2:5]:
                    c.wait()
            to = slice(h * 256 + pair * 128, h * 256 + pair * 128 + 128)
            oc, lc, mc = (jnp.where(first, x, y) for x, y in zip(got[0], got[1]))
            ml = m_v[:, to]
            top = jnp.maximum(ml, mc)
            wl, wc = jnp.exp2(ml - top), jnp.exp2(mc - top)
            num = wl * o_v[:, to] + wc * oc
            den = wl * l_v[:, to] + wc * lc
            mix_v[:, to] = (num / den).astype(BF16)
    for c in ins[5:]:
        c.wait()
    scale = vec_v[2:3, :] * gain_v[...]
    outs = []
    for b in range(2):
        rows = slice(b * 128, b * 128 + 128)
        projected = dot(mix_v[rows, :], wo_v[...])
        rs = lax.rsqrt(jnp.mean(projected * projected, axis=-1, keepdims=True) + EPSILON)
        out_v[rows, :] = (lat_v[rows, :].astype(F32) + projected * rs * scale).astype(BF16)
        there = pl.ds(b * 128, 128)
        outs.append(copy(out_v.at[there], out_ref.at[there], sems.at[9 + b]))
        outs[b].start()
    for c in outs:
        c.wait()


def call(kernel, name, ins, outs, scratch, copies, args, flops, limit):
    return pl.pallas_call(
        kernel,
        out_shape=[jax.ShapeDtypeStruct(s, d) for _, s, d in outs],
        in_specs=spec(ins),
        out_specs=spec([k for k, _, _ in outs]),
        scratch_shapes=[pltpu.VMEM(s, d) for s, d in scratch]
        + [pltpu.SemaphoreType.DMA((copies,))],
        compiler_params=pltpu.CompilerParams(vmem_limit_bytes=limit * 1024 * 1024),
        cost_estimate=pl.CostEstimate(flops=flops, bytes_accessed=0, transcendentals=0),
        name=name,
    )(*args)


def shards(
    latent, cond, ctx_rows, ctx_cond, mod_weight, norm_gain, out_gain,
    w_query, w_key, w_value, w_out, sink,
):
    sp_size = lax.axis_size("sp")
    count = sp_size * lax.axis_size("tp")
    both = ("sp", "tp")
    rows, width = latent.shape
    half = (WINDOW, width)
    wide = (rows, 1024)
    rest = (8, width)
    line = (1, width)
    square = (16, 128)

    parts, one, two, ng = call(
        entry_kernel,
        "entry",
        "hhhhhh",
        [
            ("h", (count, 8, 384), BF16),
            ("h", half, BF16),
            ("h", half, BF16),
            ("v", (72, width), F32),
        ],
        [
            (square, BF16),
            (square, BF16),
            (mod_weight.shape, BF16),
            (latent.shape, BF16),
            (ctx_rows.shape, BF16),
            (line, F32),
            ((count, 8, 384), BF16),
        ],
        9,
        (
            cond.reshape(square),
            ctx_cond.reshape(square),
            mod_weight,
            latent,
            ctx_rows,
            norm_gain.reshape(line),
        ),
        10**6,
        8,
    )
    recv = lax.all_to_all(parts, both, 0, 0, tiled=True)
    swap_one = [(i, i ^ 1) for i in range(count)]
    swap_two = [(i, i + 1 if i % 2 else i - 1) for i in range(1, count - 1)]
    one = lax.ppermute(one, both, swap_one)
    two = lax.ppermute(two, both, swap_two)
    send, vecs = call(
        context_kernel,
        "context",
        "vvvv",
        [("h", (sp_size, 64, 512), BF16), ("h", rest, F32)],
        [((64, 512), BF16), (rest, F32)],
        17,
        (recv, ng, w_key, w_value),
        10**6,
        6,
    )
    kv_ctx = lax.all_to_all(send, "sp", 0, 0, tiled=True).reshape(sp_size * 64, 512)

    lanes = np.arange(256) % 32
    freq = 10000.0 ** (-(lanes % 16) / 16.0)
    by_row = (lanes < 16).astype(np.float32)
    angle = np.arange(GRID_W)[:, None] * freq
    colc = jnp.asarray(np.cos(angle) * (1.0 - by_row), F32)
    cols = jnp.asarray(np.sin(angle) * (1.0 - by_row), F32)
    grid_row = place_of() * (rows // GRID_W) - WINDOW // GRID_W + jnp.arange(8, dtype=jnp.int32)
    angle = grid_row.astype(F32)[:, None] * jnp.asarray(freq, F32)[None, :]
    tables = (jnp.cos(angle) * by_row, jnp.sin(angle) * by_row, colc, cols)

    query, turned, o, l, m = call(
        own_kernel,
        "own",
        "shhhvvvvvv",
        [("h", wide, BF16), ("v", wide, BF16), ("v", wide, F32), ("v", wide, F32), ("v", wide, F32)],
        [(rest, F32), (latent.shape, BF16), ((4, width, 256), BF16), (latent.shape, BF16), (wide, BF16)],
        10,
        (sink, vecs, latent, w_query, w_key, w_value, *tables),
        10**10,
        16,
    )
    o, l, m = call(
        halo_kernel,
        "halo",
        "hhhvvvvvvvvvv",
        [("h", wide, F32)] * 3,
        [(rest, F32), ((2, WINDOW, width), BF16), (latent.shape, BF16), (wide, F32), (wide, F32), (wide, F32)],
        15,
        (vecs, one, two, w_key, w_value, *tables, turned, o, l, m),
        10**9,
        12,
    )
    (updated,) = call(
        final_kernel,
        "final",
        "hhhhhhhhh",
        [("h", latent.shape, BF16)],
        [
            (wide, BF16),
            (kv_ctx.shape, BF16),
            (wide, F32),
            (wide, F32),
            (wide, F32),
            (w_out.shape, BF16),
            (latent.shape, BF16),
            (rest, F32),
            (line, F32),
            (wide, BF16),
            (latent.shape, BF16),
        ],
        11,
        (query, kv_ctx, o, l, m, w_out, latent, vecs, out_gain.reshape(line)),
        10**10,
        28,
    )
    return updated


def solution(mesh):
    placed = (
        P(("dp", "sp", "tp"), None),
        P("dp"),
        P(("dp", "sp"), None),
        P(),
        P(None, "sp", "tp"),
        P(),
        P(),
        P(),
        P(),
        P(),
        P(),
        P(),
    )
    return jax.shard_map(
        shards, mesh=mesh, in_specs=placed, out_specs=P(("dp", "sp", "tp"), None), check_vma=False
    )
```

```python
import jax
import numpy as np
import jax.numpy as jnp
from jax import lax
from jax.experimental import pallas as pl
from jax.experimental.pallas import tpu as pltpu
from jax.sharding import PartitionSpec as P

HEAD_DIM = 64
WINDOW = 128
GRID_W = 64
EPSILON = 1e-06
NEG_BIG = -1e30
LOG2E = 1.4426950408889634
FACTOR = HEAD_DIM**-0.5 * LOG2E
F32 = jnp.float32
BF16 = jnp.bfloat16
VM = pltpu.MemorySpace.VMEM
HB = pltpu.MemorySpace.HBM
SM = pltpu.MemorySpace.SMEM


def spec(kinds):
    return [pl.BlockSpec(memory_space={"v": VM, "h": HB, "s": SM}[k]) for k in kinds]


def place_of():
    return lax.axis_index("sp") * lax.axis_size("tp") + lax.axis_index("tp")


def dot(a, b):
    return jnp.dot(a, b, preferred_element_type=F32)


def dot_nt(a, b):
    return lax.dot_general(a, b, (((1,), (1,)), ((), ())), preferred_element_type=F32)


def iota(shape, dim):
    return lax.broadcasted_iota(jnp.int32, shape, dim)


def pick(h, cols, transposed):
    if transposed:
        out, inp = iota((cols, 256), 0), iota((cols, 256), 1)
    else:
        out, inp = iota((256, cols), 1), iota((256, cols), 0)
    return (inp == h * HEAD_DIM + (out & (HEAD_DIM - 1))).astype(F32).astype(BF16)


def swap_matrix():
    k, c = iota((256, 256), 0), iota((256, 256), 1)
    low = (c & 63) < 32
    neg = jnp.where(low & (k == c + 32), -1.0, 0.0)
    pos = jnp.where((~low) & (k == c - 32), 1.0, 0.0)
    return (neg + pos).astype(BF16)


def normed(x, mult, shift):
    x = x.astype(F32)
    rs = lax.rsqrt(jnp.mean(x * x, axis=-1, keepdims=True) + EPSILON)
    return (x * rs * mult + shift).astype(BF16)


def entry_kernel(
    cond_ref, cctx_ref, mod_ref, lat_ref, ctx_ref, gain_ref,
    parts_ref, one_ref, two_ref, ng_ref,
    cond_v, cctx_v, mod_v, lat_v, ctx_v, gain_v, block_v, sems,
):
    sp = lax.axis_index("sp")
    odd = place_of() & 1
    copy = pltpu.make_async_copy
    ins = [
        copy(src, dst, sems.at[i])
        for i, (src, dst) in enumerate(
            (
                (cond_ref, cond_v),
                (cctx_ref, cctx_v),
                (mod_ref, mod_v),
                (lat_ref, lat_v),
                (ctx_ref, ctx_v),
                (gain_ref, gain_v),
            )
        )
    ]
    for c in ins:
        c.start()
    ins[0].wait()
    ins[1].wait()
    here = iota((16, 128), 0) == sp
    rows = []
    for ref in (cond_v, cctx_v):
        x = jnp.sum(jnp.where(here, ref[...].astype(F32), 0.0), axis=0, keepdims=True)
        rows.append(x / (1.0 + jnp.exp(-x)))
    v = jnp.concatenate(rows + [jnp.zeros((6, 128), F32)], axis=0).astype(BF16)
    ins[2].wait()
    parts = [dot(v, mod_v[i]) for i in range(3)]
    five = (parts[0][0:1], parts[0][1:2], parts[1][0:1], parts[1][1:2], parts[2][0:1])
    zero = jnp.zeros((1, 128), F32)
    rows = []
    for j in range(4):
        cut = [x[:, j * 128 : (j + 1) * 128] for x in five]
        rows.append(jnp.concatenate(cut[:3], axis=1))
        rows.append(jnp.concatenate(cut[3:] + [zero], axis=1))
    block = jnp.concatenate(rows, axis=0).astype(BF16)
    for i in range(block_v.shape[0]):
        block_v[i] = block
    outs = [copy(block_v, parts_ref, sems.at[6])]
    outs[0].start()
    ins[3].wait()
    outs.append(copy(lat_v.at[pl.ds((1 - odd) * 128, 128)], one_ref, sems.at[7]))
    outs.append(copy(lat_v.at[pl.ds(odd * 128, 128)], two_ref, sems.at[8]))
    outs[1].start()
    outs[2].start()
    ins[4].wait()
    ins[5].wait()
    x = ctx_v[...].astype(F32)
    gain = gain_v[...]
    rs = lax.rsqrt(jnp.mean(x * x, axis=-1, keepdims=True) + EPSILON)
    ng_ref[0:64, :] = x * rs * gain
    ng_ref[64:72, :] = jnp.broadcast_to(gain, (8, 2048))
    for c in outs:
        c.wait()


def context_kernel(recv_ref, ng_ref, wk_ref, wv_ref, send_ref, vec_ref, kv_v, vec_v, sems):
    sums = []
    for t in range(4):
        acc = recv_ref[t].astype(F32)
        for s in range(1, 16):
            acc = acc + recv_ref[s * 4 + t].astype(F32)
        sums.append(acc)

    def vector(v):
        cuts = []
        for t in range(4):
            for j in range(4):
                r, c = 2 * j + v // 3, (v % 3) * 128
                cuts.append(sums[t][r : r + 1, c : c + 128])
        return jnp.concatenate(cuts, axis=1)

    hidden = (ng_ref[0:64, :] * (1.0 + vector(3)) + vector(1)).astype(BF16)
    kv_v[:, 0:256] = dot(hidden, wk_ref[...]).astype(BF16)
    kv_v[:, 256:512] = dot(hidden, wv_ref[...]).astype(BF16)
    copy = pltpu.make_async_copy
    outs = [copy(kv_v, send_ref.at[i], sems.at[i]) for i in range(16)]
    for c in outs:
        c.start()
    vec_v[...] = jnp.zeros((8, 2048), F32)
    vec_v[0:1, :] = ng_ref[64:65, :] * (1.0 + vector(2))
    vec_v[1:2, :] = vector(0)
    vec_v[2:3, :] = vector(4)
    outs.append(copy(vec_v, vec_ref, sems.at[16]))
    outs[16].start()
    for c in outs:
        c.wait()


def softmax_parts(s_list, floor, va, shape):
    m = s_list[0]
    for s in s_list[1:]:
        m = jnp.maximum(m, s)
    m = jnp.max(m, axis=-1, keepdims=True)
    if floor is not None:
        m = jnp.maximum(m, floor)
    p = [jnp.exp2(s - m).astype(BF16) for s in s_list]
    p = p[0] if len(p) == 1 else jnp.concatenate(p, axis=1)
    o = dot(p, va)
    return o[:, 0:128], o[:, 128:256], jnp.broadcast_to(m, shape)


def masked_heads(q, lane):
    return [jnp.where(lane == g, q, jnp.zeros_like(q)) for g in range(4)]


def rotated(x, cos, sin, swap):
    return (x.astype(F32) * cos + dot(x, swap) * sin).astype(BF16)


def own_kernel(
    sink_ref, vec_ref, lat_ref, wq_ref, wk_ref, wv_ref, rowc_ref, rows_ref, colc_ref, cols_ref,
    q_ref, rot_ref, o_ref, l_ref, m_ref,
    vec_v, lat_v, wq_v, hid_v, q_v, wk_v, wv_v, sems,
):
    copy = pltpu.make_async_copy
    ins = [copy(vec_ref, vec_v, sems.at[0]), copy(lat_ref, lat_v, sems.at[1])]
    more = [copy(wk_ref, wk_v, sems.at[10]), copy(wv_ref, wv_v, sems.at[11])]
    for h in range(4):
        cols = pl.ds(h * 256, 256)
        ins.append(copy(wq_ref.at[:, cols], wq_v.at[h], sems.at[2 + h]))
    for c in ins[:2] + more + ins[2:]:
        c.start()
    swap = swap_matrix()
    cos = jnp.concatenate([colc_ref[...] + rowc_ref[r : r + 1, :] for r in range(2, 6)], axis=0)
    sin = jnp.concatenate([cols_ref[...] + rows_ref[r : r + 1, :] for r in range(2, 6)], axis=0)
    ins[0].wait()
    ins[1].wait()
    hid_v[...] = normed(lat_v[...], vec_v[0:1, :], vec_v[1:2, :])
    for c in more:
        c.wait()
    keys = rotated(dot(hid_v[...], wk_v[...]).astype(BF16), cos, sin, swap)
    vals = dot(hid_v[...], wv_v[...]).astype(BF16)
    lane = iota((128, 256), 1) // HEAD_DIM
    first = iota((128, 128), 1) < HEAD_DIM
    row, col = iota((128, 128), 0), iota((128, 128), 1)
    bias = (jnp.where(col <= row, 0.0, NEG_BIG), jnp.where(col >= row, 0.0, NEG_BIG))
    ones = jnp.ones((256, 128), BF16)
    outs = []
    for h in range(4):
        ins[2 + h].wait()
        at = h * 256
        query = dot(hid_v[...], wq_v[h]).astype(BF16)
        q_v[:, at : at + 256] = query
        cols = pl.ds(at, 256)
        outs.append(copy(q_v.at[:, cols], q_ref.at[:, cols], sems.at[6 + h]))
        outs[h].start()
        turned = rotated(query, cos, sin, swap)
        rot_ref[:, at : at + 256] = turned
        kt = dot_nt(pick(h, 256, True), keys).astype(BF16)
        va = jnp.concatenate([dot(vals, pick(h, 128, False)).astype(BF16), ones], axis=1)
        for b in range(2):
            rows = slice(b * 128, b * 128 + 128)
            s = dot(jnp.concatenate(masked_heads(turned[rows], lane), axis=0), kt) * FACTOR
            got = []
            for g in range(4):
                near = s[g * 128 : (g + 1) * 128, b * 128 : b * 128 + 128]
                far = s[g * 128 : (g + 1) * 128, (1 - b) * 128 : (1 - b) * 128 + 128] + bias[b]
                both = [near, far] if b == 0 else [far, near]
                sink = sink_ref[h * 4 + g] * LOG2E
                o, l, m = softmax_parts(both, sink, va, (128, 128))
                got.append((o, l + jnp.exp2(sink - m), m))
            for pair in range(2):
                to = slice(at + pair * 128, at + pair * 128 + 128)
                for ref, x, y in zip((o_ref, l_ref, m_ref), got[2 * pair], got[2 * pair + 1]):
                    ref[rows, to] = jnp.where(first, x, y)
    for c in outs:
        c.wait()


def halo_kernel(
    vec_ref, one_ref, two_ref, wk_ref, wv_ref, rowc_ref, rows_ref, colc_ref, cols_ref,
    rot_ref, o_ref, l_ref, m_ref,
    oo_ref, ll_ref, mm_ref,
    vec_v, raw_v, hid_v, o_v, l_v, m_v, wk_v, wv_v, sems,
):
    place = place_of()
    odd = place & 1
    copy = pltpu.make_async_copy
    ins = [
        copy(vec_ref, vec_v, sems.at[0]),
        copy(one_ref, raw_v.at[1 - odd], sems.at[1]),
        copy(two_ref, raw_v.at[odd], sems.at[2]),
        copy(wk_ref, wk_v, sems.at[15]),
        copy(wv_ref, wv_v, sems.at[16]),
    ]
    for c in ins:
        c.start()
    swap = swap_matrix()
    pick_rows = (0, 1, 6, 7)
    cos = jnp.concatenate([colc_ref[...] + rowc_ref[r : r + 1, :] for r in pick_rows], axis=0)
    sin = jnp.concatenate([cols_ref[...] + rows_ref[r : r + 1, :] for r in pick_rows], axis=0)
    for c in ins:
        c.wait()
    for b in range(2):
        hid_v[b * 128 : b * 128 + 128, :] = normed(raw_v[b], vec_v[0:1, :], vec_v[1:2, :])
    keys = rotated(dot(hid_v[...], wk_v[...]).astype(BF16), cos, sin, swap)
    vals = dot(hid_v[...], wv_v[...]).astype(BF16)
    lane = iota((128, 256), 1) // HEAD_DIM
    first = iota((128, 128), 1) < HEAD_DIM
    row, col = iota((128, 128), 0), iota((128, 128), 1)
    last = lax.axis_size("sp") * lax.axis_size("tp") - 1
    bias = (
        jnp.where((col >= row) & (place > 0), 0.0, NEG_BIG),
        jnp.where((col <= row) & (place < last), 0.0, NEG_BIG),
    )
    ones = jnp.ones((256, 128), BF16)
    outs = []
    for h in range(4):
        at = h * 256
        kt = dot_nt(pick(h, 256, True), keys).astype(BF16)
        va = jnp.concatenate([dot(vals, pick(h, 128, False)).astype(BF16), ones], axis=1)
        for b in range(2):
            rows = slice(b * 128, b * 128 + 128)
            turned = rot_ref[rows, at : at + 256]
            s = dot(jnp.concatenate(masked_heads(turned, lane), axis=0), kt[:, rows]) * FACTOR
            got = []
            for g in range(4):
                part = s[g * 128 : (g + 1) * 128] + bias[b]
                got.append(softmax_parts([part], None, va[rows], (128, 128)))
            for pair in range(2):
                to = slice(at + pair * 128, at + pair * 128 + 128)
                o, l, m = (
                    jnp.where(first, x, y) for x, y in zip(got[2 * pair], got[2 * pair + 1])
                )
                old = m_ref[rows, to]
                top = jnp.maximum(old, m)
                wo, wn = jnp.exp2(old - top), jnp.exp2(m - top)
                o_v[rows, to] = o_ref[rows, to] * wo + o * wn
                l_v[rows, to] = l_ref[rows, to] * wo + l * wn
                m_v[rows, to] = top
        cols = pl.ds(at, 256)
        for i, (src, dst) in enumerate(((o_v, oo_ref), (l_v, ll_ref), (m_v, mm_ref))):
            outs.append(copy(src.at[:, cols], dst.at[:, cols], sems.at[3 + 3 * h + i]))
            outs[-1].start()
    for c in outs:
        c.wait()


def final_kernel(
    q_ref, kv_ref, o_ref, l_ref, m_ref, wo_ref, lat_ref, vec_ref, gain_ref, out_ref,
    q_v, kv_v, o_v, l_v, m_v, wo_v, lat_v, vec_v, gain_v, mix_v, out_v, sems,
):
    copy = pltpu.make_async_copy
    pairs = (
        (kv_ref, kv_v), (q_ref, q_v), (o_ref, o_v), (l_ref, l_v), (m_ref, m_v),
        (wo_ref, wo_v), (lat_ref, lat_v), (vec_ref, vec_v), (gain_ref, gain_v),
    )
    ins = [copy(src, dst, sems.at[i]) for i, (src, dst) in enumerate(pairs)]
    for c in ins:
        c.start()
    lane = iota((256, 256), 1) // HEAD_DIM
    first = iota((256, 128), 1) < HEAD_DIM
    ones = jnp.ones((1024, 128), BF16)
    ins[0].wait()
    ins[1].wait()
    keys = kv_v[:, 0:256]
    vals = kv_v[:, 256:512]
    for h in range(4):
        kt = dot_nt(pick(h, 256, True), keys).astype(BF16)
        va = jnp.concatenate([dot(vals, pick(h, 128, False)).astype(BF16), ones], axis=1)
        q = q_v[:, h * 256 : (h + 1) * 256]
        for pair in range(2):
            got = []
            for g in (2 * pair, 2 * pair + 1):
                s = dot(jnp.where(lane == g, q, jnp.zeros_like(q)), kt) * FACTOR
                got.append(softmax_parts([s], None, va, (256, 128)))
            if h == 0 and pair == 0:
                for c in ins[2:5]:
                    c.wait()
            to = slice(h * 256 + pair * 128, h * 256 + pair * 128 + 128)
            oc, lc, mc = (jnp.where(first, x, y) for x, y in zip(got[0], got[1]))
            ml = m_v[:, to]
            top = jnp.maximum(ml, mc)
            wl, wc = jnp.exp2(ml - top), jnp.exp2(mc - top)
            num = wl * o_v[:, to] + wc * oc
            den = wl * l_v[:, to] + wc * lc
            mix_v[:, to] = (num / den).astype(BF16)
    for c in ins[5:]:
        c.wait()
    scale = vec_v[2:3, :] * gain_v[...]
    outs = []
    for b in range(2):
        rows = slice(b * 128, b * 128 + 128)
        projected = dot(mix_v[rows, :], wo_v[...])
        rs = lax.rsqrt(jnp.mean(projected * projected, axis=-1, keepdims=True) + EPSILON)
        out_v[rows, :] = (lat_v[rows, :].astype(F32) + projected * rs * scale).astype(BF16)
        there = pl.ds(b * 128, 128)
        outs.append(copy(out_v.at[there], out_ref.at[there], sems.at[9 + b]))
        outs[b].start()
    for c in outs:
        c.wait()


def call(kernel, name, ins, outs, scratch, copies, args, flops, limit):
    return pl.pallas_call(
        kernel,
        out_shape=[HB(s, d) if k == "h" else jax.ShapeDtypeStruct(s, d) for k, s, d in outs],
        in_specs=spec(ins),
        out_specs=spec([k for k, _, _ in outs]),
        scratch_shapes=[pltpu.VMEM(s, d) for s, d in scratch]
        + [pltpu.SemaphoreType.DMA((copies,))],
        compiler_params=pltpu.CompilerParams(vmem_limit_bytes=limit * 1024 * 1024),
        cost_estimate=pl.CostEstimate(flops=flops, bytes_accessed=0, transcendentals=0),
        name=name,
    )(*[pltpu.with_memory_space_constraint(x, HB) if k == "h" else x for k, x in zip(ins, args)])


def shards(
    latent, cond, ctx_rows, ctx_cond, mod_weight, norm_gain, out_gain,
    w_query, w_key, w_value, w_out, sink,
):
    sp_size = lax.axis_size("sp")
    count = sp_size * lax.axis_size("tp")
    both = ("sp", "tp")
    rows, width = latent.shape
    half = (WINDOW, width)
    wide = (rows, 1024)
    rest = (8, width)
    line = (1, width)
    square = (16, 128)

    parts, one, two, ng = call(
        entry_kernel,
        "entry",
        "hhhhhh",
        [
            ("h", (count, 8, 384), BF16),
            ("h", half, BF16),
            ("h", half, BF16),
            ("v", (72, width), F32),
        ],
        [
            (square, BF16),
            (square, BF16),
            (mod_weight.shape, BF16),
            (latent.shape, BF16),
            (ctx_rows.shape, BF16),
            (line, F32),
            ((count, 8, 384), BF16),
        ],
        9,
        (
            cond.reshape(square),
            ctx_cond.reshape(square),
            mod_weight,
            latent,
            ctx_rows,
            norm_gain.reshape(line),
        ),
        10**6,
        8,
    )
    recv = lax.all_to_all(parts, both, 0, 0, tiled=True)
    swap_one = [(i, i ^ 1) for i in range(count)]
    swap_two = [(i, i + 1 if i % 2 else i - 1) for i in range(1, count - 1)]
    one = lax.ppermute(one, both, swap_one)
    two = lax.ppermute(two, both, swap_two)
    send, vecs = call(
        context_kernel,
        "context",
        "vvvv",
        [("h", (sp_size, 64, 512), BF16), ("h", rest, F32)],
        [((64, 512), BF16), (rest, F32)],
        17,
        (recv, ng, w_key, w_value),
        10**6,
        6,
    )
    kv_ctx = lax.all_to_all(send, "sp", 0, 0, tiled=True).reshape(sp_size * 64, 512)

    lanes = np.arange(256) % 32
    freq = 10000.0 ** (-(lanes % 16) / 16.0)
    by_row = (lanes < 16).astype(np.float32)
    angle = np.arange(GRID_W)[:, None] * freq
    colc = jnp.asarray(np.cos(angle) * (1.0 - by_row), F32)
    cols = jnp.asarray(np.sin(angle) * (1.0 - by_row), F32)
    grid_row = place_of() * (rows // GRID_W) - WINDOW // GRID_W + jnp.arange(8, dtype=jnp.int32)
    angle = grid_row.astype(F32)[:, None] * jnp.asarray(freq, F32)[None, :]
    tables = (jnp.cos(angle) * by_row, jnp.sin(angle) * by_row, colc, cols)

    query, turned, o, l, m = call(
        own_kernel,
        "own",
        "shhhhhvvvv",
        [("h", wide, BF16), ("v", wide, BF16), ("v", wide, F32), ("v", wide, F32), ("v", wide, F32)],
        [(rest, F32), (latent.shape, BF16), ((4, width, 256), BF16), (latent.shape, BF16), (wide, BF16), (w_key.shape, BF16), (w_key.shape, BF16)],
        12,
        (sink, vecs, latent, w_query, w_key, w_value, *tables),
        10**10,
        16,
    )
    o, l, m = call(
        halo_kernel,
        "halo",
        "hhhhhvvvvvvvv",
        [("h", wide, F32)] * 3,
        [(rest, F32), ((2, WINDOW, width), BF16), (latent.shape, BF16), (wide, F32), (wide, F32), (wide, F32), (w_key.shape, BF16), (w_key.shape, BF16)],
        17,
        (vecs, one, two, w_key, w_value, *tables, turned, o, l, m),
        10**9,
        12,
    )
    (updated,) = call(
        final_kernel,
        "final",
        "hhhhhhhhh",
        [("h", latent.shape, BF16)],
        [
            (wide, BF16),
            (kv_ctx.shape, BF16),
            (wide, F32),
            (wide, F32),
            (wide, F32),
            (w_out.shape, BF16),
            (latent.shape, BF16),
            (rest, F32),
            (line, F32),
            (wide, BF16),
            (latent.shape, BF16),
        ],
        11,
        (query, kv_ctx, o, l, m, w_out, latent, vecs, out_gain.reshape(line)),
        10**10,
        28,
    )
    return updated


def solution(mesh):
    placed = (
        P(("dp", "sp", "tp"), None),
        P("dp"),
        P(("dp", "sp"), None),
        P(),
        P(None, "sp", "tp"),
        P(),
        P(),
        P(),
        P(),
        P(),
        P(),
        P(),
    )
    return jax.shard_map(
        shards, mesh=mesh, in_specs=placed, out_specs=P(("dp", "sp", "tp"), None), check_vma=False
    )
```

```python
import jax
import numpy as np
import jax.numpy as jnp
from jax import lax
from jax.experimental import pallas as pl
from jax.experimental.pallas import tpu as pltpu
from jax.sharding import PartitionSpec as P

HEAD_DIM = 64
WINDOW = 128
GRID_W = 64
EPSILON = 1e-06
NEG_BIG = -1e30
LOG2E = 1.4426950408889634
FACTOR = HEAD_DIM**-0.5 * LOG2E
F32 = jnp.float32
BF16 = jnp.bfloat16
VM = pltpu.MemorySpace.VMEM
HB = pltpu.MemorySpace.HBM
SM = pltpu.MemorySpace.SMEM


def place_of():
    return lax.axis_index("sp") * lax.axis_size("tp") + lax.axis_index("tp")


def dot(a, b):
    return jnp.dot(a, b, preferred_element_type=F32)


def dot_nt(a, b):
    return lax.dot_general(a, b, (((1,), (1,)), ((), ())), preferred_element_type=F32)


def iota(shape, dim):
    return lax.broadcasted_iota(jnp.int32, shape, dim)


def swap_matrix():
    k, c = iota((256, 256), 0), iota((256, 256), 1)
    low = (c & 63) < 32
    neg = jnp.where(low & (k == c + 32), -1.0, 0.0)
    pos = jnp.where((~low) & (k == c - 32), 1.0, 0.0)
    return (neg + pos).astype(BF16)


def normed(x, mult, shift):
    x = x.astype(F32)
    rs = lax.rsqrt(jnp.mean(x * x, axis=-1, keepdims=True) + EPSILON)
    return (x * rs * mult + shift).astype(BF16)


def entry_kernel(
    cond_ref, cctx_ref, mod_ref, lat_ref,
    parts_ref, one_ref, two_ref,
    cond_v, cctx_v, mod_v, lat_v, block_v, sems,
):
    sp = lax.axis_index("sp")
    odd = place_of() & 1
    copy = pltpu.make_async_copy
    pairs = ((mod_ref, mod_v), (cond_ref, cond_v), (cctx_ref, cctx_v), (lat_ref, lat_v))
    ins = [copy(src, dst, sems.at[i]) for i, (src, dst) in enumerate(pairs)]
    for c in ins:
        c.start()
    ins[1].wait()
    ins[2].wait()
    here = iota((16, 128), 0) == sp
    rows = []
    for ref in (cond_v, cctx_v):
        x = jnp.sum(jnp.where(here, ref[...].astype(F32), 0.0), axis=0, keepdims=True)
        rows.append(x / (1.0 + jnp.exp(-x)))
    v = jnp.concatenate(rows + [jnp.zeros((6, 128), F32)], axis=0).astype(BF16)
    ins[0].wait()
    parts = [dot(v, mod_v[i]) for i in range(3)]
    five = (parts[0][0:1], parts[0][1:2], parts[1][0:1], parts[1][1:2], parts[2][0:1])
    zero = jnp.zeros((1, 128), F32)
    rows = []
    for j in range(4):
        cut = [x[:, j * 128 : (j + 1) * 128] for x in five]
        rows.append(jnp.concatenate(cut[:3], axis=1))
        rows.append(jnp.concatenate(cut[3:] + [zero], axis=1))
    block = jnp.concatenate(rows, axis=0).astype(BF16)
    for i in range(block_v.shape[0]):
        block_v[i] = block
    outs = [copy(block_v, parts_ref, sems.at[4])]
    outs[0].start()
    ins[3].wait()
    outs.append(copy(lat_v.at[pl.ds((1 - odd) * 128, 128)], one_ref, sems.at[5]))
    outs.append(copy(lat_v.at[pl.ds(odd * 128, 128)], two_ref, sems.at[6]))
    outs[1].start()
    outs[2].start()
    for c in outs:
        c.wait()


def prep_kernel(
    after_ref, ctx_ref, gain_ref, wk_ref, wv_ref, ng_ref, wk_out, wv_out, ctx_v, gain_v, sems
):
    copy = pltpu.make_async_copy
    pairs = ((ctx_ref, ctx_v), (gain_ref, gain_v), (wk_ref, wk_out), (wv_ref, wv_out))
    ins = [copy(src, dst, sems.at[i]) for i, (src, dst) in enumerate(pairs)]
    for c in ins:
        c.start()
    ins[0].wait()
    ins[1].wait()
    x = ctx_v[...].astype(F32)
    gain = gain_v[...]
    rs = lax.rsqrt(jnp.mean(x * x, axis=-1, keepdims=True) + EPSILON)
    ng_ref[0:64, :] = x * rs * gain
    ng_ref[64:72, :] = jnp.broadcast_to(gain, (8, 2048))
    ins[2].wait()
    ins[3].wait()


def context_kernel(recv_ref, ng_ref, wk_ref, wv_ref, send_ref, vec_ref, kv_v, vec_v, sems):
    sums = []
    for t in range(4):
        acc = recv_ref[t].astype(F32)
        for s in range(1, 16):
            acc = acc + recv_ref[s * 4 + t].astype(F32)
        sums.append(acc)

    def vector(v):
        cuts = []
        for t in range(4):
            for j in range(4):
                r, c = 2 * j + v // 3, (v % 3) * 128
                cuts.append(sums[t][r : r + 1, c : c + 128])
        return jnp.concatenate(cuts, axis=1)

    hidden = (ng_ref[0:64, :] * (1.0 + vector(3)) + vector(1)).astype(BF16)
    kv_v[:, 0:256] = dot(hidden, wk_ref[...]).astype(BF16)
    kv_v[:, 256:512] = dot(hidden, wv_ref[...]).astype(BF16)
    copy = pltpu.make_async_copy
    outs = [copy(kv_v, send_ref.at[i], sems.at[i]) for i in range(16)]
    for c in outs:
        c.start()
    vec_v[...] = jnp.zeros((8, 2048), F32)
    vec_v[0:1, :] = ng_ref[64:65, :] * (1.0 + vector(2))
    vec_v[1:2, :] = vector(0)
    vec_v[2:3, :] = vector(4)
    outs.append(copy(vec_v, vec_ref, sems.at[16]))
    outs[16].start()
    for c in outs:
        c.wait()


def rotated(x, cos, sin, swap):
    return x.astype(F32) * cos + dot(x, swap) * sin


def paired(a, b, low):
    turned_a, turned_b = pltpu.roll(a, 64, 1), pltpu.roll(b, 64, 1)
    return jnp.where(low, a, turned_b).astype(BF16), jnp.where(low, turned_a, b).astype(BF16)


def split_pair(q, low):
    zero = jnp.zeros_like(q)
    return [jnp.where(low, q, zero), jnp.where(low, zero, q)]


def identity():
    return (iota((256, 256), 0) == iota((256, 256), 1)).astype(F32).astype(BF16)


def local_kernel(
    sink_ref, vec_ref, lat_ref, one_ref, two_ref, wq_ref, wk_ref, wv_ref,
    rowc_ref, rows_ref, colc_ref, cols_ref,
    q_ref, o_ref, l_ref, m_ref,
    vec_v, lat_v, wq_v, wk_v, wv_v, hid_v, rot_v, o_v, l_v, m_v, sems,
):
    place = place_of()
    odd = place & 1
    last = lax.axis_size("sp") * lax.axis_size("tp") - 1
    copy = pltpu.make_async_copy
    ins = [
        copy(vec_ref, vec_v, sems.at[0]),
        copy(lat_ref, lat_v.at[pl.ds(128, 256)], sems.at[1]),
        copy(one_ref, lat_v.at[pl.ds((1 - odd) * 384, 128)], sems.at[2]),
        copy(two_ref, lat_v.at[pl.ds(odd * 384, 128)], sems.at[3]),
        copy(wk_ref, wk_v, sems.at[4]),
        copy(wv_ref, wv_v, sems.at[5]),
    ]
    for h in range(4):
        cols = pl.ds(h * 256, 256)
        ins.append(copy(wq_ref.at[:, cols], wq_v.at[h], sems.at[6 + h]))
    for c in ins:
        c.start()
    swap = swap_matrix()
    cos = jnp.concatenate([colc_ref[...] + rowc_ref[r : r + 1, :] for r in range(8)], axis=0)
    sin = jnp.concatenate([cols_ref[...] + rows_ref[r : r + 1, :] for r in range(8)], axis=0)
    for c in ins[:4]:
        c.wait()
    mult, shift = vec_v[0:1, :], vec_v[1:2, :]
    for r in range(4):
        rows = slice(r * 128, r * 128 + 128)
        hid_v[rows, :] = normed(lat_v[rows, :], mult, shift)
    ins[4].wait()
    ins[5].wait()
    keys = rotated(dot(hid_v[...], wk_v[...]).astype(BF16), cos, sin, swap).astype(BF16)
    kt = dot_nt(identity(), keys).astype(BF16)
    vals = dot(hid_v[...], wv_v[...]).astype(BF16)
    ones = jnp.ones((512, 128), BF16)
    low_own = iota((256, 128), 1) < HEAD_DIM
    low = iota((128, 128), 1) < HEAD_DIM
    row, col = iota((128, 128), 0), iota((128, 128), 1)
    from_low = jnp.where(col >= row, 0.0, NEG_BIG)
    from_high = jnp.where(col <= row, 0.0, NEG_BIG)
    bias = (
        (from_low + jnp.where(place > 0, 0.0, NEG_BIG), from_high),
        (from_low, from_high + jnp.where(place < last, 0.0, NEG_BIG)),
    )
    outs = []
    for a in range(2):
        plain, turned = [], []
        for h in (2 * a, 2 * a + 1):
            ins[6 + h].wait()
            q = dot(hid_v[128:384, :], wq_v[h]).astype(BF16)
            plain.append(q.astype(F32))
            turned.append(rotated(q, cos[128:384], sin[128:384], swap))
        for p in range(2):
            piece = slice(p * 128, p * 128 + 128)
            at = a * 512 + p * 256
            for ref, x in ((q_ref, plain), (rot_v, turned)):
                one, two = paired(x[0][:, piece], x[1][:, piece], low_own)
                ref[:, at : at + 128] = one
                ref[:, at + 128 : at + 256] = two
        va = jnp.concatenate([vals[:, a * 128 : a * 128 + 128], ones], axis=1)
        for b in range(2):
            rows = slice(b * 128, b * 128 + 128)
            seen = slice(b * 128, b * 128 + 384)
            stacked = []
            for g in range(4):
                stacked += split_pair(rot_v[rows, a * 512 + g * 128 : a * 512 + g * 128 + 128], low)
            s = dot(jnp.concatenate(stacked, axis=0), kt[a * 128 : a * 128 + 128, seen])
            ps, ms = [], []
            for i in range(8):
                si = s[i * 128 : i * 128 + 128]
                s0, s1, s2 = si[:, 0:128] + bias[b][0], si[:, 128:256], si[:, 256:384] + bias[b][1]
                sink = sink_ref[(2 * a + i % 2) * 4 + i // 2] * LOG2E
                m = jnp.max(jnp.maximum(jnp.maximum(s0, s1), s2), axis=-1, keepdims=True)
                m = jnp.maximum(m * FACTOR, sink)
                p = [jnp.exp2(x * FACTOR - m).astype(BF16) for x in (s0, s1, s2)]
                ps.append(jnp.concatenate(p, axis=1))
                ms.append((jnp.broadcast_to(m, (128, 128)), sink))
            o = dot(jnp.concatenate(ps, axis=0), va[seen])
            for g in range(4):
                to = slice(a * 512 + g * 128, a * 512 + g * 128 + 128)
                x, y = o[g * 256 : g * 256 + 128], o[g * 256 + 128 : g * 256 + 256]
                (mx, sx), (my, sy) = ms[2 * g], ms[2 * g + 1]
                m = jnp.where(low, mx, my)
                o_v[rows, to] = jnp.where(low, x[:, 0:128], y[:, 0:128])
                l_v[rows, to] = jnp.where(low, x[:, 128:256], y[:, 128:256]) + jnp.exp2(
                    jnp.where(low, sx, sy) - m
                )
                m_v[rows, to] = m
        cols = pl.ds(a * 512, 512)
        for i, (src, dst) in enumerate(((o_v, o_ref), (l_v, l_ref), (m_v, m_ref))):
            outs.append(copy(src.at[:, cols], dst.at[:, cols], sems.at[10 + 3 * a + i]))
            outs[-1].start()
    for c in outs:
        c.wait()


def final_kernel(
    q_ref, kv_ref, o_ref, l_ref, m_ref, wo_ref, lat_ref, vec_ref, gain_ref, out_ref,
    o_v, l_v, m_v, wo_v, lat_v, vec_v, gain_v, mix_v, out_v, sems,
):
    copy = pltpu.make_async_copy
    pairs = [
        (o_ref, o_v), (l_ref, l_v), (m_ref, m_v), (lat_ref, lat_v), (vec_ref, vec_v), (gain_ref, gain_v),
    ]
    for a in range(2):
        for g in range(4):
            for i in range(2):
                head = (2 * a + i) * 4 + g
                to = ((a * 4 + g) * 2 + i) * HEAD_DIM
                pairs.append((wo_ref.at[pl.ds(head * 64, 64)], wo_v.at[pl.ds(to, 64)]))
    ins = [copy(src, dst, sems.at[i]) for i, (src, dst) in enumerate(pairs)]
    for c in ins:
        c.start()
    low = iota((256, 128), 1) < HEAD_DIM
    ones = jnp.ones((1024, 128), BF16)
    kt = dot_nt(identity(), kv_ref[:, 0:256]).astype(BF16)
    for a in range(2):
        va = jnp.concatenate([kv_ref[:, 256 + a * 128 : 384 + a * 128], ones], axis=1)
        for g in range(4):
            to = slice(a * 512 + g * 128, a * 512 + g * 128 + 128)
            stacked = jnp.concatenate(split_pair(q_ref[:, to], low), axis=0)
            s = dot(stacked, kt[a * 128 : a * 128 + 128, :])
            m = jnp.max(s, axis=-1, keepdims=True) * FACTOR
            o = dot(jnp.exp2(s * FACTOR - m).astype(BF16), va)
            m = jnp.broadcast_to(m, (512, 128))
            if a == 0 and g == 0:
                for c in ins[:3]:
                    c.wait()
            mc = jnp.where(low, m[0:256], m[256:512])
            oc = jnp.where(low, o[0:256, 0:128], o[256:512, 0:128])
            lc = jnp.where(low, o[0:256, 128:256], o[256:512, 128:256])
            ml = m_v[:, to]
            top = jnp.maximum(ml, mc)
            wl, wc = jnp.exp2(ml - top), jnp.exp2(mc - top)
            num = wl * o_v[:, to] + wc * oc
            den = wl * l_v[:, to] + wc * lc
            mix_v[:, to] = (num / den).astype(BF16)
    for c in ins[3:]:
        c.wait()
    scale = vec_v[2:3, :] * gain_v[...]
    outs = []
    for b in range(2):
        rows = slice(b * 128, b * 128 + 128)
        projected = dot(mix_v[rows, :], wo_v[...])
        rs = lax.rsqrt(jnp.mean(projected * projected, axis=-1, keepdims=True) + EPSILON)
        out_v[rows, :] = (lat_v[rows, :].astype(F32) + projected * rs * scale).astype(BF16)
        there = pl.ds(b * 128, 128)
        outs.append(copy(out_v.at[there], out_ref.at[there], sems.at[len(ins) + b]))
        outs[b].start()
    for c in outs:
        c.wait()


KINDS = {"v": VM, "V": VM, "h": HB, "s": SM}
FIXED = {"V": VM, "h": HB}


def spec(kinds):
    return [pl.BlockSpec(memory_space=KINDS[k]) for k in kinds]


def call(kernel, name, ins, outs, scratch, copies, args, flops, limit):
    return pl.pallas_call(
        kernel,
        out_shape=[FIXED.get(k, jax.ShapeDtypeStruct)(s, d) for k, s, d in outs],
        in_specs=spec(ins),
        out_specs=spec([k for k, _, _ in outs]),
        scratch_shapes=[pltpu.VMEM(s, d) for s, d in scratch]
        + [pltpu.SemaphoreType.DMA((copies,))],
        compiler_params=pltpu.CompilerParams(vmem_limit_bytes=limit * 1024 * 1024),
        cost_estimate=pl.CostEstimate(flops=flops, bytes_accessed=0, transcendentals=0),
        name=name,
    )(
        *[
            pltpu.with_memory_space_constraint(x, FIXED[k]) if k in FIXED else x
            for k, x in zip(ins, args)
        ]
    )


def shards(
    latent, cond, ctx_rows, ctx_cond, mod_weight, norm_gain, out_gain,
    w_query, w_key, w_value, w_out, sink,
):
    sp_size = lax.axis_size("sp")
    count = sp_size * lax.axis_size("tp")
    both = ("sp", "tp")
    rows, width = latent.shape
    half = (WINDOW, width)
    wide = (rows, 1024)
    rest = (8, width)
    line = (1, width)
    square = (16, 128)
    small = w_key.shape

    parts, one, two = call(
        entry_kernel,
        "entry",
        "hhhh",
        [("h", (count, 8, 384), BF16), ("h", half, BF16), ("h", half, BF16)],
        [
            (square, BF16),
            (square, BF16),
            (mod_weight.shape, BF16),
            (latent.shape, BF16),
            ((count, 8, 384), BF16),
        ],
        7,
        (cond.reshape(square), ctx_cond.reshape(square), mod_weight, latent),
        10**6,
        8,
    )
    ng, wk_near, wv_near = call(
        prep_kernel,
        "prep",
        "hhhhh",
        [("V", (72, width), F32), ("V", small, BF16), ("V", small, BF16)],
        [(ctx_rows.shape, BF16), (line, F32)],
        4,
        (one, ctx_rows, norm_gain.reshape(line), w_key, w_value),
        2 * 10**9,
        4,
    )
    recv = lax.all_to_all(parts, both, 0, 0, tiled=True)
    swap_one = [(i, i ^ 1) for i in range(count)]
    swap_two = [(i, i + 1 if i % 2 else i - 1) for i in range(1, count - 1)]
    one = lax.ppermute(one, both, swap_one)
    two = lax.ppermute(two, both, swap_two)
    send, vecs = call(
        context_kernel,
        "context",
        "vVVV",
        [("h", (sp_size, 64, 512), BF16), ("h", rest, F32)],
        [((64, 512), BF16), (rest, F32)],
        17,
        (recv, ng, wk_near, wv_near),
        10**6,
        6,
    )
    kv_ctx = lax.all_to_all(send, "sp", 0, 0, tiled=True).reshape(sp_size * 64, 512)

    lanes = np.arange(256) % 32
    freq = 10000.0 ** (-(lanes % 16) / 16.0)
    by_row = (lanes < 16).astype(np.float32)
    angle = np.arange(GRID_W)[:, None] * freq
    colc = jnp.asarray(np.cos(angle) * (1.0 - by_row), F32)
    cols = jnp.asarray(np.sin(angle) * (1.0 - by_row), F32)
    grid_row = place_of() * (rows // GRID_W) - WINDOW // GRID_W + jnp.arange(8, dtype=jnp.int32)
    angle = grid_row.astype(F32)[:, None] * jnp.asarray(freq, F32)[None, :]
    tables = (jnp.cos(angle) * by_row, jnp.sin(angle) * by_row, colc, cols)

    query, o, l, m = call(
        local_kernel,
        "local",
        "shhhhhhhvvvv",
        [("V", wide, BF16), ("h", wide, F32), ("h", wide, F32), ("h", wide, F32)],
        [
            (rest, F32),
            ((2 * rows, width), BF16),
            ((4, width, 256), BF16),
            (small, BF16),
            (small, BF16),
            ((2 * rows, width), BF16),
            (wide, BF16),
            (wide, F32),
            (wide, F32),
            (wide, F32),
        ],
        16,
        (sink, vecs, latent, one, two, w_query, w_key, w_value, *tables),
        10**10,
        26,
    )
    (updated,) = call(
        final_kernel,
        "final",
        "VVhhhhhhh",
        [("h", latent.shape, BF16)],
        [
            (wide, F32),
            (wide, F32),
            (wide, F32),
            (w_out.shape, BF16),
            (latent.shape, BF16),
            (rest, F32),
            (line, F32),
            (wide, BF16),
            (latent.shape, BF16),
        ],
        24,
        (query, kv_ctx, o, l, m, w_out, latent, vecs, out_gain.reshape(line)),
        10**10,
        28,
    )
    return updated


def solution(mesh):
    placed = (
        P(("dp", "sp", "tp"), None),
        P("dp"),
        P(("dp", "sp"), None),
        P(),
        P(None, "sp", "tp"),
        P(),
        P(),
        P(),
        P(),
        P(),
        P(),
        P(),
    )
    return jax.shard_map(
        shards, mesh=mesh, in_specs=placed, out_specs=P(("dp", "sp", "tp"), None), check_vma=False
    )
```

```python
import jax
import numpy as np
import jax.numpy as jnp
from jax import lax
from jax.experimental import pallas as pl
from jax.experimental.pallas import tpu as pltpu
from jax.sharding import PartitionSpec as P

HEAD_DIM = 64
WINDOW = 128
GRID_W = 64
EPSILON = 1e-06
NEG_BIG = -1e30
LOG2E = 1.4426950408889634
FACTOR = HEAD_DIM**-0.5 * LOG2E
F32 = jnp.float32
BF16 = jnp.bfloat16
VM = pltpu.MemorySpace.VMEM
HB = pltpu.MemorySpace.HBM
SM = pltpu.MemorySpace.SMEM


def place_of():
    return lax.axis_index("sp") * lax.axis_size("tp") + lax.axis_index("tp")


def dot(a, b):
    return jnp.dot(a, b, preferred_element_type=F32)


def dot_nt(a, b):
    return lax.dot_general(a, b, (((1,), (1,)), ((), ())), preferred_element_type=F32)


def iota(shape, dim):
    return lax.broadcasted_iota(jnp.int32, shape, dim)


def swap_matrix():
    k, c = iota((256, 256), 0), iota((256, 256), 1)
    low = (c & 63) < 32
    neg = jnp.where(low & (k == c + 32), -1.0, 0.0)
    pos = jnp.where((~low) & (k == c - 32), 1.0, 0.0)
    return (neg + pos).astype(BF16)


def normed(x, mult, shift):
    x = x.astype(F32)
    rs = lax.rsqrt(jnp.mean(x * x, axis=-1, keepdims=True) + EPSILON)
    return (x * rs * mult + shift).astype(BF16)


def entry_kernel(
    cond_ref, cctx_ref, mod_ref, lat_ref,
    parts_ref, one_ref, two_ref,
    cond_v, cctx_v, mod_v, lat_v, block_v, sems,
):
    sp = lax.axis_index("sp")
    odd = place_of() & 1
    copy = pltpu.make_async_copy
    pairs = ((mod_ref, mod_v), (cond_ref, cond_v), (cctx_ref, cctx_v), (lat_ref, lat_v))
    ins = [copy(src, dst, sems.at[i]) for i, (src, dst) in enumerate(pairs)]
    for c in ins:
        c.start()
    ins[1].wait()
    ins[2].wait()
    here = iota((16, 128), 0) == sp
    rows = []
    for ref in (cond_v, cctx_v):
        x = jnp.sum(jnp.where(here, ref[...].astype(F32), 0.0), axis=0, keepdims=True)
        rows.append(x / (1.0 + jnp.exp(-x)))
    v = jnp.concatenate(rows + [jnp.zeros((6, 128), F32)], axis=0).astype(BF16)
    ins[0].wait()
    parts = [dot(v, mod_v[i]) for i in range(3)]
    five = (parts[0][0:1], parts[0][1:2], parts[1][0:1], parts[1][1:2], parts[2][0:1])
    zero = jnp.zeros((1, 128), F32)
    rows = []
    for j in range(4):
        cut = [x[:, j * 128 : (j + 1) * 128] for x in five]
        rows.append(jnp.concatenate(cut[:3], axis=1))
        rows.append(jnp.concatenate(cut[3:] + [zero], axis=1))
    block = jnp.concatenate(rows, axis=0).astype(BF16)
    for i in range(block_v.shape[0]):
        block_v[i] = block
    outs = [copy(block_v, parts_ref, sems.at[4])]
    outs[0].start()
    ins[3].wait()
    outs.append(copy(lat_v.at[pl.ds((1 - odd) * 128, 128)], one_ref, sems.at[5]))
    outs.append(copy(lat_v.at[pl.ds(odd * 128, 128)], two_ref, sems.at[6]))
    outs[1].start()
    outs[2].start()
    for c in outs:
        c.wait()


def prep_kernel(
    after_ref, ctx_ref, gain_ref, wk_ref, wv_ref, ng_ref, wk_out, wv_out, ctx_v, gain_v, sems
):
    copy = pltpu.make_async_copy
    pairs = ((ctx_ref, ctx_v), (gain_ref, gain_v), (wk_ref, wk_out), (wv_ref, wv_out))
    ins = [copy(src, dst, sems.at[i]) for i, (src, dst) in enumerate(pairs)]
    for c in ins:
        c.start()
    ins[0].wait()
    ins[1].wait()
    x = ctx_v[...].astype(F32)
    gain = gain_v[...]
    rs = lax.rsqrt(jnp.mean(x * x, axis=-1, keepdims=True) + EPSILON)
    ng_ref[0:64, :] = x * rs * gain
    ng_ref[64:72, :] = jnp.broadcast_to(gain, (8, 2048))
    ins[2].wait()
    ins[3].wait()


def context_kernel(recv_ref, ng_ref, wk_ref, wv_ref, send_ref, vec_ref, kv_v, vec_v, sems):
    sums = []
    for t in range(4):
        acc = recv_ref[t].astype(F32)
        for s in range(1, 16):
            acc = acc + recv_ref[s * 4 + t].astype(F32)
        sums.append(acc)

    def vector(v):
        cuts = []
        for t in range(4):
            for j in range(4):
                r, c = 2 * j + v // 3, (v % 3) * 128
                cuts.append(sums[t][r : r + 1, c : c + 128])
        return jnp.concatenate(cuts, axis=1)

    hidden = (ng_ref[0:64, :] * (1.0 + vector(3)) + vector(1)).astype(BF16)
    kv_v[:, 0:256] = dot(hidden, wk_ref[...]).astype(BF16)
    kv_v[:, 256:512] = dot(hidden, wv_ref[...]).astype(BF16)
    copy = pltpu.make_async_copy
    outs = [copy(kv_v, send_ref.at[i], sems.at[i]) for i in range(16)]
    for c in outs:
        c.start()
    vec_v[...] = jnp.zeros((8, 2048), F32)
    vec_v[0:1, :] = ng_ref[64:65, :] * (1.0 + vector(2))
    vec_v[1:2, :] = vector(0)
    vec_v[2:3, :] = vector(4)
    outs.append(copy(vec_v, vec_ref, sems.at[16]))
    outs[16].start()
    for c in outs:
        c.wait()


def rotated(x, cos, sin, swap):
    return x.astype(F32) * cos + dot(x, swap) * sin


def paired(a, b, low):
    turned_a, turned_b = pltpu.roll(a, 64, 1), pltpu.roll(b, 64, 1)
    return jnp.where(low, a, turned_b).astype(BF16), jnp.where(low, turned_a, b).astype(BF16)


def split_pair(q, low):
    zero = jnp.zeros_like(q)
    return [jnp.where(low, q, zero), jnp.where(low, zero, q)]


def identity():
    return (iota((256, 256), 0) == iota((256, 256), 1)).astype(F32).astype(BF16)


def local_kernel(
    sink_ref, vec_ref, lat_ref, one_ref, two_ref, wq_ref, wk_ref, wv_ref,
    rowc_ref, rows_ref, colc_ref, cols_ref,
    q_ref, o_ref, l_ref, m_ref,
    vec_v, lat_v, wq_v, wkv_v, hid_v, o_v, l_v, m_v, sems,
):
    place = place_of()
    odd = place & 1
    last = lax.axis_size("sp") * lax.axis_size("tp") - 1
    copy = pltpu.make_async_copy
    own = [
        copy(vec_ref, vec_v, sems.at[0]),
        copy(lat_ref, lat_v.at[pl.ds(128, 256)], sems.at[1]),
    ]
    halo = [
        copy(one_ref, lat_v.at[pl.ds((1 - odd) * 384, 128)], sems.at[2]),
        copy(two_ref, lat_v.at[pl.ds(odd * 384, 128)], sems.at[3]),
    ]
    weights = [
        copy(wk_ref, wkv_v.at[:, pl.ds(0, 256)], sems.at[4]),
        copy(wv_ref, wkv_v.at[:, pl.ds(256, 256)], sems.at[5]),
        copy(wq_ref.at[:, pl.ds(0, 512)], wq_v.at[0], sems.at[6]),
        copy(wq_ref.at[:, pl.ds(512, 512)], wq_v.at[1], sems.at[7]),
    ]
    for c in own + halo:
        c.start()
    swap = swap_matrix()
    cos = jnp.concatenate([colc_ref[...] + rowc_ref[r : r + 1, :] for r in range(8)], axis=0)
    sin = jnp.concatenate([cols_ref[...] + rows_ref[r : r + 1, :] for r in range(8)], axis=0)
    for c in own:
        c.wait()
    for c in weights:
        c.start()
    mult, shift = vec_v[0:1, :], vec_v[1:2, :]
    for r in (1, 2):
        rows = slice(r * 128, r * 128 + 128)
        hid_v[rows, :] = normed(lat_v[rows, :], mult, shift)
    for c in halo:
        c.wait()
    for r in (0, 3):
        rows = slice(r * 128, r * 128 + 128)
        hid_v[rows, :] = normed(lat_v[rows, :], mult, shift)
    for c in weights:
        c.wait()
    kv = dot(hid_v[...], wkv_v[...]).astype(BF16)
    keys = rotated(kv[:, 0:256], cos, sin, swap).astype(BF16)
    kt = dot_nt(identity(), keys).astype(BF16)
    ones = jnp.ones((512, 128), BF16)
    low_own = iota((256, 128), 1) < HEAD_DIM
    low = iota((128, 128), 1) < HEAD_DIM
    row, col = iota((128, 128), 0), iota((128, 128), 1)
    from_low = jnp.where(col >= row, 0.0, NEG_BIG)
    from_high = jnp.where(col <= row, 0.0, NEG_BIG)
    bias = (
        (from_low + jnp.where(place > 0, 0.0, NEG_BIG), from_high),
        (from_low, from_high + jnp.where(place < last, 0.0, NEG_BIG)),
    )
    slabs = []
    for a in range(2):
        q = dot(hid_v[128:384, :], wq_v[a]).astype(BF16)
        plain, turned = [], []
        for h in range(2):
            part = q[:, h * 256 : h * 256 + 256]
            plain.append(part.astype(F32))
            turned.append(rotated(part, cos[128:384], sin[128:384], swap))
        for p in range(2):
            piece = slice(p * 128, p * 128 + 128)
            at = a * 512 + p * 256
            one, two = paired(plain[0][:, piece], plain[1][:, piece], low_own)
            q_ref[:, at : at + 128] = one
            q_ref[:, at + 128 : at + 256] = two
            slabs += paired(turned[0][:, piece], turned[1][:, piece], low_own)
    for a in range(2):
        va = jnp.concatenate([kv[:, 256 + a * 128 : 384 + a * 128], ones], axis=1)
        for b in range(2):
            rows = slice(b * 128, b * 128 + 128)
            seen = slice(b * 128, b * 128 + 384)
            stacked = []
            for g in range(4):
                stacked += split_pair(slabs[a * 4 + g][rows], low)
            s = dot(jnp.concatenate(stacked, axis=0), kt[a * 128 : a * 128 + 128, seen])
            ps, ms = [], []
            for i in range(8):
                si = s[i * 128 : i * 128 + 128]
                s0, s1, s2 = si[:, 0:128] + bias[b][0], si[:, 128:256], si[:, 256:384] + bias[b][1]
                sink = sink_ref[(2 * a + i % 2) * 4 + i // 2] * LOG2E
                m = jnp.max(jnp.maximum(jnp.maximum(s0, s1), s2), axis=-1, keepdims=True)
                m = jnp.maximum(m * FACTOR, sink)
                p = [jnp.exp2(x * FACTOR - m).astype(BF16) for x in (s0, s1, s2)]
                ps.append(jnp.concatenate(p, axis=1))
                ms.append((jnp.broadcast_to(m, (128, 128)), sink))
            o = dot(jnp.concatenate(ps, axis=0), va[seen])
            for g in range(4):
                to = slice(a * 512 + g * 128, a * 512 + g * 128 + 128)
                x, y = o[g * 256 : g * 256 + 128], o[g * 256 + 128 : g * 256 + 256]
                (mx, sx), (my, sy) = ms[2 * g], ms[2 * g + 1]
                m = jnp.where(low, mx, my)
                o_v[rows, to] = jnp.where(low, x[:, 0:128], y[:, 0:128])
                l_v[rows, to] = jnp.where(low, x[:, 128:256], y[:, 128:256]) + jnp.exp2(
                    jnp.where(low, sx, sy) - m
                )
                m_v[rows, to] = m
    outs = [
        copy(src, dst, sems.at[8 + i])
        for i, (src, dst) in enumerate(((o_v, o_ref), (l_v, l_ref), (m_v, m_ref)))
    ]
    for c in outs:
        c.start()
    for c in outs:
        c.wait()


def final_kernel(
    q_ref, kv_ref, o_ref, l_ref, m_ref, wo_ref, lat_ref, vec_ref, gain_ref, out_ref,
    o_v, l_v, m_v, wo_v, lat_v, vec_v, gain_v, oc_v, lc_v, mc_v, out_v, sems,
):
    copy = pltpu.make_async_copy
    pairs = [
        (o_ref, o_v), (l_ref, l_v), (m_ref, m_v), (lat_ref, lat_v), (vec_ref, vec_v), (gain_ref, gain_v),
    ]
    for a in range(2):
        for g in range(4):
            for i in range(2):
                head = (2 * a + i) * 4 + g
                to = ((a * 4 + g) * 2 + i) * HEAD_DIM
                pairs.append((wo_ref.at[pl.ds(head * 64, 64)], wo_v.at[pl.ds(to, 64)]))
    ins = [copy(src, dst, sems.at[i]) for i, (src, dst) in enumerate(pairs)]
    for c in ins:
        c.start()
    low = iota((256, 128), 1) < HEAD_DIM
    ones = jnp.ones((1024, 128), BF16)
    kt = dot_nt(identity(), kv_ref[:, 0:256]).astype(BF16)
    slabs = [slice(i * 128, i * 128 + 128) for i in range(8)]

    def scores(i):
        stacked = jnp.concatenate(split_pair(q_ref[:, slabs[i]], low), axis=0)
        return dot(stacked, kt[(i // 4) * 128 : (i // 4) * 128 + 128, :])

    s = scores(0)
    for i in range(8):
        coming = scores(i + 1) if i < 7 else None
        a = i // 4
        va = jnp.concatenate([kv_ref[:, 256 + a * 128 : 384 + a * 128], ones], axis=1)
        m = jnp.max(s, axis=-1, keepdims=True) * FACTOR
        o = dot(jnp.exp2(s * FACTOR - m).astype(BF16), va)
        m = jnp.broadcast_to(m, (512, 128))
        mc_v[:, slabs[i]] = jnp.where(low, m[0:256], m[256:512])
        oc_v[:, slabs[i]] = jnp.where(low, o[0:256, 0:128], o[256:512, 0:128])
        lc_v[:, slabs[i]] = jnp.where(low, o[0:256, 128:256], o[256:512, 128:256])
        s = coming
    for c in ins:
        c.wait()
    scale = vec_v[2:3, :] * gain_v[...]
    outs = []
    for b in range(2):
        rows = slice(b * 128, b * 128 + 128)
        mixed = []
        for to in slabs:
            ml, mc = m_v[rows, to], mc_v[rows, to]
            top = jnp.maximum(ml, mc)
            wl, wc = jnp.exp2(ml - top), jnp.exp2(mc - top)
            num = wl * o_v[rows, to] + wc * oc_v[rows, to]
            den = wl * l_v[rows, to] + wc * lc_v[rows, to]
            mixed.append((num / den).astype(BF16))
        projected = dot(jnp.concatenate(mixed, axis=1), wo_v[...])
        rs = lax.rsqrt(jnp.mean(projected * projected, axis=-1, keepdims=True) + EPSILON)
        out_v[rows, :] = (lat_v[rows, :].astype(F32) + projected * rs * scale).astype(BF16)
        there = pl.ds(b * 128, 128)
        outs.append(copy(out_v.at[there], out_ref.at[there], sems.at[len(ins) + b]))
        outs[b].start()
    for c in outs:
        c.wait()


KINDS = {"v": VM, "V": VM, "h": HB, "s": SM}
FIXED = {"V": VM, "h": HB}


def spec(kinds):
    return [pl.BlockSpec(memory_space=KINDS[k]) for k in kinds]


def call(kernel, name, ins, outs, scratch, copies, args, flops, limit):
    return pl.pallas_call(
        kernel,
        out_shape=[FIXED.get(k, jax.ShapeDtypeStruct)(s, d) for k, s, d in outs],
        in_specs=spec(ins),
        out_specs=spec([k for k, _, _ in outs]),
        scratch_shapes=[pltpu.VMEM(s, d) for s, d in scratch]
        + [pltpu.SemaphoreType.DMA((copies,))],
        compiler_params=pltpu.CompilerParams(vmem_limit_bytes=limit * 1024 * 1024),
        cost_estimate=pl.CostEstimate(flops=flops, bytes_accessed=0, transcendentals=0),
        name=name,
    )(
        *[
            pltpu.with_memory_space_constraint(x, FIXED[k]) if k in FIXED else x
            for k, x in zip(ins, args)
        ]
    )


def shards(
    latent, cond, ctx_rows, ctx_cond, mod_weight, norm_gain, out_gain,
    w_query, w_key, w_value, w_out, sink,
):
    sp_size = lax.axis_size("sp")
    count = sp_size * lax.axis_size("tp")
    both = ("sp", "tp")
    rows, width = latent.shape
    half = (WINDOW, width)
    wide = (rows, 1024)
    rest = (8, width)
    line = (1, width)
    square = (16, 128)
    small = w_key.shape

    parts, one, two = call(
        entry_kernel,
        "entry",
        "hhhh",
        [("h", (count, 8, 384), BF16), ("h", half, BF16), ("h", half, BF16)],
        [
            (square, BF16),
            (square, BF16),
            (mod_weight.shape, BF16),
            (latent.shape, BF16),
            ((count, 8, 384), BF16),
        ],
        7,
        (cond.reshape(square), ctx_cond.reshape(square), mod_weight, latent),
        10**6,
        8,
    )
    ng, wk_near, wv_near = call(
        prep_kernel,
        "prep",
        "hhhhh",
        [("V", (72, width), F32), ("V", small, BF16), ("V", small, BF16)],
        [(ctx_rows.shape, BF16), (line, F32)],
        4,
        (one, ctx_rows, norm_gain.reshape(line), w_key, w_value),
        2 * 10**9,
        4,
    )
    recv = lax.all_to_all(parts, both, 0, 0, tiled=True)
    swap_one = [(i, i ^ 1) for i in range(count)]
    swap_two = [(i, i + 1 if i % 2 else i - 1) for i in range(1, count - 1)]
    one = lax.ppermute(one, both, swap_one)
    two = lax.ppermute(two, both, swap_two)
    send, vecs = call(
        context_kernel,
        "context",
        "vVVV",
        [("h", (sp_size, 64, 512), BF16), ("h", rest, F32)],
        [((64, 512), BF16), (rest, F32)],
        17,
        (recv, ng, wk_near, wv_near),
        10**6,
        6,
    )
    kv_ctx = lax.all_to_all(send, "sp", 0, 0, tiled=True).reshape(sp_size * 64, 512)

    lanes = np.arange(256) % 32
    freq = 10000.0 ** (-(lanes % 16) / 16.0)
    by_row = (lanes < 16).astype(np.float32)
    angle = np.arange(GRID_W)[:, None] * freq
    colc = jnp.asarray(np.cos(angle) * (1.0 - by_row), F32)
    cols = jnp.asarray(np.sin(angle) * (1.0 - by_row), F32)
    grid_row = place_of() * (rows // GRID_W) - WINDOW // GRID_W + jnp.arange(8, dtype=jnp.int32)
    angle = grid_row.astype(F32)[:, None] * jnp.asarray(freq, F32)[None, :]
    tables = (jnp.cos(angle) * by_row, jnp.sin(angle) * by_row, colc, cols)

    query, o, l, m = call(
        local_kernel,
        "local",
        "shhhhhhhvvvv",
        [("V", wide, BF16), ("h", wide, F32), ("h", wide, F32), ("h", wide, F32)],
        [
            (rest, F32),
            ((2 * rows, width), BF16),
            ((2, width, 512), BF16),
            ((width, 512), BF16),
            ((2 * rows, width), BF16),
            (wide, F32),
            (wide, F32),
            (wide, F32),
        ],
        11,
        (sink, vecs, latent, one, two, w_query, w_key, w_value, *tables),
        10**10,
        26,
    )
    (updated,) = call(
        final_kernel,
        "final",
        "VVhhhhhhh",
        [("h", latent.shape, BF16)],
        [
            (wide, F32),
            (wide, F32),
            (wide, F32),
            (w_out.shape, BF16),
            (latent.shape, BF16),
            (rest, F32),
            (line, F32),
            (wide, F32),
            (wide, F32),
            (wide, F32),
            (latent.shape, BF16),
        ],
        24,
        (query, kv_ctx, o, l, m, w_out, latent, vecs, out_gain.reshape(line)),
        10**10,
        28,
    )
    return updated


def solution(mesh):
    placed = (
        P(("dp", "sp", "tp"), None),
        P("dp"),
        P(("dp", "sp"), None),
        P(),
        P(None, "sp", "tp"),
        P(),
        P(),
        P(),
        P(),
        P(),
        P(),
        P(),
    )
    return jax.shard_map(
        shards, mesh=mesh, in_specs=placed, out_specs=P(("dp", "sp", "tp"), None), check_vma=False
    )
```

```python
import jax
import numpy as np
import jax.numpy as jnp
from jax import lax
from jax.experimental import pallas as pl
from jax.experimental.pallas import tpu as pltpu
from jax.sharding import PartitionSpec as P

HEAD_DIM = 64
WINDOW = 128
GRID_W = 64
EPSILON = 1e-06
NEG_BIG = -1e30
LOG2E = 1.4426950408889634
FACTOR = HEAD_DIM**-0.5 * LOG2E
F32 = jnp.float32
BF16 = jnp.bfloat16
VM = pltpu.MemorySpace.VMEM
HB = pltpu.MemorySpace.HBM
SM = pltpu.MemorySpace.SMEM


def place_of():
    return lax.axis_index("sp") * lax.axis_size("tp") + lax.axis_index("tp")


def dot(a, b):
    return jnp.dot(a, b, preferred_element_type=F32)


def dot_nt(a, b):
    return lax.dot_general(a, b, (((1,), (1,)), ((), ())), preferred_element_type=F32)


def iota(shape, dim):
    return lax.broadcasted_iota(jnp.int32, shape, dim)


def swap_matrix():
    k, c = iota((256, 256), 0), iota((256, 256), 1)
    low = (c & 63) < 32
    neg = jnp.where(low & (k == c + 32), -1.0, 0.0)
    pos = jnp.where((~low) & (k == c - 32), 1.0, 0.0)
    return (neg + pos).astype(BF16)


def normed(x, mult, shift):
    x = x.astype(F32)
    rs = lax.rsqrt(jnp.mean(x * x, axis=-1, keepdims=True) + EPSILON)
    return (x * rs * mult + shift).astype(BF16)


def entry_kernel(
    cond_ref, cctx_ref, mod_ref, parts_ref, cond_v, cctx_v, mod_v, block_v, sems
):
    sp = lax.axis_index("sp")
    copy = pltpu.make_async_copy
    pairs = ((mod_ref, mod_v), (cond_ref, cond_v), (cctx_ref, cctx_v))
    ins = [copy(src, dst, sems.at[i]) for i, (src, dst) in enumerate(pairs)]
    for c in ins:
        c.start()
    ins[1].wait()
    ins[2].wait()
    here = iota((16, 128), 0) == sp
    rows = []
    for ref in (cond_v, cctx_v):
        x = jnp.sum(jnp.where(here, ref[...].astype(F32), 0.0), axis=0, keepdims=True)
        rows.append(x / (1.0 + jnp.exp(-x)))
    v = jnp.concatenate(rows + [jnp.zeros((6, 128), F32)], axis=0).astype(BF16)
    ins[0].wait()
    parts = [dot(v, mod_v[i]) for i in range(3)]
    five = (parts[0][0:1], parts[0][1:2], parts[1][0:1], parts[1][1:2], parts[2][0:1])
    zero = jnp.zeros((1, 128), F32)
    rows = []
    for j in range(4):
        cut = [x[:, j * 128 : (j + 1) * 128] for x in five]
        rows.append(jnp.concatenate(cut[:3], axis=1))
        rows.append(jnp.concatenate(cut[3:] + [zero], axis=1))
    block = jnp.concatenate(rows, axis=0).astype(BF16)
    for i in range(block_v.shape[0]):
        block_v[i] = block
    out = copy(block_v, parts_ref, sems.at[3])
    out.start()
    out.wait()


def prep_kernel(
    after_ref, ctx_ref, gain_ref, wk_ref, wv_ref, lat_ref,
    ng_ref, wk_out, wv_out, one_ref, two_ref,
    ctx_v, gain_v, lat_v, sems,
):
    odd = place_of() & 1
    copy = pltpu.make_async_copy
    pairs = ((ctx_ref, ctx_v), (gain_ref, gain_v), (wk_ref, wk_out), (wv_ref, wv_out))
    ins = [copy(src, dst, sems.at[i]) for i, (src, dst) in enumerate(pairs)]
    rows = copy(lat_ref, lat_v, sems.at[4])
    outs = [
        copy(lat_v.at[pl.ds((1 - odd) * 128, 128)], one_ref, sems.at[5]),
        copy(lat_v.at[pl.ds(odd * 128, 128)], two_ref, sems.at[6]),
    ]
    rows.start()
    for c in ins:
        c.start()
    rows.wait()
    for c in outs:
        c.start()
    ins[0].wait()
    ins[1].wait()
    x = ctx_v[...].astype(F32)
    gain = gain_v[...]
    rs = lax.rsqrt(jnp.mean(x * x, axis=-1, keepdims=True) + EPSILON)
    ng_ref[0:64, :] = x * rs * gain
    ng_ref[64:72, :] = jnp.broadcast_to(gain, (8, 2048))
    for c in ins[2:] + outs:
        c.wait()


def context_kernel(recv_ref, ng_ref, wk_ref, wv_ref, send_ref, vec_ref, kv_v, vec_v, sems):
    sums = []
    for t in range(4):
        acc = recv_ref[t].astype(F32)
        for s in range(1, 16):
            acc = acc + recv_ref[s * 4 + t].astype(F32)
        sums.append(acc)

    def vector(v):
        cuts = []
        for t in range(4):
            for j in range(4):
                r, c = 2 * j + v // 3, (v % 3) * 128
                cuts.append(sums[t][r : r + 1, c : c + 128])
        return jnp.concatenate(cuts, axis=1)

    hidden = (ng_ref[0:64, :] * (1.0 + vector(3)) + vector(1)).astype(BF16)
    kv_v[:, 0:256] = dot(hidden, wk_ref[...]).astype(BF16)
    kv_v[:, 256:512] = dot(hidden, wv_ref[...]).astype(BF16)
    copy = pltpu.make_async_copy
    outs = [copy(kv_v, send_ref.at[i], sems.at[i]) for i in range(16)]
    for c in outs:
        c.start()
    vec_v[...] = jnp.zeros((8, 2048), F32)
    vec_v[0:1, :] = ng_ref[64:65, :] * (1.0 + vector(2))
    vec_v[1:2, :] = vector(0)
    vec_v[2:3, :] = vector(4)
    outs.append(copy(vec_v, vec_ref, sems.at[16]))
    outs[16].start()
    for c in outs:
        c.wait()


def rotated(x, cos, sin, swap):
    return x.astype(F32) * cos + dot(x, swap) * sin


def paired(a, b, low):
    turned_a, turned_b = pltpu.roll(a, 64, 1), pltpu.roll(b, 64, 1)
    return jnp.where(low, a, turned_b).astype(BF16), jnp.where(low, turned_a, b).astype(BF16)


def split_pair(q, low):
    zero = jnp.zeros_like(q)
    return [jnp.where(low, q, zero), jnp.where(low, zero, q)]


def identity():
    return (iota((256, 256), 0) == iota((256, 256), 1)).astype(F32).astype(BF16)


def local_kernel(
    sink_ref, vec_ref, lat_ref, one_ref, two_ref, wq_ref, wk_ref, wv_ref,
    rowc_ref, rows_ref, colc_ref, cols_ref,
    q_ref, o_ref, lse_ref,
    vec_v, lat_v, wq_v, wkv_v, hid_v, sems,
):
    place = place_of()
    odd = place & 1
    last = lax.axis_size("sp") * lax.axis_size("tp") - 1
    copy = pltpu.make_async_copy
    own = [
        copy(vec_ref, vec_v, sems.at[0]),
        copy(lat_ref, lat_v.at[pl.ds(128, 256)], sems.at[1]),
    ]
    halo = [
        copy(one_ref, lat_v.at[pl.ds((1 - odd) * 384, 128)], sems.at[2]),
        copy(two_ref, lat_v.at[pl.ds(odd * 384, 128)], sems.at[3]),
    ]
    weights = [
        copy(wk_ref, wkv_v.at[:, pl.ds(0, 256)], sems.at[4]),
        copy(wv_ref, wkv_v.at[:, pl.ds(256, 256)], sems.at[5]),
        copy(wq_ref.at[:, pl.ds(0, 512)], wq_v.at[0], sems.at[6]),
        copy(wq_ref.at[:, pl.ds(512, 512)], wq_v.at[1], sems.at[7]),
    ]
    for c in own + halo:
        c.start()
    swap = swap_matrix()
    cos = jnp.concatenate([colc_ref[...] + rowc_ref[r : r + 1, :] for r in range(8)], axis=0)
    sin = jnp.concatenate([cols_ref[...] + rows_ref[r : r + 1, :] for r in range(8)], axis=0)
    for c in own:
        c.wait()
    for c in weights:
        c.start()
    mult, shift = vec_v[0:1, :], vec_v[1:2, :]
    for r in (1, 2):
        rows = slice(r * 128, r * 128 + 128)
        hid_v[rows, :] = normed(lat_v[rows, :], mult, shift)
    for c in halo:
        c.wait()
    for r in (0, 3):
        rows = slice(r * 128, r * 128 + 128)
        hid_v[rows, :] = normed(lat_v[rows, :], mult, shift)
    for c in weights[:2]:
        c.wait()
    kv = dot(hid_v[...], wkv_v[...]).astype(BF16)
    keys = rotated(kv[:, 0:256], cos, sin, swap).astype(BF16)
    kt = dot_nt(identity(), keys).astype(BF16)
    ones = jnp.ones((512, 128), BF16)
    low_own = iota((256, 128), 1) < HEAD_DIM
    low = iota((128, 128), 1) < HEAD_DIM
    row, col = iota((128, 128), 0), iota((128, 128), 1)
    from_low = jnp.where(col >= row, 0.0, NEG_BIG)
    from_high = jnp.where(col <= row, 0.0, NEG_BIG)
    bias = (
        (from_low + jnp.where(place > 0, 0.0, NEG_BIG), from_high),
        (from_low, from_high + jnp.where(place < last, 0.0, NEG_BIG)),
    )
    for c in weights[2:]:
        c.wait()
    slabs = []
    for a in range(2):
        q = dot(hid_v[128:384, :], wq_v[a]).astype(BF16)
        plain, turned = [], []
        for h in range(2):
            part = q[:, h * 256 : h * 256 + 256]
            plain.append(part.astype(F32))
            turned.append(rotated(part, cos[128:384], sin[128:384], swap))
        for p in range(2):
            piece = slice(p * 128, p * 128 + 128)
            at = a * 512 + p * 256
            one, two = paired(plain[0][:, piece], plain[1][:, piece], low_own)
            q_ref[:, at : at + 128] = one
            q_ref[:, at + 128 : at + 256] = two
            slabs += paired(turned[0][:, piece], turned[1][:, piece], low_own)
    eighth = (iota((128, 128), 1) & 63) >> 3
    lse = [jnp.zeros((128, 128), F32) for _ in range(2)]
    for a in range(2):
        va = jnp.concatenate([kv[:, 256 + a * 128 : 384 + a * 128], ones], axis=1)
        for b in range(2):
            rows = slice(b * 128, b * 128 + 128)
            seen = slice(b * 128, b * 128 + 384)
            stacked = []
            for g in range(4):
                stacked += split_pair(slabs[a * 4 + g][rows], low)
            s = dot(jnp.concatenate(stacked, axis=0), kt[a * 128 : a * 128 + 128, seen])
            ps, ms = [], []
            for i in range(8):
                si = s[i * 128 : i * 128 + 128]
                s0, s1, s2 = si[:, 0:128] + bias[b][0], si[:, 128:256], si[:, 256:384] + bias[b][1]
                sink = sink_ref[(2 * a + i % 2) * 4 + i // 2] * LOG2E
                m = jnp.max(jnp.maximum(jnp.maximum(s0, s1), s2), axis=-1, keepdims=True)
                m = jnp.maximum(m * FACTOR, sink)
                p = [jnp.exp2(x * FACTOR - m).astype(BF16) for x in (s0, s1, s2)]
                ps.append(jnp.concatenate(p, axis=1))
                ms.append((jnp.broadcast_to(m, (128, 128)), sink))
            o = dot(jnp.concatenate(ps, axis=0), va[seen])
            for g in range(4):
                to = slice(a * 512 + g * 128, a * 512 + g * 128 + 128)
                x, y = o[g * 256 : g * 256 + 128], o[g * 256 + 128 : g * 256 + 256]
                (mx, sx), (my, sy) = ms[2 * g], ms[2 * g + 1]
                m = jnp.where(low, mx, my)
                l = jnp.where(low, x[:, 128:256], y[:, 128:256])
                l = l + jnp.exp2(jnp.where(low, sx, sy) - m)
                o_ref[rows, to] = jnp.where(low, x[:, 0:128], y[:, 0:128]) / l
                lse[b] = jnp.where(eighth == a * 4 + g, m + jnp.log2(l), lse[b])
    for b in range(2):
        lse_ref[b * 128 : b * 128 + 128, :] = lse[b]


def final_kernel(
    q_ref, kv_ref, o_ref, lse_ref, wo_ref, lat_ref, vec_ref, gain_ref, out_ref,
    wo_v, lat_v, vec_v, gain_v, oc_v, lc_v, mc_v, out_v, sems,
):
    copy = pltpu.make_async_copy
    pairs = [(lat_ref, lat_v), (vec_ref, vec_v), (gain_ref, gain_v)]
    for a in range(2):
        for g in range(4):
            for i in range(2):
                head = (2 * a + i) * 4 + g
                to = ((a * 4 + g) * 2 + i) * HEAD_DIM
                pairs.append((wo_ref.at[pl.ds(head * 64, 64)], wo_v.at[pl.ds(to, 64)]))
    ins = [copy(src, dst, sems.at[i]) for i, (src, dst) in enumerate(pairs)]
    for c in ins:
        c.start()
    low = iota((256, 128), 1) < HEAD_DIM
    ones = jnp.ones((1024, 128), BF16)
    kt = dot_nt(identity(), kv_ref[:, 0:256]).astype(BF16)
    slabs = [slice(i * 128, i * 128 + 128) for i in range(8)]

    def scores(i):
        stacked = jnp.concatenate(split_pair(q_ref[:, slabs[i]], low), axis=0)
        return dot(stacked, kt[(i // 4) * 128 : (i // 4) * 128 + 128, :])

    s = scores(0)
    for i in range(8):
        coming = scores(i + 1) if i < 7 else None
        a = i // 4
        va = jnp.concatenate([kv_ref[:, 256 + a * 128 : 384 + a * 128], ones], axis=1)
        m = jnp.max(s, axis=-1, keepdims=True) * FACTOR
        o = dot(jnp.exp2(s * FACTOR - m).astype(BF16), va)
        m = jnp.broadcast_to(m, (512, 128))
        mc_v[:, slabs[i]] = jnp.where(low, m[0:256], m[256:512])
        oc_v[:, slabs[i]] = jnp.where(low, o[0:256, 0:128], o[256:512, 0:128])
        lc_v[:, slabs[i]] = jnp.where(low, o[0:256, 128:256], o[256:512, 128:256])
        s = coming
    for c in ins:
        c.wait()
    scale = vec_v[2:3, :] * gain_v[...]
    outs = []
    for b in range(2):
        rows = slice(b * 128, b * 128 + 128)
        mixed = []
        for i, to in enumerate(slabs):
            here = [lse_ref[rows, c : c + 1] for c in (i * 8, i * 8 + 64)]
            here = [jnp.broadcast_to(x, (128, 128)) for x in here]
            ml, mc = jnp.where(low[0:128], here[0], here[1]), mc_v[rows, to]
            top = jnp.maximum(ml, mc)
            wl, wc = jnp.exp2(ml - top), jnp.exp2(mc - top)
            num = wl * o_ref[rows, to] + wc * oc_v[rows, to]
            den = wl + wc * lc_v[rows, to]
            mixed.append((num / den).astype(BF16))
        projected = dot(jnp.concatenate(mixed, axis=1), wo_v[...])
        rs = lax.rsqrt(jnp.mean(projected * projected, axis=-1, keepdims=True) + EPSILON)
        out_v[rows, :] = (lat_v[rows, :].astype(F32) + projected * rs * scale).astype(BF16)
        there = pl.ds(b * 128, 128)
        outs.append(copy(out_v.at[there], out_ref.at[there], sems.at[len(ins) + b]))
        outs[b].start()
    for c in outs:
        c.wait()


KINDS = {"v": VM, "V": VM, "h": HB, "s": SM}
FIXED = {"V": VM, "h": HB}


def spec(kinds):
    return [pl.BlockSpec(memory_space=KINDS[k]) for k in kinds]


def call(kernel, name, ins, outs, scratch, copies, args, flops, limit):
    return pl.pallas_call(
        kernel,
        out_shape=[FIXED.get(k, jax.ShapeDtypeStruct)(s, d) for k, s, d in outs],
        in_specs=spec(ins),
        out_specs=spec([k for k, _, _ in outs]),
        scratch_shapes=[pltpu.VMEM(s, d) for s, d in scratch]
        + [pltpu.SemaphoreType.DMA((copies,))],
        compiler_params=pltpu.CompilerParams(vmem_limit_bytes=limit * 1024 * 1024),
        cost_estimate=pl.CostEstimate(flops=flops, bytes_accessed=0, transcendentals=0),
        name=name,
    )(
        *[
            pltpu.with_memory_space_constraint(x, FIXED[k]) if k in FIXED else x
            for k, x in zip(ins, args)
        ]
    )


def shards(
    latent, cond, ctx_rows, ctx_cond, mod_weight, norm_gain, out_gain,
    w_query, w_key, w_value, w_out, sink,
):
    sp_size = lax.axis_size("sp")
    count = sp_size * lax.axis_size("tp")
    both = ("sp", "tp")
    rows, width = latent.shape
    half = (WINDOW, width)
    wide = (rows, 1024)
    rest = (8, width)
    line = (1, width)
    square = (16, 128)
    small = w_key.shape

    (parts,) = call(
        entry_kernel,
        "entry",
        "hhh",
        [("h", (count, 8, 384), BF16)],
        [(square, BF16), (square, BF16), (mod_weight.shape, BF16), ((count, 8, 384), BF16)],
        4,
        (cond.reshape(square), ctx_cond.reshape(square), mod_weight),
        10**6,
        8,
    )
    ng, wk_near, wv_near, one, two = call(
        prep_kernel,
        "prep",
        "hhhhhh",
        [
            ("V", (72, width), F32),
            ("V", small, BF16),
            ("V", small, BF16),
            ("h", half, BF16),
            ("h", half, BF16),
        ],
        [(ctx_rows.shape, BF16), (line, F32), (latent.shape, BF16)],
        7,
        (parts, ctx_rows, norm_gain.reshape(line), w_key, w_value, latent),
        2 * 10**9,
        4,
    )
    recv = lax.all_to_all(parts, both, 0, 0, tiled=True)
    swap_one = [(i, i ^ 1) for i in range(count)]
    swap_two = [(i, i + 1 if i % 2 else i - 1) for i in range(1, count - 1)]
    one = lax.ppermute(one, both, swap_one)
    two = lax.ppermute(two, both, swap_two)
    send, vecs = call(
        context_kernel,
        "context",
        "vVVV",
        [("h", (sp_size, 64, 512), BF16), ("h", rest, F32)],
        [((64, 512), BF16), (rest, F32)],
        17,
        (recv, ng, wk_near, wv_near),
        10**6,
        6,
    )
    kv_ctx = lax.all_to_all(send, "sp", 0, 0, tiled=True).reshape(sp_size * 64, 512)

    lanes = np.arange(256) % 32
    freq = 10000.0 ** (-(lanes % 16) / 16.0)
    by_row = (lanes < 16).astype(np.float32)
    angle = np.arange(GRID_W)[:, None] * freq
    colc = jnp.asarray(np.cos(angle) * (1.0 - by_row), F32)
    cols = jnp.asarray(np.sin(angle) * (1.0 - by_row), F32)
    grid_row = place_of() * (rows // GRID_W) - WINDOW // GRID_W + jnp.arange(8, dtype=jnp.int32)
    angle = grid_row.astype(F32)[:, None] * jnp.asarray(freq, F32)[None, :]
    tables = (jnp.cos(angle) * by_row, jnp.sin(angle) * by_row, colc, cols)

    query, o, lse = call(
        local_kernel,
        "local",
        "shhhhhhhvvvv",
        [("V", wide, BF16), ("V", wide, F32), ("V", (rows, 128), F32)],
        [
            (rest, F32),
            ((2 * rows, width), BF16),
            ((2, width, 512), BF16),
            ((width, 512), BF16),
            ((2 * rows, width), BF16),
        ],
        8,
        (sink, vecs, latent, one, two, w_query, w_key, w_value, *tables),
        10**10,
        26,
    )
    (updated,) = call(
        final_kernel,
        "final",
        "VVVVhhhh",
        [("h", latent.shape, BF16)],
        [
            (w_out.shape, BF16),
            (latent.shape, BF16),
            (rest, F32),
            (line, F32),
            (wide, F32),
            (wide, F32),
            (wide, F32),
            (latent.shape, BF16),
        ],
        21,
        (query, kv_ctx, o, lse, w_out, latent, vecs, out_gain.reshape(line)),
        10**10,
        28,
    )
    return updated


def solution(mesh):
    placed = (
        P(("dp", "sp", "tp"), None),
        P("dp"),
        P(("dp", "sp"), None),
        P(),
        P(None, "sp", "tp"),
        P(),
        P(),
        P(),
        P(),
        P(),
        P(),
        P(),
    )
    return jax.shard_map(
        shards, mesh=mesh, in_specs=placed, out_specs=P(("dp", "sp", "tp"), None), check_vma=False
    )
```

```python
import jax
import numpy as np
import jax.numpy as jnp
from jax import lax
from jax.experimental import pallas as pl
from jax.experimental.pallas import tpu as pltpu
from jax.sharding import PartitionSpec as P

HEAD_DIM = 64
WINDOW = 128
GRID_W = 64
EPSILON = 1e-06
NEG_BIG = -1e30
LOG2E = 1.4426950408889634
FACTOR = HEAD_DIM**-0.5 * LOG2E
F32 = jnp.float32
BF16 = jnp.bfloat16
VM = pltpu.MemorySpace.VMEM
HB = pltpu.MemorySpace.HBM
SM = pltpu.MemorySpace.SMEM


def place_of():
    return lax.axis_index("sp") * lax.axis_size("tp") + lax.axis_index("tp")


def dot(a, b):
    return jnp.dot(a, b, preferred_element_type=F32)


def dot_nt(a, b):
    return lax.dot_general(a, b, (((1,), (1,)), ((), ())), preferred_element_type=F32)


def iota(shape, dim):
    return lax.broadcasted_iota(jnp.int32, shape, dim)


def swap_matrix():
    k, c = iota((256, 256), 0), iota((256, 256), 1)
    low = (c & 63) < 32
    neg = jnp.where(low & (k == c + 32), -1.0, 0.0)
    pos = jnp.where((~low) & (k == c - 32), 1.0, 0.0)
    return (neg + pos).astype(BF16)


def normed(x, mult, shift):
    x = x.astype(F32)
    rs = lax.rsqrt(jnp.mean(x * x, axis=-1, keepdims=True) + EPSILON)
    return (x * rs * mult + shift).astype(BF16)


def entry_kernel(
    cond_ref, cctx_ref, mod_ref, lat_ref,
    parts_ref, one_ref, two_ref,
    cond_v, cctx_v, mod_v, lat_v, block_v, sems,
):
    sp = lax.axis_index("sp")
    odd = place_of() & 1
    copy = pltpu.make_async_copy
    pairs = ((mod_ref, mod_v), (cond_ref, cond_v), (cctx_ref, cctx_v), (lat_ref, lat_v))
    ins = [copy(src, dst, sems.at[i]) for i, (src, dst) in enumerate(pairs)]
    for c in ins:
        c.start()
    ins[1].wait()
    ins[2].wait()
    here = iota((16, 128), 0) == sp
    rows = []
    for ref in (cond_v, cctx_v):
        x = jnp.sum(jnp.where(here, ref[...].astype(F32), 0.0), axis=0, keepdims=True)
        rows.append(x / (1.0 + jnp.exp(-x)))
    v = jnp.concatenate(rows + [jnp.zeros((6, 128), F32)], axis=0).astype(BF16)
    ins[0].wait()
    parts = [dot(v, mod_v[i]) for i in range(3)]
    five = (parts[0][0:1], parts[0][1:2], parts[1][0:1], parts[1][1:2], parts[2][0:1])
    zero = jnp.zeros((1, 128), F32)
    rows = []
    for j in range(4):
        cut = [x[:, j * 128 : (j + 1) * 128] for x in five]
        rows.append(jnp.concatenate(cut[:3], axis=1))
        rows.append(jnp.concatenate(cut[3:] + [zero], axis=1))
    block = jnp.concatenate(rows, axis=0).astype(BF16)
    for i in range(block_v.shape[0]):
        block_v[i] = block
    outs = [
        copy(block_v, parts_ref, sems.at[4]),
        copy(lat_v.at[pl.ds((1 - odd) * 128, 128)], one_ref, sems.at[5]),
        copy(lat_v.at[pl.ds(odd * 128, 128)], two_ref, sems.at[6]),
    ]
    outs[0].start()
    ins[3].wait()
    outs[1].start()
    outs[2].start()
    for c in outs:
        c.wait()


def prep_kernel(
    after_ref, ctx_ref, gain_ref, wk_ref, wv_ref, ng_ref, wk_out, wv_out, ctx_v, gain_v, sems
):
    copy = pltpu.make_async_copy
    pairs = ((ctx_ref, ctx_v), (gain_ref, gain_v), (wk_ref, wk_out), (wv_ref, wv_out))
    ins = [copy(src, dst, sems.at[i]) for i, (src, dst) in enumerate(pairs)]
    for c in ins:
        c.start()
    ins[0].wait()
    ins[1].wait()
    x = ctx_v[...].astype(F32)
    gain = gain_v[...]
    rs = lax.rsqrt(jnp.mean(x * x, axis=-1, keepdims=True) + EPSILON)
    ng_ref[0:64, :] = x * rs * gain
    ng_ref[64:72, :] = jnp.broadcast_to(gain, (8, 2048))
    for c in ins[2:]:
        c.wait()


def context_kernel(recv_ref, ng_ref, wk_ref, wv_ref, send_ref, vec_ref, kv_v, vec_v, sems):
    sums = []
    for t in range(4):
        acc = recv_ref[t].astype(F32)
        for s in range(1, 16):
            acc = acc + recv_ref[s * 4 + t].astype(F32)
        sums.append(acc)

    def vector(v):
        cuts = []
        for t in range(4):
            for j in range(4):
                r, c = 2 * j + v // 3, (v % 3) * 128
                cuts.append(sums[t][r : r + 1, c : c + 128])
        return jnp.concatenate(cuts, axis=1)

    hidden = (ng_ref[0:64, :] * (1.0 + vector(3)) + vector(1)).astype(BF16)
    kv_v[:, 0:256] = dot(hidden, wk_ref[...]).astype(BF16)
    kv_v[:, 256:512] = dot(hidden, wv_ref[...]).astype(BF16)
    copy = pltpu.make_async_copy
    outs = [copy(kv_v, send_ref.at[i], sems.at[i]) for i in range(16)]
    for c in outs:
        c.start()
    vec_v[...] = jnp.zeros((8, 2048), F32)
    vec_v[0:1, :] = ng_ref[64:65, :] * (1.0 + vector(2))
    vec_v[1:2, :] = vector(0)
    vec_v[2:3, :] = vector(4)
    outs.append(copy(vec_v, vec_ref, sems.at[16]))
    outs[16].start()
    for c in outs:
        c.wait()


def rotated(x, cos, sin, swap):
    return x.astype(F32) * cos + dot(x, swap) * sin


def paired(a, b, low):
    turned_a, turned_b = pltpu.roll(a, 64, 1), pltpu.roll(b, 64, 1)
    return jnp.where(low, a, turned_b).astype(BF16), jnp.where(low, turned_a, b).astype(BF16)


def split_pair(q, low):
    zero = jnp.zeros_like(q)
    return [jnp.where(low, q, zero), jnp.where(low, zero, q)]


def identity():
    return (iota((256, 256), 0) == iota((256, 256), 1)).astype(F32).astype(BF16)


def local_kernel(
    sink_ref, vec_ref, lat_ref, one_ref, two_ref, wq_ref, wk_ref, wv_ref,
    rowc_ref, rows_ref, colc_ref, cols_ref,
    q_ref, o_ref, lse_ref,
    vec_v, lat_v, wq_v, wkv_v, hid_v, sems,
):
    place = place_of()
    odd = place & 1
    last = lax.axis_size("sp") * lax.axis_size("tp") - 1
    copy = pltpu.make_async_copy
    own = [
        copy(vec_ref, vec_v, sems.at[0]),
        copy(lat_ref, lat_v.at[pl.ds(128, 256)], sems.at[1]),
    ]
    halo = [
        copy(one_ref, lat_v.at[pl.ds((1 - odd) * 384, 128)], sems.at[2]),
        copy(two_ref, lat_v.at[pl.ds(odd * 384, 128)], sems.at[3]),
    ]
    weights = [
        copy(wk_ref, wkv_v.at[:, pl.ds(0, 256)], sems.at[4]),
        copy(wv_ref, wkv_v.at[:, pl.ds(256, 256)], sems.at[5]),
        copy(wq_ref.at[:, pl.ds(0, 512)], wq_v.at[0], sems.at[6]),
        copy(wq_ref.at[:, pl.ds(512, 512)], wq_v.at[1], sems.at[7]),
    ]
    for c in own + halo:
        c.start()
    swap = swap_matrix()
    cos = jnp.concatenate([colc_ref[...] + rowc_ref[r : r + 1, :] for r in range(8)], axis=0)
    sin = jnp.concatenate([cols_ref[...] + rows_ref[r : r + 1, :] for r in range(8)], axis=0)
    for c in own:
        c.wait()
    for c in weights:
        c.start()
    mult, shift = vec_v[0:1, :], vec_v[1:2, :]
    for r in (1, 2):
        rows = slice(r * 128, r * 128 + 128)
        hid_v[rows, :] = normed(lat_v[rows, :], mult, shift)
    for c in halo:
        c.wait()
    for r in (0, 3):
        rows = slice(r * 128, r * 128 + 128)
        hid_v[rows, :] = normed(lat_v[rows, :], mult, shift)
    for c in weights[:2]:
        c.wait()
    kv = dot(hid_v[...], wkv_v[...]).astype(BF16)
    keys = rotated(kv[:, 0:256], cos, sin, swap).astype(BF16)
    kt = dot_nt(identity(), keys).astype(BF16)
    ones = jnp.ones((512, 128), BF16)
    low_own = iota((256, 128), 1) < HEAD_DIM
    low = iota((128, 128), 1) < HEAD_DIM
    row, col = iota((128, 128), 0), iota((128, 128), 1)
    from_low = jnp.where(col >= row, 0.0, NEG_BIG)
    from_high = jnp.where(col <= row, 0.0, NEG_BIG)
    bias = (
        (from_low + jnp.where(place > 0, 0.0, NEG_BIG), from_high),
        (from_low, from_high + jnp.where(place < last, 0.0, NEG_BIG)),
    )
    for c in weights[2:]:
        c.wait()
    slabs = []
    for a in range(2):
        q = dot(hid_v[128:384, :], wq_v[a]).astype(BF16)
        plain, turned = [], []
        for h in range(2):
            part = q[:, h * 256 : h * 256 + 256]
            plain.append(part.astype(F32))
            turned.append(rotated(part, cos[128:384], sin[128:384], swap))
        for p in range(2):
            piece = slice(p * 128, p * 128 + 128)
            at = a * 512 + p * 256
            one, two = paired(plain[0][:, piece], plain[1][:, piece], low_own)
            q_ref[:, at : at + 128] = one
            q_ref[:, at + 128 : at + 256] = two
            slabs += paired(turned[0][:, piece], turned[1][:, piece], low_own)
    eighth = (iota((128, 128), 1) & 63) >> 3
    lse = [jnp.zeros((128, 128), F32) for _ in range(2)]
    for a in range(2):
        va = jnp.concatenate([kv[:, 256 + a * 128 : 384 + a * 128], ones], axis=1)
        for b in range(2):
            rows = slice(b * 128, b * 128 + 128)
            seen = slice(b * 128, b * 128 + 384)
            stacked = []
            for g in range(4):
                stacked += split_pair(slabs[a * 4 + g][rows], low)
            s = dot(jnp.concatenate(stacked, axis=0), kt[a * 128 : a * 128 + 128, seen])
            ps, ms = [], []
            for i in range(8):
                si = s[i * 128 : i * 128 + 128]
                s0, s1, s2 = si[:, 0:128] + bias[b][0], si[:, 128:256], si[:, 256:384] + bias[b][1]
                sink = sink_ref[(2 * a + i % 2) * 4 + i // 2] * LOG2E
                m = jnp.max(jnp.maximum(jnp.maximum(s0, s1), s2), axis=-1, keepdims=True)
                m = jnp.maximum(m * FACTOR, sink)
                p = [jnp.exp2(x * FACTOR - m).astype(BF16) for x in (s0, s1, s2)]
                ps.append(jnp.concatenate(p, axis=1))
                ms.append((jnp.broadcast_to(m, (128, 128)), sink))
            o = dot(jnp.concatenate(ps, axis=0), va[seen])
            for g in range(4):
                to = slice(a * 512 + g * 128, a * 512 + g * 128 + 128)
                x, y = o[g * 256 : g * 256 + 128], o[g * 256 + 128 : g * 256 + 256]
                (mx, sx), (my, sy) = ms[2 * g], ms[2 * g + 1]
                m = jnp.where(low, mx, my)
                l = jnp.where(low, x[:, 128:256], y[:, 128:256])
                l = l + jnp.exp2(jnp.where(low, sx, sy) - m)
                o_ref[rows, to] = jnp.where(low, x[:, 0:128], y[:, 0:128]) / l
                lse[b] = jnp.where(eighth == a * 4 + g, m + jnp.log2(l), lse[b])
    for b in range(2):
        lse_ref[b * 128 : b * 128 + 128, :] = lse[b]


def final_kernel(
    q_ref, kv_ref, o_ref, lse_ref, wo_ref, lat_ref, vec_ref, gain_ref, out_ref,
    wo_v, lat_v, vec_v, gain_v, mix_v, out_v, kt_v, va_v, even_v, odd_v, sems,
):
    copy = pltpu.make_async_copy
    pairs = [(lat_ref, lat_v), (vec_ref, vec_v), (gain_ref, gain_v)]
    for a in range(2):
        for g in range(4):
            for i in range(2):
                head = (2 * a + i) * 4 + g
                to = ((a * 4 + g) * 2 + i) * HEAD_DIM
                pairs.append((wo_ref.at[pl.ds(head * 64, 64)], wo_v.at[pl.ds(to, 64)]))
    ins = [copy(src, dst, sems.at[i]) for i, (src, dst) in enumerate(pairs)]
    for c in ins:
        c.start()
    low = iota((256, 128), 1) < HEAD_DIM
    eye = identity()
    for a in range(2):
        kt_v[a] = dot_nt(eye[a * 128 : a * 128 + 128], kv_ref[:, 0:256]).astype(BF16)
        va_v[a, :, 0:128] = kv_ref[:, 256 + a * 128 : 384 + a * 128]
        va_v[a, :, 128:256] = jnp.ones((1024, 128), BF16)

    def scores(i, s_ref):
        q = q_ref[:, pl.ds(pl.multiple_of(i * 128, 128), 128)]
        stacked = jnp.concatenate(split_pair(q, low), axis=0)
        s_ref[...] = dot(stacked, kt_v[i // 4])

    def attend(i, s_ref):
        s = s_ref[...]
        m = jnp.max(s, axis=-1, keepdims=True) * FACTOR
        o = dot(jnp.exp2(s * FACTOR - m).astype(BF16), va_v[i // 4])
        m = jnp.broadcast_to(m, (512, 128))
        mc = jnp.where(low, m[0:256], m[256:512])
        oc = jnp.where(low, o[0:256, 0:128], o[256:512, 0:128])
        lc = jnp.where(low, o[0:256, 128:256], o[256:512, 128:256])
        at = pl.ds(pl.multiple_of(i * 128, 128), 128)
        lse = pltpu.roll(lse_ref[...], (128 - 8 * i) & 127, 1)
        here = [jnp.broadcast_to(lse[:, c : c + 1], (256, 128)) for c in (0, 64)]
        ml = jnp.where(low, here[0], here[1])
        top = jnp.maximum(ml, mc)
        wl, wc = jnp.exp2(ml - top), jnp.exp2(mc - top)
        mix_v[:, at] = ((wl * o_ref[:, at] + wc * oc) / (wl + wc * lc)).astype(BF16)

    scores(0, even_v)

    def two(j, carry):
        i = 2 * j
        scores(i + 1, odd_v)
        attend(i, even_v)
        scores(jnp.minimum(i + 2, 7), even_v)
        attend(i + 1, odd_v)
        return carry

    lax.fori_loop(0, 4, two, 0)
    for c in ins:
        c.wait()
    scale = vec_v[2:3, :] * gain_v[...]
    outs = []
    for b in range(2):
        rows = slice(b * 128, b * 128 + 128)
        projected = dot(mix_v[rows, :], wo_v[...])
        rs = lax.rsqrt(jnp.mean(projected * projected, axis=-1, keepdims=True) + EPSILON)
        out_v[rows, :] = (lat_v[rows, :].astype(F32) + projected * rs * scale).astype(BF16)
        there = pl.ds(b * 128, 128)
        outs.append(copy(out_v.at[there], out_ref.at[there], sems.at[len(ins) + b]))
        outs[b].start()
    for c in outs:
        c.wait()


KINDS = {"v": VM, "V": VM, "h": HB, "s": SM}
FIXED = {"V": VM, "h": HB}


def spec(kinds):
    return [pl.BlockSpec(memory_space=KINDS[k]) for k in kinds]


def call(kernel, name, ins, outs, scratch, copies, args, flops, limit):
    return pl.pallas_call(
        kernel,
        out_shape=[FIXED.get(k, jax.ShapeDtypeStruct)(s, d) for k, s, d in outs],
        in_specs=spec(ins),
        out_specs=spec([k for k, _, _ in outs]),
        scratch_shapes=[pltpu.VMEM(s, d) for s, d in scratch]
        + [pltpu.SemaphoreType.DMA((copies,))],
        compiler_params=pltpu.CompilerParams(vmem_limit_bytes=limit * 1024 * 1024),
        cost_estimate=pl.CostEstimate(flops=flops, bytes_accessed=0, transcendentals=0),
        name=name,
    )(
        *[
            pltpu.with_memory_space_constraint(x, FIXED[k]) if k in FIXED else x
            for k, x in zip(ins, args)
        ]
    )


def shards(
    latent, cond, ctx_rows, ctx_cond, mod_weight, norm_gain, out_gain,
    w_query, w_key, w_value, w_out, sink,
):
    sp_size = lax.axis_size("sp")
    count = sp_size * lax.axis_size("tp")
    both = ("sp", "tp")
    rows, width = latent.shape
    half = (WINDOW, width)
    wide = (rows, 1024)
    rest = (8, width)
    line = (1, width)
    square = (16, 128)
    small = w_key.shape

    parts, one, two = call(
        entry_kernel,
        "entry",
        "hhhh",
        [("h", (count, 8, 384), BF16), ("h", half, BF16), ("h", half, BF16)],
        [
            (square, BF16),
            (square, BF16),
            (mod_weight.shape, BF16),
            (latent.shape, BF16),
            ((count, 8, 384), BF16),
        ],
        7,
        (cond.reshape(square), ctx_cond.reshape(square), mod_weight, latent),
        10**6,
        8,
    )
    ng, wk_near, wv_near = call(
        prep_kernel,
        "prep",
        "hhhhh",
        [("V", (72, width), F32), ("V", small, BF16), ("V", small, BF16)],
        [(ctx_rows.shape, BF16), (line, F32)],
        4,
        (one, ctx_rows, norm_gain.reshape(line), w_key, w_value),
        2 * 10**9,
        4,
    )
    recv = lax.all_to_all(parts, both, 0, 0, tiled=True)
    swap_one = [(i, i ^ 1) for i in range(count)]
    swap_two = [(i, i + 1 if i % 2 else i - 1) for i in range(1, count - 1)]
    one = lax.ppermute(one, both, swap_one)
    two = lax.ppermute(two, both, swap_two)
    send, vecs = call(
        context_kernel,
        "context",
        "vVVV",
        [("h", (sp_size, 64, 512), BF16), ("h", rest, F32)],
        [((64, 512), BF16), (rest, F32)],
        17,
        (recv, ng, wk_near, wv_near),
        10**6,
        6,
    )
    kv_ctx = lax.all_to_all(send, "sp", 0, 0, tiled=True).reshape(sp_size * 64, 512)

    lanes = np.arange(256) % 32
    freq = 10000.0 ** (-(lanes % 16) / 16.0)
    by_row = (lanes < 16).astype(np.float32)
    angle = np.arange(GRID_W)[:, None] * freq
    colc = jnp.asarray(np.cos(angle) * (1.0 - by_row), F32)
    cols = jnp.asarray(np.sin(angle) * (1.0 - by_row), F32)
    grid_row = place_of() * (rows // GRID_W) - WINDOW // GRID_W + jnp.arange(8, dtype=jnp.int32)
    angle = grid_row.astype(F32)[:, None] * jnp.asarray(freq, F32)[None, :]
    tables = (jnp.cos(angle) * by_row, jnp.sin(angle) * by_row, colc, cols)

    query, o, lse = call(
        local_kernel,
        "local",
        "shhhhhhhvvvv",
        [("V", wide, BF16), ("V", wide, F32), ("V", (rows, 128), F32)],
        [
            (rest, F32),
            ((2 * rows, width), BF16),
            ((2, width, 512), BF16),
            ((width, 512), BF16),
            ((2 * rows, width), BF16),
        ],
        8,
        (sink, vecs, latent, one, two, w_query, w_key, w_value, *tables),
        10**10,
        26,
    )
    (updated,) = call(
        final_kernel,
        "final",
        "VVVVhhhh",
        [("h", latent.shape, BF16)],
        [
            (w_out.shape, BF16),
            (latent.shape, BF16),
            (rest, F32),
            (line, F32),
            (wide, BF16),
            (latent.shape, BF16),
            ((2, 128, 1024), BF16),
            ((2, 1024, 256), BF16),
            ((512, 1024), F32),
            ((512, 1024), F32),
        ],
        21,
        (query, kv_ctx, o, lse, w_out, latent, vecs, out_gain.reshape(line)),
        10**10,
        28,
    )
    return updated


def solution(mesh):
    placed = (
        P(("dp", "sp", "tp"), None),
        P("dp"),
        P(("dp", "sp"), None),
        P(),
        P(None, "sp", "tp"),
        P(),
        P(),
        P(),
        P(),
        P(),
        P(),
        P(),
    )
    return jax.shard_map(
        shards, mesh=mesh, in_specs=placed, out_specs=P(("dp", "sp", "tp"), None), check_vma=False
    )
```

```python
import jax
import numpy as np
import jax.numpy as jnp
from jax import lax
from jax.experimental import pallas as pl
from jax.experimental.pallas import tpu as pltpu
from jax.sharding import PartitionSpec as P

HEAD_DIM = 64
WINDOW = 128
GRID_W = 64
EPSILON = 1e-06
NEG_BIG = -1e30
LOG2E = 1.4426950408889634
FACTOR = HEAD_DIM**-0.5 * LOG2E
F32 = jnp.float32
BF16 = jnp.bfloat16
VM = pltpu.MemorySpace.VMEM
HB = pltpu.MemorySpace.HBM
SM = pltpu.MemorySpace.SMEM


def place_of():
    return lax.axis_index("sp") * lax.axis_size("tp") + lax.axis_index("tp")


def dot(a, b):
    return jnp.dot(a, b, preferred_element_type=F32)


def dot_nt(a, b):
    return lax.dot_general(a, b, (((1,), (1,)), ((), ())), preferred_element_type=F32)


def iota(shape, dim):
    return lax.broadcasted_iota(jnp.int32, shape, dim)


def swap_matrix():
    k, c = iota((256, 256), 0), iota((256, 256), 1)
    low = (c & 63) < 32
    neg = jnp.where(low & (k == c + 32), -1.0, 0.0)
    pos = jnp.where((~low) & (k == c - 32), 1.0, 0.0)
    return (neg + pos).astype(BF16)


def normed(x, mult, shift):
    x = x.astype(F32)
    rs = lax.rsqrt(jnp.mean(x * x, axis=-1, keepdims=True) + EPSILON)
    return (x * rs * mult + shift).astype(BF16)


def entry_kernel(
    cond_ref, cctx_ref, mod_ref, lat_ref,
    parts_ref, one_ref, two_ref,
    cond_v, cctx_v, mod_v, lat_v, block_v, sems,
):
    sp = lax.axis_index("sp")
    odd = place_of() & 1
    copy = pltpu.make_async_copy
    pairs = ((mod_ref, mod_v), (cond_ref, cond_v), (cctx_ref, cctx_v), (lat_ref, lat_v))
    ins = [copy(src, dst, sems.at[i]) for i, (src, dst) in enumerate(pairs)]
    for c in ins:
        c.start()
    ins[1].wait()
    ins[2].wait()
    here = iota((16, 128), 0) == sp
    rows = []
    for ref in (cond_v, cctx_v):
        x = jnp.sum(jnp.where(here, ref[...].astype(F32), 0.0), axis=0, keepdims=True)
        rows.append(x / (1.0 + jnp.exp(-x)))
    v = jnp.concatenate(rows + [jnp.zeros((6, 128), F32)], axis=0).astype(BF16)
    ins[0].wait()
    parts = [dot(v, mod_v[i]) for i in range(3)]
    five = (parts[0][0:1], parts[0][1:2], parts[1][0:1], parts[1][1:2], parts[2][0:1])
    zero = jnp.zeros((1, 128), F32)
    rows = []
    for j in range(4):
        cut = [x[:, j * 128 : (j + 1) * 128] for x in five]
        rows.append(jnp.concatenate(cut[:3], axis=1))
        rows.append(jnp.concatenate(cut[3:] + [zero], axis=1))
    block = jnp.concatenate(rows, axis=0).astype(BF16)
    for i in range(block_v.shape[0]):
        block_v[i] = block
    outs = [
        copy(block_v, parts_ref, sems.at[4]),
        copy(lat_v.at[pl.ds((1 - odd) * 128, 128)], one_ref, sems.at[5]),
        copy(lat_v.at[pl.ds(odd * 128, 128)], two_ref, sems.at[6]),
    ]
    outs[0].start()
    ins[3].wait()
    outs[1].start()
    outs[2].start()
    for c in outs:
        c.wait()


def prep_kernel(
    after_ref, ctx_ref, gain_ref, wk_ref, wv_ref, ng_ref, wk_out, wv_out, ctx_v, gain_v, sems
):
    copy = pltpu.make_async_copy
    pairs = ((ctx_ref, ctx_v), (gain_ref, gain_v), (wk_ref, wk_out), (wv_ref, wv_out))
    ins = [copy(src, dst, sems.at[i]) for i, (src, dst) in enumerate(pairs)]
    for c in ins:
        c.start()
    ins[0].wait()
    ins[1].wait()
    x = ctx_v[...].astype(F32)
    gain = gain_v[...]
    rs = lax.rsqrt(jnp.mean(x * x, axis=-1, keepdims=True) + EPSILON)
    ng_ref[0:64, :] = x * rs * gain
    ng_ref[64:72, :] = jnp.broadcast_to(gain, (8, 2048))
    for c in ins[2:]:
        c.wait()


def context_kernel(recv_ref, ng_ref, wk_ref, wv_ref, send_ref, vec_ref, kv_v, vec_v, sems):
    sums = []
    for t in range(4):
        acc = recv_ref[t].astype(F32)
        for s in range(1, 16):
            acc = acc + recv_ref[s * 4 + t].astype(F32)
        sums.append(acc)

    def vector(v):
        cuts = []
        for t in range(4):
            for j in range(4):
                r, c = 2 * j + v // 3, (v % 3) * 128
                cuts.append(sums[t][r : r + 1, c : c + 128])
        return jnp.concatenate(cuts, axis=1)

    hidden = (ng_ref[0:64, :] * (1.0 + vector(3)) + vector(1)).astype(BF16)
    kv_v[:, 0:256] = dot(hidden, wk_ref[...]).astype(BF16)
    kv_v[:, 256:512] = dot(hidden, wv_ref[...]).astype(BF16)
    copy = pltpu.make_async_copy
    outs = [copy(kv_v, send_ref.at[i], sems.at[i]) for i in range(16)]
    for c in outs:
        c.start()
    vec_v[...] = jnp.zeros((8, 2048), F32)
    vec_v[0:1, :] = ng_ref[64:65, :] * (1.0 + vector(2))
    vec_v[1:2, :] = vector(0)
    vec_v[2:3, :] = vector(4)
    outs.append(copy(vec_v, vec_ref, sems.at[16]))
    outs[16].start()
    for c in outs:
        c.wait()


def rotated(x, cos, sin, swap):
    return x.astype(F32) * cos + dot(x, swap) * sin


def paired(a, b, low):
    turned_a, turned_b = pltpu.roll(a, 64, 1), pltpu.roll(b, 64, 1)
    return jnp.where(low, a, turned_b).astype(BF16), jnp.where(low, turned_a, b).astype(BF16)


def split_pair(q, low):
    zero = jnp.zeros_like(q)
    return [jnp.where(low, q, zero), jnp.where(low, zero, q)]


def identity():
    return (iota((256, 256), 0) == iota((256, 256), 1)).astype(F32).astype(BF16)


def local_kernel(
    sink_ref, vec_ref, lat_ref, one_ref, two_ref, wq_ref, wk_ref, wv_ref,
    rowc_ref, rows_ref, colc_ref, cols_ref,
    q_ref, o_ref, lse_ref,
    vec_v, lat_v, wq_v, wkv_v, hid_v, sems,
):
    place = place_of()
    odd = place & 1
    last = lax.axis_size("sp") * lax.axis_size("tp") - 1
    copy = pltpu.make_async_copy
    own = [
        copy(vec_ref, vec_v, sems.at[0]),
        copy(lat_ref, lat_v.at[pl.ds(128, 256)], sems.at[1]),
    ]
    halo = [
        copy(one_ref, lat_v.at[pl.ds((1 - odd) * 384, 128)], sems.at[2]),
        copy(two_ref, lat_v.at[pl.ds(odd * 384, 128)], sems.at[3]),
    ]
    weights = [
        copy(wk_ref, wkv_v.at[:, pl.ds(0, 256)], sems.at[4]),
        copy(wv_ref, wkv_v.at[:, pl.ds(256, 256)], sems.at[5]),
        copy(wq_ref.at[:, pl.ds(0, 512)], wq_v.at[0], sems.at[6]),
        copy(wq_ref.at[:, pl.ds(512, 512)], wq_v.at[1], sems.at[7]),
    ]
    for c in own + halo:
        c.start()
    swap = swap_matrix()
    cos = jnp.concatenate([colc_ref[...] + rowc_ref[r : r + 1, :] for r in range(8)], axis=0)
    sin = jnp.concatenate([cols_ref[...] + rows_ref[r : r + 1, :] for r in range(8)], axis=0)
    for c in own:
        c.wait()
    for c in weights:
        c.start()
    mult, shift = vec_v[0:1, :], vec_v[1:2, :]
    for r in (1, 2):
        rows = slice(r * 128, r * 128 + 128)
        hid_v[rows, :] = normed(lat_v[rows, :], mult, shift)
    for c in halo:
        c.wait()
    for r in (0, 3):
        rows = slice(r * 128, r * 128 + 128)
        hid_v[rows, :] = normed(lat_v[rows, :], mult, shift)
    for c in weights[:2]:
        c.wait()
    kv = dot(hid_v[...], wkv_v[...]).astype(BF16)
    keys = rotated(kv[:, 0:256], cos, sin, swap).astype(BF16)
    kt = dot_nt(identity(), keys).astype(BF16)
    ones = jnp.ones((512, 128), BF16)
    low_own = iota((256, 128), 1) < HEAD_DIM
    low = iota((128, 128), 1) < HEAD_DIM
    row, col = iota((128, 128), 0), iota((128, 128), 1)
    from_low = jnp.where(col >= row, 0.0, NEG_BIG)
    from_high = jnp.where(col <= row, 0.0, NEG_BIG)
    bias = (
        (from_low + jnp.where(place > 0, 0.0, NEG_BIG), from_high),
        (from_low, from_high + jnp.where(place < last, 0.0, NEG_BIG)),
    )
    for c in weights[2:]:
        c.wait()
    slabs = []
    for a in range(2):
        q = dot(hid_v[128:384, :], wq_v[a])
        plain, turned = [], []
        for h in range(2):
            part = q[:, h * 256 : h * 256 + 256]
            plain.append(part * FACTOR)
            part = part.astype(BF16)
            turned.append(rotated(part, cos[128:384], sin[128:384], swap) * FACTOR)
        for p in range(2):
            piece = slice(p * 128, p * 128 + 128)
            at = a * 512 + p * 256
            one, two = paired(plain[0][:, piece], plain[1][:, piece], low_own)
            q_ref[:, at : at + 128] = one
            q_ref[:, at + 128 : at + 256] = two
            slabs += paired(turned[0][:, piece], turned[1][:, piece], low_own)
    eighth = (iota((128, 128), 1) & 63) >> 3
    lse = [jnp.zeros((128, 128), F32) for _ in range(2)]
    for a in range(2):
        va = jnp.concatenate([kv[:, 256 + a * 128 : 384 + a * 128], ones], axis=1)
        for b in range(2):
            rows = slice(b * 128, b * 128 + 128)
            seen = slice(b * 128, b * 128 + 384)
            stacked = []
            for g in range(4):
                stacked += split_pair(slabs[a * 4 + g][rows], low)
            s = dot(jnp.concatenate(stacked, axis=0), kt[a * 128 : a * 128 + 128, seen])
            ps, ms = [], []
            for i in range(8):
                si = s[i * 128 : i * 128 + 128]
                s0, s1, s2 = si[:, 0:128] + bias[b][0], si[:, 128:256], si[:, 256:384] + bias[b][1]
                sink = sink_ref[(2 * a + i % 2) * 4 + i // 2] * LOG2E
                m = jnp.max(jnp.maximum(jnp.maximum(s0, s1), s2), axis=-1, keepdims=True)
                m = jnp.maximum(m, sink)
                p = [jnp.exp2(x - m).astype(BF16) for x in (s0, s1, s2)]
                ps.append(jnp.concatenate(p, axis=1))
                ms.append((jnp.broadcast_to(m, (128, 128)), sink))
            o = dot(jnp.concatenate(ps, axis=0), va[seen])
            for g in range(4):
                to = slice(a * 512 + g * 128, a * 512 + g * 128 + 128)
                x, y = o[g * 256 : g * 256 + 128], o[g * 256 + 128 : g * 256 + 256]
                (mx, sx), (my, sy) = ms[2 * g], ms[2 * g + 1]
                m = jnp.where(low, mx, my)
                l = jnp.where(low, x[:, 128:256], y[:, 128:256])
                l = l + jnp.exp2(jnp.where(low, sx, sy) - m)
                o_ref[rows, to] = jnp.where(low, x[:, 0:128], y[:, 0:128]) / l
                lse[b] = jnp.where(eighth == a * 4 + g, m + jnp.log2(l), lse[b])
    for b in range(2):
        lse_ref[b * 128 : b * 128 + 128, :] = lse[b]


def final_kernel(
    q_ref, kv_ref, o_ref, lse_ref, wo_ref, lat_ref, vec_ref, gain_ref, out_ref,
    wo_v, lat_v, vec_v, gain_v, mix_v, out_v, kt_v, va_v, even_v, odd_v, sems,
):
    copy = pltpu.make_async_copy
    pairs = [(lat_ref, lat_v), (vec_ref, vec_v), (gain_ref, gain_v)]
    for a in range(2):
        for g in range(4):
            for i in range(2):
                head = (2 * a + i) * 4 + g
                to = ((a * 4 + g) * 2 + i) * HEAD_DIM
                pairs.append((wo_ref.at[pl.ds(head * 64, 64)], wo_v.at[pl.ds(to, 64)]))
    ins = [copy(src, dst, sems.at[i]) for i, (src, dst) in enumerate(pairs)]
    for c in ins:
        c.start()
    low = iota((256, 128), 1) < HEAD_DIM
    eye = identity()
    for a in range(2):
        kt_v[a] = dot_nt(eye[a * 128 : a * 128 + 128], kv_ref[:, 0:256]).astype(BF16)
        va_v[a, :, 0:128] = kv_ref[:, 256 + a * 128 : 384 + a * 128]
        va_v[a, :, 128:256] = jnp.ones((1024, 128), BF16)

    def scores(i, s_ref):
        q = q_ref[:, pl.ds(pl.multiple_of(i * 128, 128), 128)]
        stacked = jnp.concatenate(split_pair(q, low), axis=0)
        s_ref[...] = dot(stacked, kt_v[i // 4])

    def attend(i, s_ref):
        s = s_ref[...]
        m = jnp.max(s, axis=-1, keepdims=True)
        o = dot(jnp.exp2(s - m).astype(BF16), va_v[i // 4])
        m = jnp.broadcast_to(m, (512, 128))
        mc = jnp.where(low, m[0:256], m[256:512])
        oc = jnp.where(low, o[0:256, 0:128], o[256:512, 0:128])
        lc = jnp.where(low, o[0:256, 128:256], o[256:512, 128:256])
        at = pl.ds(pl.multiple_of(i * 128, 128), 128)
        lse = pltpu.roll(lse_ref[...], (128 - 8 * i) & 127, 1)
        here = [jnp.broadcast_to(lse[:, c : c + 1], (256, 128)) for c in (0, 64)]
        ml = jnp.where(low, here[0], here[1])
        top = jnp.maximum(ml, mc)
        wl, wc = jnp.exp2(ml - top), jnp.exp2(mc - top)
        mix_v[:, at] = ((wl * o_ref[:, at] + wc * oc) / (wl + wc * lc)).astype(BF16)

    scores(0, even_v)

    def two(j, carry):
        i = 2 * j
        scores(i + 1, odd_v)
        attend(i, even_v)
        scores(i + 2, even_v)
        attend(i + 1, odd_v)
        return carry

    lax.fori_loop(0, 3, two, 0)
    for c in ins:
        c.wait()
    scores(7, odd_v)
    attend(6, even_v)
    attend(7, odd_v)
    scale = vec_v[2:3, :] * gain_v[...]
    outs = []
    for b in range(2):
        rows = slice(b * 128, b * 128 + 128)
        projected = dot(mix_v[rows, :], wo_v[...])
        rs = lax.rsqrt(jnp.mean(projected * projected, axis=-1, keepdims=True) + EPSILON)
        out_v[rows, :] = (lat_v[rows, :].astype(F32) + projected * rs * scale).astype(BF16)
        there = pl.ds(b * 128, 128)
        outs.append(copy(out_v.at[there], out_ref.at[there], sems.at[len(ins) + b]))
        outs[b].start()
    for c in outs:
        c.wait()


KINDS = {"v": VM, "V": VM, "h": HB, "s": SM}
FIXED = {"V": VM, "h": HB}


def spec(kinds):
    return [pl.BlockSpec(memory_space=KINDS[k]) for k in kinds]


def call(kernel, name, ins, outs, scratch, copies, args, flops, limit):
    return pl.pallas_call(
        kernel,
        out_shape=[FIXED.get(k, jax.ShapeDtypeStruct)(s, d) for k, s, d in outs],
        in_specs=spec(ins),
        out_specs=spec([k for k, _, _ in outs]),
        scratch_shapes=[pltpu.VMEM(s, d) for s, d in scratch]
        + [pltpu.SemaphoreType.DMA((copies,))],
        compiler_params=pltpu.CompilerParams(vmem_limit_bytes=limit * 1024 * 1024),
        cost_estimate=pl.CostEstimate(flops=flops, bytes_accessed=0, transcendentals=0),
        name=name,
    )(
        *[
            pltpu.with_memory_space_constraint(x, FIXED[k]) if k in FIXED else x
            for k, x in zip(ins, args)
        ]
    )


def shards(
    latent, cond, ctx_rows, ctx_cond, mod_weight, norm_gain, out_gain,
    w_query, w_key, w_value, w_out, sink,
):
    sp_size = lax.axis_size("sp")
    count = sp_size * lax.axis_size("tp")
    both = ("sp", "tp")
    rows, width = latent.shape
    half = (WINDOW, width)
    wide = (rows, 1024)
    rest = (8, width)
    line = (1, width)
    square = (16, 128)
    small = w_key.shape

    parts, one, two = call(
        entry_kernel,
        "entry",
        "hhhh",
        [("h", (count, 8, 384), BF16), ("h", half, BF16), ("h", half, BF16)],
        [
            (square, BF16),
            (square, BF16),
            (mod_weight.shape, BF16),
            (latent.shape, BF16),
            ((count, 8, 384), BF16),
        ],
        7,
        (cond.reshape(square), ctx_cond.reshape(square), mod_weight, latent),
        10**6,
        8,
    )
    ng, wk_near, wv_near = call(
        prep_kernel,
        "prep",
        "hhhhh",
        [("V", (72, width), F32), ("V", small, BF16), ("V", small, BF16)],
        [(ctx_rows.shape, BF16), (line, F32)],
        4,
        (one, ctx_rows, norm_gain.reshape(line), w_key, w_value),
        2 * 10**9,
        4,
    )
    recv = lax.all_to_all(parts, both, 0, 0, tiled=True)
    swap_one = [(i, i ^ 1) for i in range(count)]
    swap_two = [(i, i + 1 if i % 2 else i - 1) for i in range(1, count - 1)]
    one = lax.ppermute(one, both, swap_one)
    two = lax.ppermute(two, both, swap_two)
    send, vecs = call(
        context_kernel,
        "context",
        "vVVV",
        [("h", (sp_size, 64, 512), BF16), ("h", rest, F32)],
        [((64, 512), BF16), (rest, F32)],
        17,
        (recv, ng, wk_near, wv_near),
        10**6,
        6,
    )
    kv_ctx = lax.all_to_all(send, "sp", 0, 0, tiled=True).reshape(sp_size * 64, 512)

    lanes = np.arange(256) % 32
    freq = 10000.0 ** (-(lanes % 16) / 16.0)
    by_row = (lanes < 16).astype(np.float32)
    angle = np.arange(GRID_W)[:, None] * freq
    colc = jnp.asarray(np.cos(angle) * (1.0 - by_row), F32)
    cols = jnp.asarray(np.sin(angle) * (1.0 - by_row), F32)
    grid_row = place_of() * (rows // GRID_W) - WINDOW // GRID_W + jnp.arange(8, dtype=jnp.int32)
    angle = grid_row.astype(F32)[:, None] * jnp.asarray(freq, F32)[None, :]
    tables = (jnp.cos(angle) * by_row, jnp.sin(angle) * by_row, colc, cols)

    query, o, lse = call(
        local_kernel,
        "local",
        "shhhhhhhvvvv",
        [("V", wide, BF16), ("V", wide, F32), ("V", (rows, 128), F32)],
        [
            (rest, F32),
            ((2 * rows, width), BF16),
            ((2, width, 512), BF16),
            ((width, 512), BF16),
            ((2 * rows, width), BF16),
        ],
        8,
        (sink, vecs, latent, one, two, w_query, w_key, w_value, *tables),
        10**10,
        26,
    )
    (updated,) = call(
        final_kernel,
        "final",
        "VVVVhhhh",
        [("h", latent.shape, BF16)],
        [
            (w_out.shape, BF16),
            (latent.shape, BF16),
            (rest, F32),
            (line, F32),
            (wide, BF16),
            (latent.shape, BF16),
            ((2, 128, 1024), BF16),
            ((2, 1024, 256), BF16),
            ((512, 1024), F32),
            ((512, 1024), F32),
        ],
        21,
        (query, kv_ctx, o, lse, w_out, latent, vecs, out_gain.reshape(line)),
        10**10,
        28,
    )
    return updated


def solution(mesh):
    placed = (
        P(("dp", "sp", "tp"), None),
        P("dp"),
        P(("dp", "sp"), None),
        P(),
        P(None, "sp", "tp"),
        P(),
        P(),
        P(),
        P(),
        P(),
        P(),
        P(),
    )
    return jax.shard_map(
        shards, mesh=mesh, in_specs=placed, out_specs=P(("dp", "sp", "tp"), None), check_vma=False
    )
```

```python
import jax
import numpy as np
import jax.numpy as jnp
from jax import lax
from jax.experimental import pallas as pl
from jax.experimental.pallas import tpu as pltpu
from jax.sharding import PartitionSpec as P

HEAD_DIM = 64
WINDOW = 128
GRID_W = 64
EPSILON = 1e-06
NEG_BIG = -1e30
LOG2E = 1.4426950408889634
FACTOR = HEAD_DIM**-0.5 * LOG2E
F32 = jnp.float32
BF16 = jnp.bfloat16
VM = pltpu.MemorySpace.VMEM
HB = pltpu.MemorySpace.HBM
SM = pltpu.MemorySpace.SMEM


def place_of():
    return lax.axis_index("sp") * lax.axis_size("tp") + lax.axis_index("tp")


def dot(a, b):
    return jnp.dot(a, b, preferred_element_type=F32)


def dot_nt(a, b):
    return lax.dot_general(a, b, (((1,), (1,)), ((), ())), preferred_element_type=F32)


def iota(shape, dim):
    return lax.broadcasted_iota(jnp.int32, shape, dim)


def swap_matrix():
    k, c = iota((256, 256), 0), iota((256, 256), 1)
    low = (c & 63) < 32
    neg = jnp.where(low & (k == c + 32), -1.0, 0.0)
    pos = jnp.where((~low) & (k == c - 32), 1.0, 0.0)
    return (neg + pos).astype(BF16)


def normed(x, mult, shift):
    x = x.astype(F32)
    rs = lax.rsqrt(jnp.mean(x * x, axis=-1, keepdims=True) + EPSILON)
    return (x * rs * mult + shift).astype(BF16)


def entry_kernel(
    cond_ref, cctx_ref, mod_ref, lat_ref,
    parts_ref, one_ref, two_ref,
    cond_v, cctx_v, mod_v, lat_v, block_v, sems,
):
    sp = lax.axis_index("sp")
    odd = place_of() & 1
    copy = pltpu.make_async_copy
    pairs = ((mod_ref, mod_v), (cond_ref, cond_v), (cctx_ref, cctx_v), (lat_ref, lat_v))
    ins = [copy(src, dst, sems.at[i]) for i, (src, dst) in enumerate(pairs)]
    for c in ins:
        c.start()
    ins[1].wait()
    ins[2].wait()
    here = iota((16, 128), 0) == sp
    rows = []
    for ref in (cond_v, cctx_v):
        x = jnp.sum(jnp.where(here, ref[...].astype(F32), 0.0), axis=0, keepdims=True)
        rows.append(x / (1.0 + jnp.exp(-x)))
    v = jnp.concatenate(rows + [jnp.zeros((6, 128), F32)], axis=0).astype(BF16)
    ins[0].wait()
    parts = [dot(v, mod_v[i]) for i in range(3)]
    five = (parts[0][0:1], parts[0][1:2], parts[1][0:1], parts[1][1:2], parts[2][0:1])
    zero = jnp.zeros((1, 128), F32)
    rows = []
    for j in range(4):
        cut = [x[:, j * 128 : (j + 1) * 128] for x in five]
        rows.append(jnp.concatenate(cut[:3], axis=1))
        rows.append(jnp.concatenate(cut[3:] + [zero], axis=1))
    block = jnp.concatenate(rows, axis=0).astype(BF16)
    for i in range(block_v.shape[0]):
        block_v[i] = block
    outs = [
        copy(block_v, parts_ref, sems.at[4]),
        copy(lat_v.at[pl.ds((1 - odd) * 128, 128)], one_ref, sems.at[5]),
        copy(lat_v.at[pl.ds(odd * 128, 128)], two_ref, sems.at[6]),
    ]
    outs[0].start()
    ins[3].wait()
    outs[1].start()
    outs[2].start()
    for c in outs:
        c.wait()


def prep_kernel(
    after_ref, ctx_ref, gain_ref, wk_ref, wv_ref, ng_ref, wk_out, wv_out, ctx_v, gain_v, sems
):
    copy = pltpu.make_async_copy
    pairs = ((ctx_ref, ctx_v), (gain_ref, gain_v), (wk_ref, wk_out), (wv_ref, wv_out))
    ins = [copy(src, dst, sems.at[i]) for i, (src, dst) in enumerate(pairs)]
    for c in ins:
        c.start()
    ins[0].wait()
    ins[1].wait()
    x = ctx_v[...].astype(F32)
    gain = gain_v[...]
    rs = lax.rsqrt(jnp.mean(x * x, axis=-1, keepdims=True) + EPSILON)
    ng_ref[0:64, :] = x * rs * gain
    ng_ref[64:72, :] = jnp.broadcast_to(gain, (8, 2048))
    for c in ins[2:]:
        c.wait()


def context_kernel(recv_ref, ng_ref, wk_ref, wv_ref, send_ref, vec_ref, kv_v, vec_v, sems):
    sums = []
    for t in range(4):
        acc = recv_ref[t].astype(F32)
        for s in range(1, 16):
            acc = acc + recv_ref[s * 4 + t].astype(F32)
        sums.append(acc)

    def vector(v):
        cuts = []
        for t in range(4):
            for j in range(4):
                r, c = 2 * j + v // 3, (v % 3) * 128
                cuts.append(sums[t][r : r + 1, c : c + 128])
        return jnp.concatenate(cuts, axis=1)

    hidden = (ng_ref[0:64, :] * (1.0 + vector(3)) + vector(1)).astype(BF16)
    kv_v[:, 0:256] = dot(hidden, wk_ref[...]).astype(BF16)
    kv_v[:, 256:512] = dot(hidden, wv_ref[...]).astype(BF16)
    copy = pltpu.make_async_copy
    outs = [copy(kv_v, send_ref.at[i], sems.at[i]) for i in range(16)]
    for c in outs:
        c.start()
    vec_v[...] = jnp.zeros((8, 2048), F32)
    vec_v[0:1, :] = ng_ref[64:65, :] * (1.0 + vector(2))
    vec_v[1:2, :] = vector(0)
    vec_v[2:3, :] = vector(4)
    outs.append(copy(vec_v, vec_ref, sems.at[16]))
    outs[16].start()
    for c in outs:
        c.wait()


def rotated(x, cos, sin, swap):
    return x.astype(F32) * cos + dot(x, swap) * sin


def paired(a, b, low):
    turned_a, turned_b = pltpu.roll(a, 64, 1), pltpu.roll(b, 64, 1)
    return jnp.where(low, a, turned_b).astype(BF16), jnp.where(low, turned_a, b).astype(BF16)


def split_pair(q, low):
    zero = jnp.zeros_like(q)
    return [jnp.where(low, q, zero), jnp.where(low, zero, q)]


def identity():
    return (iota((256, 256), 0) == iota((256, 256), 1)).astype(F32).astype(BF16)


def local_kernel(
    sink_ref, vec_ref, lat_ref, one_ref, two_ref, wq_ref, wk_ref, wv_ref,
    rowc_ref, rows_ref, colc_ref, cols_ref,
    q_ref, o_ref, lse_ref,
    vec_v, lat_v, wq_v, wkv_v, hid_v, sems,
):
    place = place_of()
    odd = place & 1
    last = lax.axis_size("sp") * lax.axis_size("tp") - 1
    copy = pltpu.make_async_copy
    own = [
        copy(vec_ref, vec_v, sems.at[0]),
        copy(lat_ref, lat_v.at[pl.ds(128, 256)], sems.at[1]),
    ]
    halo = [
        copy(one_ref, lat_v.at[pl.ds((1 - odd) * 384, 128)], sems.at[2]),
        copy(two_ref, lat_v.at[pl.ds(odd * 384, 128)], sems.at[3]),
    ]
    weights = [
        copy(wk_ref, wkv_v.at[:, pl.ds(0, 256)], sems.at[4]),
        copy(wv_ref, wkv_v.at[:, pl.ds(256, 256)], sems.at[5]),
        copy(wq_ref.at[:, pl.ds(0, 512)], wq_v.at[0], sems.at[6]),
        copy(wq_ref.at[:, pl.ds(512, 512)], wq_v.at[1], sems.at[7]),
    ]
    for c in own + halo:
        c.start()
    swap = swap_matrix()
    cos = jnp.concatenate([colc_ref[...] + rowc_ref[r : r + 1, :] for r in range(8)], axis=0)
    sin = jnp.concatenate([cols_ref[...] + rows_ref[r : r + 1, :] for r in range(8)], axis=0)
    for c in own:
        c.wait()
    for c in weights:
        c.start()
    mult, shift = vec_v[0:1, :], vec_v[1:2, :]
    for r in (1, 2):
        rows = slice(r * 128, r * 128 + 128)
        hid_v[rows, :] = normed(lat_v[rows, :], mult, shift)
    for c in halo:
        c.wait()
    for r in (0, 3):
        rows = slice(r * 128, r * 128 + 128)
        hid_v[rows, :] = normed(lat_v[rows, :], mult, shift)
    for c in weights[:2]:
        c.wait()
    kv = dot(hid_v[...], wkv_v[...]).astype(BF16)
    keys = rotated(kv[:, 0:256], cos, sin, swap).astype(BF16)
    kt = dot_nt(identity(), keys).astype(BF16)
    ones = jnp.ones((512, 128), BF16)
    low_own = iota((256, 128), 1) < HEAD_DIM
    low = iota((128, 128), 1) < HEAD_DIM
    row, col = iota((128, 128), 0), iota((128, 128), 1)
    from_low = jnp.where(col >= row, 0.0, NEG_BIG)
    from_high = jnp.where(col <= row, 0.0, NEG_BIG)
    bias = (
        (from_low + jnp.where(place > 0, 0.0, NEG_BIG), from_high),
        (from_low, from_high + jnp.where(place < last, 0.0, NEG_BIG)),
    )
    for c in weights[2:]:
        c.wait()
    slabs = []
    for a in range(2):
        q = dot(hid_v[128:384, :], wq_v[a])
        plain, turned = [], []
        for h in range(2):
            part = q[:, h * 256 : h * 256 + 256]
            plain.append(part * FACTOR)
            part = part.astype(BF16)
            turned.append(rotated(part, cos[128:384], sin[128:384], swap) * FACTOR)
        for p in range(2):
            piece = slice(p * 128, p * 128 + 128)
            at = a * 512 + p * 256
            one, two = paired(plain[0][:, piece], plain[1][:, piece], low_own)
            q_ref[:, at : at + 128] = one
            q_ref[:, at + 128 : at + 256] = two
            slabs += paired(turned[0][:, piece], turned[1][:, piece], low_own)
    eighth = (iota((128, 128), 1) & 63) >> 3
    lse = [jnp.zeros((128, 128), F32) for _ in range(2)]
    for a in range(2):
        va = jnp.concatenate([kv[:, 256 + a * 128 : 384 + a * 128], ones], axis=1)
        for b in range(2):
            rows = slice(b * 128, b * 128 + 128)
            seen = slice(b * 128, b * 128 + 384)
            stacked = []
            for g in range(4):
                stacked += split_pair(slabs[a * 4 + g][rows], low)
            s = dot(jnp.concatenate(stacked, axis=0), kt[a * 128 : a * 128 + 128, seen])
            ps, ms = [], []
            for i in range(8):
                si = s[i * 128 : i * 128 + 128]
                s0, s1, s2 = si[:, 0:128] + bias[b][0], si[:, 128:256], si[:, 256:384] + bias[b][1]
                sink = sink_ref[(2 * a + i % 2) * 4 + i // 2] * LOG2E
                m = jnp.max(jnp.maximum(jnp.maximum(s0, s1), s2), axis=-1, keepdims=True)
                m = jnp.maximum(m, sink)
                p = [jnp.exp2(x - m).astype(BF16) for x in (s0, s1, s2)]
                ps.append(jnp.concatenate(p, axis=1))
                ms.append((jnp.broadcast_to(m, (128, 128)), sink))
            o = dot(jnp.concatenate(ps, axis=0), va[seen])
            for g in range(4):
                to = slice(a * 512 + g * 128, a * 512 + g * 128 + 128)
                x, y = o[g * 256 : g * 256 + 128], o[g * 256 + 128 : g * 256 + 256]
                (mx, sx), (my, sy) = ms[2 * g], ms[2 * g + 1]
                m = jnp.where(low, mx, my)
                l = jnp.where(low, x[:, 128:256], y[:, 128:256])
                l = l + jnp.exp2(jnp.where(low, sx, sy) - m)
                o_ref[rows, to] = jnp.where(low, x[:, 0:128], y[:, 0:128]) / l
                lse[b] = jnp.where(eighth == a * 4 + g, m + jnp.log2(l), lse[b])
    for b in range(2):
        lse_ref[b * 128 : b * 128 + 128, :] = lse[b]


def final_kernel(
    q_ref, kv_ref, o_ref, lse_ref, wo_ref, lat_ref, vec_ref, gain_ref, out_ref,
    wo_v, lat_v, vec_v, gain_v, mix_v, out_v, kt_v, va_v, even_v, odd_v, sems,
):
    copy = pltpu.make_async_copy
    pairs = [(lat_ref, lat_v), (vec_ref, vec_v), (gain_ref, gain_v)]
    for a in range(2):
        for g in range(4):
            for i in range(2):
                head = (2 * a + i) * 4 + g
                to = ((a * 4 + g) * 2 + i) * HEAD_DIM
                pairs.append((wo_ref.at[pl.ds(head * 64, 64)], wo_v.at[pl.ds(to, 64)]))
    ins = [copy(src, dst, sems.at[i]) for i, (src, dst) in enumerate(pairs)]
    for c in ins:
        c.start()
    low = iota((256, 128), 1) < HEAD_DIM
    eye = identity()
    keys = dot_nt(eye, kv_ref[:, 0:256]).astype(BF16)
    for a in range(2):
        kt_v[a] = keys[a * 128 : a * 128 + 128]
        va_v[a, :, 0:128] = kv_ref[:, 256 + a * 128 : 384 + a * 128]
        va_v[a, :, 128:256] = jnp.ones((1024, 128), BF16)

    def scores(i, s_ref):
        q = q_ref[:, pl.ds(pl.multiple_of(i * 128, 128), 128)]
        stacked = jnp.concatenate(split_pair(q, low), axis=0)
        s_ref[...] = dot(stacked, kt_v[i // 4])

    def attend(i, s_ref):
        s = s_ref[...]
        m = jnp.max(s, axis=-1, keepdims=True)
        o = dot(jnp.exp2(s - m).astype(BF16), va_v[i // 4])
        m = jnp.broadcast_to(m, (512, 128))
        mc = jnp.where(low, m[0:256], m[256:512])
        oc = jnp.where(low, o[0:256, 0:128], o[256:512, 0:128])
        lc = jnp.where(low, o[0:256, 128:256], o[256:512, 128:256])
        at = pl.ds(pl.multiple_of(i * 128, 128), 128)
        lse = pltpu.roll(lse_ref[...], (128 - 8 * i) & 127, 1)
        here = [jnp.broadcast_to(lse[:, c : c + 1], (256, 128)) for c in (0, 64)]
        ml = jnp.where(low, here[0], here[1])
        top = jnp.maximum(ml, mc)
        wl, wc = jnp.exp2(ml - top), jnp.exp2(mc - top)
        mix_v[:, at] = ((wl * o_ref[:, at] + wc * oc) / (wl + wc * lc)).astype(BF16)

    scores(0, even_v)

    def two(j, carry):
        i = 2 * j
        scores(i + 1, odd_v)
        attend(i, even_v)
        scores(i + 2, even_v)
        attend(i + 1, odd_v)
        return carry

    lax.fori_loop(0, 3, two, 0)
    for c in ins:
        c.wait()
    scores(7, odd_v)
    part = dot(mix_v[:, 0:768], wo_v[0:768])
    attend(6, even_v)
    attend(7, odd_v)
    scale = vec_v[2:3, :] * gain_v[...]
    outs = []
    for b in range(2):
        rows = slice(b * 128, b * 128 + 128)
        projected = part[rows] + dot(mix_v[rows, 768:1024], wo_v[768:1024])
        rs = lax.rsqrt(jnp.mean(projected * projected, axis=-1, keepdims=True) + EPSILON)
        out_v[rows, :] = (lat_v[rows, :].astype(F32) + projected * rs * scale).astype(BF16)
        there = pl.ds(b * 128, 128)
        outs.append(copy(out_v.at[there], out_ref.at[there], sems.at[len(ins) + b]))
        outs[b].start()
    for c in outs:
        c.wait()


KINDS = {"v": VM, "V": VM, "h": HB, "s": SM}
FIXED = {"V": VM, "h": HB}


def spec(kinds):
    return [pl.BlockSpec(memory_space=KINDS[k]) for k in kinds]


def call(kernel, name, ins, outs, scratch, copies, args, flops, limit):
    return pl.pallas_call(
        kernel,
        out_shape=[FIXED.get(k, jax.ShapeDtypeStruct)(s, d) for k, s, d in outs],
        in_specs=spec(ins),
        out_specs=spec([k for k, _, _ in outs]),
        scratch_shapes=[pltpu.VMEM(s, d) for s, d in scratch]
        + [pltpu.SemaphoreType.DMA((copies,))],
        compiler_params=pltpu.CompilerParams(vmem_limit_bytes=limit * 1024 * 1024),
        cost_estimate=pl.CostEstimate(flops=flops, bytes_accessed=0, transcendentals=0),
        name=name,
    )(
        *[
            pltpu.with_memory_space_constraint(x, FIXED[k]) if k in FIXED else x
            for k, x in zip(ins, args)
        ]
    )


def shards(
    latent, cond, ctx_rows, ctx_cond, mod_weight, norm_gain, out_gain,
    w_query, w_key, w_value, w_out, sink,
):
    sp_size = lax.axis_size("sp")
    count = sp_size * lax.axis_size("tp")
    both = ("sp", "tp")
    rows, width = latent.shape
    half = (WINDOW, width)
    wide = (rows, 1024)
    rest = (8, width)
    line = (1, width)
    square = (16, 128)
    small = w_key.shape

    parts, one, two = call(
        entry_kernel,
        "entry",
        "hhhh",
        [("h", (count, 8, 384), BF16), ("h", half, BF16), ("h", half, BF16)],
        [
            (square, BF16),
            (square, BF16),
            (mod_weight.shape, BF16),
            (latent.shape, BF16),
            ((count, 8, 384), BF16),
        ],
        7,
        (cond.reshape(square), ctx_cond.reshape(square), mod_weight, latent),
        10**6,
        8,
    )
    ng, wk_near, wv_near = call(
        prep_kernel,
        "prep",
        "hhhhh",
        [("V", (72, width), F32), ("V", small, BF16), ("V", small, BF16)],
        [(ctx_rows.shape, BF16), (line, F32)],
        4,
        (one, ctx_rows, norm_gain.reshape(line), w_key, w_value),
        2 * 10**9,
        4,
    )
    recv = lax.all_to_all(parts, both, 0, 0, tiled=True)
    swap_one = [(i, i ^ 1) for i in range(count)]
    swap_two = [(i, i + 1 if i % 2 else i - 1) for i in range(1, count - 1)]
    one = lax.ppermute(one, both, swap_one)
    two = lax.ppermute(two, both, swap_two)
    send, vecs = call(
        context_kernel,
        "context",
        "vVVV",
        [("h", (sp_size, 64, 512), BF16), ("h", rest, F32)],
        [((64, 512), BF16), (rest, F32)],
        17,
        (recv, ng, wk_near, wv_near),
        10**6,
        6,
    )
    kv_ctx = lax.all_to_all(send, "sp", 0, 0, tiled=True).reshape(sp_size * 64, 512)

    lanes = np.arange(256) % 32
    freq = 10000.0 ** (-(lanes % 16) / 16.0)
    by_row = (lanes < 16).astype(np.float32)
    angle = np.arange(GRID_W)[:, None] * freq
    colc = jnp.asarray(np.cos(angle) * (1.0 - by_row), F32)
    cols = jnp.asarray(np.sin(angle) * (1.0 - by_row), F32)
    grid_row = place_of() * (rows // GRID_W) - WINDOW // GRID_W + jnp.arange(8, dtype=jnp.int32)
    angle = grid_row.astype(F32)[:, None] * jnp.asarray(freq, F32)[None, :]
    tables = (jnp.cos(angle) * by_row, jnp.sin(angle) * by_row, colc, cols)

    query, o, lse = call(
        local_kernel,
        "local",
        "shhhhhhhvvvv",
        [("V", wide, BF16), ("V", wide, F32), ("V", (rows, 128), F32)],
        [
            (rest, F32),
            ((2 * rows, width), BF16),
            ((2, width, 512), BF16),
            ((width, 512), BF16),
            ((2 * rows, width), BF16),
        ],
        8,
        (sink, vecs, latent, one, two, w_query, w_key, w_value, *tables),
        10**10,
        26,
    )
    (updated,) = call(
        final_kernel,
        "final",
        "VVVVhhhh",
        [("h", latent.shape, BF16)],
        [
            (w_out.shape, BF16),
            (latent.shape, BF16),
            (rest, F32),
            (line, F32),
            (wide, BF16),
            (latent.shape, BF16),
            ((2, 128, 1024), BF16),
            ((2, 1024, 256), BF16),
            ((512, 1024), F32),
            ((512, 1024), F32),
        ],
        21,
        (query, kv_ctx, o, lse, w_out, latent, vecs, out_gain.reshape(line)),
        10**10,
        28,
    )
    return updated


def solution(mesh):
    placed = (
        P(("dp", "sp", "tp"), None),
        P("dp"),
        P(("dp", "sp"), None),
        P(),
        P(None, "sp", "tp"),
        P(),
        P(),
        P(),
        P(),
        P(),
        P(),
        P(),
    )
    return jax.shard_map(
        shards, mesh=mesh, in_specs=placed, out_specs=P(("dp", "sp", "tp"), None), check_vma=False
    )
```

```python
import jax
import numpy as np
import jax.numpy as jnp
from jax import lax
from jax.experimental import pallas as pl
from jax.experimental.pallas import tpu as pltpu
from jax.sharding import PartitionSpec as P

HEAD_DIM = 64
WINDOW = 128
GRID_W = 64
EPSILON = 1e-06
NEG_BIG = -1e30
LOG2E = 1.4426950408889634
FACTOR = HEAD_DIM**-0.5 * LOG2E
F32 = jnp.float32
BF16 = jnp.bfloat16
VM = pltpu.MemorySpace.VMEM
HB = pltpu.MemorySpace.HBM
SM = pltpu.MemorySpace.SMEM


def place_of():
    return lax.axis_index("sp") * lax.axis_size("tp") + lax.axis_index("tp")


def dot(a, b):
    return jnp.dot(a, b, preferred_element_type=F32)


def dot_nt(a, b):
    return lax.dot_general(a, b, (((1,), (1,)), ((), ())), preferred_element_type=F32)


def iota(shape, dim):
    return lax.broadcasted_iota(jnp.int32, shape, dim)


def swap_matrix():
    k, c = iota((256, 256), 0), iota((256, 256), 1)
    low = (c & 63) < 32
    neg = jnp.where(low & (k == c + 32), -1.0, 0.0)
    pos = jnp.where((~low) & (k == c - 32), 1.0, 0.0)
    return (neg + pos).astype(BF16)


def normed(x, mult, shift):
    x = x.astype(F32)
    rs = lax.rsqrt(jnp.mean(x * x, axis=-1, keepdims=True) + EPSILON)
    return (x * rs * mult + shift).astype(BF16)


def entry_kernel(
    cond_ref, cctx_ref, mod_ref, lat_ref,
    parts_ref, one_ref, two_ref,
    cond_v, cctx_v, mod_v, lat_v, block_v, sems,
):
    sp = lax.axis_index("sp")
    odd = place_of() & 1
    copy = pltpu.make_async_copy
    pairs = ((mod_ref, mod_v), (cond_ref, cond_v), (cctx_ref, cctx_v), (lat_ref, lat_v))
    ins = [copy(src, dst, sems.at[i]) for i, (src, dst) in enumerate(pairs)]
    for c in ins:
        c.start()
    ins[1].wait()
    ins[2].wait()
    here = iota((16, 128), 0) == sp
    rows = []
    for ref in (cond_v, cctx_v):
        x = jnp.sum(jnp.where(here, ref[...].astype(F32), 0.0), axis=0, keepdims=True)
        rows.append(x / (1.0 + jnp.exp(-x)))
    v = jnp.concatenate(rows + [jnp.zeros((6, 128), F32)], axis=0).astype(BF16)
    ins[0].wait()
    parts = [dot(v, mod_v[i]) for i in range(3)]
    five = (parts[0][0:1], parts[0][1:2], parts[1][0:1], parts[1][1:2], parts[2][0:1])
    rows = []
    for j in range(4):
        exact = jnp.concatenate([x[:, j * 128 : (j + 1) * 128] for x in five], axis=1)
        high = exact.astype(BF16).astype(F32)
        rows += [high, exact - high]
    block = jnp.concatenate(rows, axis=0).astype(BF16)
    for i in range(block_v.shape[0]):
        block_v[i] = block
    outs = [
        copy(block_v, parts_ref, sems.at[4]),
        copy(lat_v.at[pl.ds((1 - odd) * 128, 128)], one_ref, sems.at[5]),
        copy(lat_v.at[pl.ds(odd * 128, 128)], two_ref, sems.at[6]),
    ]
    outs[0].start()
    ins[3].wait()
    outs[1].start()
    outs[2].start()
    for c in outs:
        c.wait()


def prep_kernel(
    after_ref, ctx_ref, gain_ref, wk_ref, wv_ref, ng_ref, wk_out, wv_out, ctx_v, gain_v, sems
):
    copy = pltpu.make_async_copy
    pairs = ((ctx_ref, ctx_v), (gain_ref, gain_v), (wk_ref, wk_out), (wv_ref, wv_out))
    ins = [copy(src, dst, sems.at[i]) for i, (src, dst) in enumerate(pairs)]
    for c in ins:
        c.start()
    ins[0].wait()
    ins[1].wait()
    x = ctx_v[...].astype(F32)
    gain = gain_v[...]
    rs = lax.rsqrt(jnp.mean(x * x, axis=-1, keepdims=True) + EPSILON)
    ng_ref[0:64, :] = x * rs * gain
    ng_ref[64:72, :] = jnp.broadcast_to(gain, (8, 2048))
    for c in ins[2:]:
        c.wait()


def context_kernel(recv_ref, ng_ref, wk_ref, wv_ref, send_ref, vec_ref, kv_v, vec_v, sems):
    sums = []
    for t in range(4):
        acc = recv_ref[t].astype(F32)
        for s in range(1, 16):
            acc = acc + recv_ref[s * 4 + t].astype(F32)
        sums.append(acc)

    def vector(v):
        cuts = []
        for t in range(4):
            for j in range(4):
                both = sums[t][2 * j : 2 * j + 2, v * 128 : v * 128 + 128]
                cuts.append(both[0:1] + both[1:2])
        return jnp.concatenate(cuts, axis=1)

    hidden = (ng_ref[0:64, :] * (1.0 + vector(3)) + vector(1)).astype(BF16)
    kv_v[:, 0:256] = dot(hidden, wk_ref[...]).astype(BF16)
    kv_v[:, 256:512] = dot(hidden, wv_ref[...]).astype(BF16)
    copy = pltpu.make_async_copy
    outs = [copy(kv_v, send_ref.at[i], sems.at[i]) for i in range(16)]
    for c in outs:
        c.start()
    vec_v[...] = jnp.zeros((8, 2048), F32)
    vec_v[0:1, :] = ng_ref[64:65, :] * (1.0 + vector(2))
    vec_v[1:2, :] = vector(0)
    vec_v[2:3, :] = vector(4)
    outs.append(copy(vec_v, vec_ref, sems.at[16]))
    outs[16].start()
    for c in outs:
        c.wait()


def rotated(x, cos, sin, swap):
    return x.astype(F32) * cos + dot(x, swap) * sin


def paired(a, b, low):
    turned_a, turned_b = pltpu.roll(a, 64, 1), pltpu.roll(b, 64, 1)
    return jnp.where(low, a, turned_b).astype(BF16), jnp.where(low, turned_a, b).astype(BF16)


def split_pair(q, low):
    zero = jnp.zeros_like(q)
    return [jnp.where(low, q, zero), jnp.where(low, zero, q)]


def identity():
    return (iota((256, 256), 0) == iota((256, 256), 1)).astype(F32).astype(BF16)


def local_kernel(
    sink_ref, vec_ref, lat_ref, one_ref, two_ref, wq_ref, wk_ref, wv_ref,
    rowc_ref, rows_ref, colc_ref, cols_ref,
    q_ref, o_ref, lse_ref,
    vec_v, lat_v, wq_v, wkv_v, hid_v, sems,
):
    place = place_of()
    odd = place & 1
    last = lax.axis_size("sp") * lax.axis_size("tp") - 1
    copy = pltpu.make_async_copy
    own = [
        copy(vec_ref, vec_v, sems.at[0]),
        copy(lat_ref, lat_v.at[pl.ds(128, 256)], sems.at[1]),
    ]
    halo = [
        copy(one_ref, lat_v.at[pl.ds((1 - odd) * 384, 128)], sems.at[2]),
        copy(two_ref, lat_v.at[pl.ds(odd * 384, 128)], sems.at[3]),
    ]
    weights = [
        copy(wk_ref, wkv_v.at[:, pl.ds(0, 256)], sems.at[4]),
        copy(wv_ref, wkv_v.at[:, pl.ds(256, 256)], sems.at[5]),
        copy(wq_ref.at[:, pl.ds(0, 512)], wq_v.at[0], sems.at[6]),
        copy(wq_ref.at[:, pl.ds(512, 512)], wq_v.at[1], sems.at[7]),
    ]
    for c in own + halo:
        c.start()
    swap = swap_matrix()
    cos = jnp.concatenate([colc_ref[...] + rowc_ref[r : r + 1, :] for r in range(8)], axis=0)
    sin = jnp.concatenate([cols_ref[...] + rows_ref[r : r + 1, :] for r in range(8)], axis=0)
    for c in own:
        c.wait()
    for c in weights:
        c.start()
    mult, shift = vec_v[0:1, :], vec_v[1:2, :]
    for r in (1, 2):
        rows = slice(r * 128, r * 128 + 128)
        hid_v[rows, :] = normed(lat_v[rows, :], mult, shift)
    for c in halo:
        c.wait()
    for r in (0, 3):
        rows = slice(r * 128, r * 128 + 128)
        hid_v[rows, :] = normed(lat_v[rows, :], mult, shift)
    for c in weights[:2]:
        c.wait()
    kv = dot(hid_v[...], wkv_v[...]).astype(BF16)
    keys = rotated(kv[:, 0:256], cos, sin, swap).astype(BF16)
    kt = dot_nt(identity(), keys).astype(BF16)
    ones = jnp.ones((512, 128), BF16)
    low_own = iota((256, 128), 1) < HEAD_DIM
    low = iota((128, 128), 1) < HEAD_DIM
    row, col = iota((128, 128), 0), iota((128, 128), 1)
    from_low = jnp.where(col >= row, 0.0, NEG_BIG)
    from_high = jnp.where(col <= row, 0.0, NEG_BIG)
    bias = (
        (from_low + jnp.where(place > 0, 0.0, NEG_BIG), from_high),
        (from_low, from_high + jnp.where(place < last, 0.0, NEG_BIG)),
    )
    for c in weights[2:]:
        c.wait()
    slabs = []
    for a in range(2):
        q = dot(hid_v[128:384, :], wq_v[a]).astype(BF16)
        plain, turned = [], []
        for h in range(2):
            part = q[:, h * 256 : h * 256 + 256]
            plain.append(part.astype(F32))
            turned.append(rotated(part, cos[128:384], sin[128:384], swap))
        for p in range(2):
            piece = slice(p * 128, p * 128 + 128)
            at = a * 512 + p * 256
            one, two = paired(plain[0][:, piece], plain[1][:, piece], low_own)
            q_ref[:, at : at + 128] = one
            q_ref[:, at + 128 : at + 256] = two
            slabs += paired(turned[0][:, piece], turned[1][:, piece], low_own)
    eighth = (iota((128, 128), 1) & 63) >> 3
    lse = [jnp.zeros((128, 128), F32) for _ in range(2)]
    for a in range(2):
        va = jnp.concatenate([kv[:, 256 + a * 128 : 384 + a * 128], ones], axis=1)
        for b in range(2):
            rows = slice(b * 128, b * 128 + 128)
            seen = slice(b * 128, b * 128 + 384)
            stacked = []
            for g in range(4):
                stacked += split_pair(slabs[a * 4 + g][rows], low)
            s = dot(jnp.concatenate(stacked, axis=0), kt[a * 128 : a * 128 + 128, seen])
            ps, ms = [], []
            for i in range(8):
                si = s[i * 128 : i * 128 + 128]
                s0, s1, s2 = si[:, 0:128] + bias[b][0], si[:, 128:256], si[:, 256:384] + bias[b][1]
                sink = sink_ref[(2 * a + i % 2) * 4 + i // 2] * LOG2E
                m = jnp.max(jnp.maximum(jnp.maximum(s0, s1), s2), axis=-1, keepdims=True)
                m = jnp.maximum(m * FACTOR, sink)
                p = [jnp.exp2(x * FACTOR - m).astype(BF16) for x in (s0, s1, s2)]
                ps.append(jnp.concatenate(p, axis=1))
                ms.append((jnp.broadcast_to(m, (128, 128)), sink))
            o = dot(jnp.concatenate(ps, axis=0), va[seen])
            for g in range(4):
                to = slice(a * 512 + g * 128, a * 512 + g * 128 + 128)
                x, y = o[g * 256 : g * 256 + 128], o[g * 256 + 128 : g * 256 + 256]
                (mx, sx), (my, sy) = ms[2 * g], ms[2 * g + 1]
                m = jnp.where(low, mx, my)
                l = jnp.where(low, x[:, 128:256], y[:, 128:256])
                l = l + jnp.exp2(jnp.where(low, sx, sy) - m)
                o_ref[rows, to] = jnp.where(low, x[:, 0:128], y[:, 0:128]) / l
                lse[b] = jnp.where(eighth == a * 4 + g, m + jnp.log2(l), lse[b])
    for b in range(2):
        lse_ref[b * 128 : b * 128 + 128, :] = lse[b]


def final_kernel(
    q_ref, kv_ref, o_ref, lse_ref, wo_ref, lat_ref, vec_ref, gain_ref, out_ref,
    wo_v, lat_v, vec_v, gain_v, mix_v, out_v, kt_v, va_v, even_v, odd_v, sems,
):
    copy = pltpu.make_async_copy
    pairs = [(lat_ref, lat_v), (vec_ref, vec_v), (gain_ref, gain_v)]
    for a in range(2):
        for g in range(4):
            for i in range(2):
                head = (2 * a + i) * 4 + g
                to = ((a * 4 + g) * 2 + i) * HEAD_DIM
                pairs.append((wo_ref.at[pl.ds(head * 64, 64)], wo_v.at[pl.ds(to, 64)]))
    ins = [copy(src, dst, sems.at[i]) for i, (src, dst) in enumerate(pairs)]
    for c in ins:
        c.start()
    low = iota((256, 128), 1) < HEAD_DIM
    eye = identity()
    keys = dot_nt(eye, kv_ref[:, 0:256]).astype(BF16)
    for a in range(2):
        kt_v[a] = keys[a * 128 : a * 128 + 128]
        va_v[a, :, 0:128] = kv_ref[:, 256 + a * 128 : 384 + a * 128]
        va_v[a, :, 128:256] = jnp.ones((1024, 128), BF16)

    def scores(i, s_ref):
        q = q_ref[:, pl.ds(pl.multiple_of(i * 128, 128), 128)]
        stacked = jnp.concatenate(split_pair(q, low), axis=0)
        s_ref[...] = dot(stacked, kt_v[i // 4])

    def attend(i, s_ref):
        s = s_ref[...]
        m = jnp.max(s, axis=-1, keepdims=True) * FACTOR
        o = dot(jnp.exp2(s * FACTOR - m).astype(BF16), va_v[i // 4])
        m = jnp.broadcast_to(m, (512, 128))
        mc = jnp.where(low, m[0:256], m[256:512])
        oc = jnp.where(low, o[0:256, 0:128], o[256:512, 0:128])
        lc = jnp.where(low, o[0:256, 128:256], o[256:512, 128:256])
        at = pl.ds(pl.multiple_of(i * 128, 128), 128)
        lse = pltpu.roll(lse_ref[...], (128 - 8 * i) & 127, 1)
        here = [jnp.broadcast_to(lse[:, c : c + 1], (256, 128)) for c in (0, 64)]
        ml = jnp.where(low, here[0], here[1])
        top = jnp.maximum(ml, mc)
        wl, wc = jnp.exp2(ml - top), jnp.exp2(mc - top)
        mix_v[:, at] = ((wl * o_ref[:, at] + wc * oc) / (wl + wc * lc)).astype(BF16)

    scores(0, even_v)

    def two(j, carry):
        i = 2 * j
        scores(i + 1, odd_v)
        attend(i, even_v)
        scores(i + 2, even_v)
        attend(i + 1, odd_v)
        return carry

    lax.fori_loop(0, 3, two, 0)
    for c in ins:
        c.wait()
    scores(7, odd_v)
    part = dot(mix_v[:, 0:768], wo_v[0:768])
    attend(6, even_v)
    attend(7, odd_v)
    scale = vec_v[2:3, :] * gain_v[...]
    outs = []
    for b in range(2):
        rows = slice(b * 128, b * 128 + 128)
        projected = part[rows] + dot(mix_v[rows, 768:1024], wo_v[768:1024])
        rs = lax.rsqrt(jnp.mean(projected * projected, axis=-1, keepdims=True) + EPSILON)
        out_v[rows, :] = (lat_v[rows, :].astype(F32) + projected * rs * scale).astype(BF16)
        there = pl.ds(b * 128, 128)
        outs.append(copy(out_v.at[there], out_ref.at[there], sems.at[len(ins) + b]))
        outs[b].start()
    for c in outs:
        c.wait()


KINDS = {"v": VM, "V": VM, "h": HB, "s": SM}
FIXED = {"V": VM, "h": HB}


def spec(kinds):
    return [pl.BlockSpec(memory_space=KINDS[k]) for k in kinds]


def call(kernel, name, ins, outs, scratch, copies, args, flops, limit):
    return pl.pallas_call(
        kernel,
        out_shape=[FIXED.get(k, jax.ShapeDtypeStruct)(s, d) for k, s, d in outs],
        in_specs=spec(ins),
        out_specs=spec([k for k, _, _ in outs]),
        scratch_shapes=[pltpu.VMEM(s, d) for s, d in scratch]
        + [pltpu.SemaphoreType.DMA((copies,))],
        compiler_params=pltpu.CompilerParams(vmem_limit_bytes=limit * 1024 * 1024),
        cost_estimate=pl.CostEstimate(flops=flops, bytes_accessed=0, transcendentals=0),
        name=name,
    )(
        *[
            pltpu.with_memory_space_constraint(x, FIXED[k]) if k in FIXED else x
            for k, x in zip(ins, args)
        ]
    )


def shards(
    latent, cond, ctx_rows, ctx_cond, mod_weight, norm_gain, out_gain,
    w_query, w_key, w_value, w_out, sink,
):
    sp_size = lax.axis_size("sp")
    count = sp_size * lax.axis_size("tp")
    both = ("sp", "tp")
    rows, width = latent.shape
    half = (WINDOW, width)
    wide = (rows, 1024)
    rest = (8, width)
    line = (1, width)
    square = (16, 128)
    small = w_key.shape

    parts, one, two = call(
        entry_kernel,
        "entry",
        "hhhh",
        [("h", (count, 8, 640), BF16), ("h", half, BF16), ("h", half, BF16)],
        [
            (square, BF16),
            (square, BF16),
            (mod_weight.shape, BF16),
            (latent.shape, BF16),
            ((count, 8, 640), BF16),
        ],
        7,
        (cond.reshape(square), ctx_cond.reshape(square), mod_weight, latent),
        10**6,
        8,
    )
    ng, wk_near, wv_near = call(
        prep_kernel,
        "prep",
        "hhhhh",
        [("V", (72, width), F32), ("V", small, BF16), ("V", small, BF16)],
        [(ctx_rows.shape, BF16), (line, F32)],
        4,
        (one, ctx_rows, norm_gain.reshape(line), w_key, w_value),
        2 * 10**9,
        4,
    )
    recv = lax.all_to_all(parts, both, 0, 0, tiled=True)
    swap_one = [(i, i ^ 1) for i in range(count)]
    swap_two = [(i, i + 1 if i % 2 else i - 1) for i in range(1, count - 1)]
    one = lax.ppermute(one, both, swap_one)
    two = lax.ppermute(two, both, swap_two)
    send, vecs = call(
        context_kernel,
        "context",
        "vVVV",
        [("h", (sp_size, 64, 512), BF16), ("h", rest, F32)],
        [((64, 512), BF16), (rest, F32)],
        17,
        (recv, ng, wk_near, wv_near),
        10**6,
        6,
    )
    kv_ctx = lax.all_to_all(send, "sp", 0, 0, tiled=True).reshape(sp_size * 64, 512)

    lanes = np.arange(256) % 32
    freq = 10000.0 ** (-(lanes % 16) / 16.0)
    by_row = (lanes < 16).astype(np.float32)
    angle = np.arange(GRID_W)[:, None] * freq
    colc = jnp.asarray(np.cos(angle) * (1.0 - by_row), F32)
    cols = jnp.asarray(np.sin(angle) * (1.0 - by_row), F32)
    grid_row = place_of() * (rows // GRID_W) - WINDOW // GRID_W + jnp.arange(8, dtype=jnp.int32)
    angle = grid_row.astype(F32)[:, None] * jnp.asarray(freq, F32)[None, :]
    tables = (jnp.cos(angle) * by_row, jnp.sin(angle) * by_row, colc, cols)

    query, o, lse = call(
        local_kernel,
        "local",
        "shhhhhhhvvvv",
        [("V", wide, BF16), ("V", wide, F32), ("V", (rows, 128), F32)],
        [
            (rest, F32),
            ((2 * rows, width), BF16),
            ((2, width, 512), BF16),
            ((width, 512), BF16),
            ((2 * rows, width), BF16),
        ],
        8,
        (sink, vecs, latent, one, two, w_query, w_key, w_value, *tables),
        10**10,
        26,
    )
    (updated,) = call(
        final_kernel,
        "final",
        "VVVVhhhh",
        [("h", latent.shape, BF16)],
        [
            (w_out.shape, BF16),
            (latent.shape, BF16),
            (rest, F32),
            (line, F32),
            (wide, BF16),
            (latent.shape, BF16),
            ((2, 128, 1024), BF16),
            ((2, 1024, 256), BF16),
            ((512, 1024), F32),
            ((512, 1024), F32),
        ],
        21,
        (query, kv_ctx, o, lse, w_out, latent, vecs, out_gain.reshape(line)),
        10**10,
        28,
    )
    return updated


def solution(mesh):
    placed = (
        P(("dp", "sp", "tp"), None),
        P("dp"),
        P(("dp", "sp"), None),
        P(),
        P(None, "sp", "tp"),
        P(),
        P(),
        P(),
        P(),
        P(),
        P(),
        P(),
    )
    return jax.shard_map(
        shards, mesh=mesh, in_specs=placed, out_specs=P(("dp", "sp", "tp"), None), check_vma=False
    )
```

```python
import jax
import numpy as np
import jax.numpy as jnp
from jax import lax
from jax.experimental import pallas as pl
from jax.experimental.pallas import tpu as pltpu
from jax.sharding import PartitionSpec as P

HEAD_DIM = 64
WINDOW = 128
GRID_W = 64
EPSILON = 1e-06
NEG_BIG = -1e30
LOG2E = 1.4426950408889634
FACTOR = HEAD_DIM**-0.5 * LOG2E
F32 = jnp.float32
BF16 = jnp.bfloat16
VM = pltpu.MemorySpace.VMEM
HB = pltpu.MemorySpace.HBM
SM = pltpu.MemorySpace.SMEM


def place_of():
    return lax.axis_index("sp") * lax.axis_size("tp") + lax.axis_index("tp")


def dot(a, b):
    return jnp.dot(a, b, preferred_element_type=F32)


def dot_nt(a, b):
    return lax.dot_general(a, b, (((1,), (1,)), ((), ())), preferred_element_type=F32)


def iota(shape, dim):
    return lax.broadcasted_iota(jnp.int32, shape, dim)


def swap_matrix():
    k, c = iota((256, 256), 0), iota((256, 256), 1)
    low = (c & 63) < 32
    neg = jnp.where(low & (k == c + 32), -1.0, 0.0)
    pos = jnp.where((~low) & (k == c - 32), 1.0, 0.0)
    return (neg + pos).astype(BF16)


def normed(x, mult, shift):
    x = x.astype(F32)
    rs = lax.rsqrt(jnp.mean(x * x, axis=-1, keepdims=True) + EPSILON)
    return (x * rs * mult + shift).astype(BF16)


def entry_kernel(
    cond_ref, cctx_ref, mod_ref, lat_ref,
    parts_ref, one_ref, two_ref,
    cond_v, cctx_v, mod_v, lat_v, block_v, sems,
):
    sp = lax.axis_index("sp")
    odd = place_of() & 1
    copy = pltpu.make_async_copy
    pairs = ((mod_ref, mod_v), (cond_ref, cond_v), (cctx_ref, cctx_v), (lat_ref, lat_v))
    ins = [copy(src, dst, sems.at[i]) for i, (src, dst) in enumerate(pairs)]
    for c in ins:
        c.start()
    ins[1].wait()
    ins[2].wait()
    here = iota((16, 128), 0) == sp
    rows = []
    for ref in (cond_v, cctx_v):
        x = jnp.sum(jnp.where(here, ref[...].astype(F32), 0.0), axis=0, keepdims=True)
        rows.append(x / (1.0 + jnp.exp(-x)))
    v = jnp.concatenate(rows + [jnp.zeros((6, 128), F32)], axis=0).astype(BF16)
    ins[0].wait()
    parts = [dot(v, mod_v[i]) for i in range(3)]
    five = (parts[0][0:1], parts[0][1:2], parts[1][0:1], parts[1][1:2], parts[2][0:1])
    rows = []
    for j in range(4):
        exact = jnp.concatenate([x[:, j * 128 : (j + 1) * 128] for x in five], axis=1)
        high = exact.astype(BF16).astype(F32)
        rows += [high, exact - high]
    block = jnp.concatenate(rows, axis=0).astype(BF16)
    for i in range(block_v.shape[0]):
        block_v[i] = block
    outs = [
        copy(block_v, parts_ref, sems.at[4]),
        copy(lat_v.at[pl.ds((1 - odd) * 128, 128)], one_ref, sems.at[5]),
        copy(lat_v.at[pl.ds(odd * 128, 128)], two_ref, sems.at[6]),
    ]
    outs[0].start()
    ins[3].wait()
    outs[1].start()
    outs[2].start()
    for c in outs:
        c.wait()


def prep_kernel(
    after_ref, ctx_ref, gain_ref, wk_ref, wv_ref, ng_ref, wk_out, wv_out, ctx_v, gain_v, sems
):
    copy = pltpu.make_async_copy
    pairs = ((ctx_ref, ctx_v), (gain_ref, gain_v), (wk_ref, wk_out), (wv_ref, wv_out))
    ins = [copy(src, dst, sems.at[i]) for i, (src, dst) in enumerate(pairs)]
    for c in ins:
        c.start()
    ins[0].wait()
    ins[1].wait()
    x = ctx_v[...].astype(F32)
    gain = gain_v[...]
    rs = lax.rsqrt(jnp.mean(x * x, axis=-1, keepdims=True) + EPSILON)
    ng_ref[0:64, :] = x * rs * gain
    ng_ref[64:72, :] = jnp.broadcast_to(gain, (8, 2048))
    for c in ins[2:]:
        c.wait()


def context_kernel(recv_ref, ng_ref, wk_ref, wv_ref, send_ref, vec_ref, kv_v, vec_v, sems):
    sums = []
    for t in range(4):
        acc = recv_ref[t].astype(F32)
        for s in range(1, 16):
            acc = acc + recv_ref[s * 4 + t].astype(F32)
        sums.append(acc)

    def vector(v):
        cuts = []
        for t in range(4):
            for j in range(4):
                both = sums[t][2 * j : 2 * j + 2, v * 128 : v * 128 + 128]
                cuts.append(both[0:1] + both[1:2])
        return jnp.concatenate(cuts, axis=1)

    hidden = (ng_ref[0:64, :] * (1.0 + vector(3)) + vector(1)).astype(BF16)
    kv_v[:, 0:256] = dot(hidden, wk_ref[...]).astype(BF16)
    kv_v[:, 256:512] = dot(hidden, wv_ref[...]).astype(BF16)
    copy = pltpu.make_async_copy
    outs = [copy(kv_v, send_ref.at[i], sems.at[i]) for i in range(16)]
    for c in outs:
        c.start()
    vec_v[...] = jnp.zeros((8, 2048), F32)
    vec_v[0:1, :] = ng_ref[64:65, :] * (1.0 + vector(2))
    vec_v[1:2, :] = vector(0)
    vec_v[2:3, :] = vector(4)
    outs.append(copy(vec_v, vec_ref, sems.at[16]))
    outs[16].start()
    for c in outs:
        c.wait()


def rotated(x, cos, sin, swap):
    return x.astype(F32) * cos + dot(x, swap) * sin


def paired(a, b, low):
    turned_a, turned_b = pltpu.roll(a, 64, 1), pltpu.roll(b, 64, 1)
    return jnp.where(low, a, turned_b).astype(BF16), jnp.where(low, turned_a, b).astype(BF16)


def split_pair(q, low):
    zero = jnp.zeros_like(q)
    return [jnp.where(low, q, zero), jnp.where(low, zero, q)]


def identity():
    return (iota((256, 256), 0) == iota((256, 256), 1)).astype(F32).astype(BF16)


def local_kernel(
    sink_ref, vec_ref, lat_ref, one_ref, two_ref, wq_ref, wk_ref, wv_ref,
    rowc_ref, rows_ref, colc_ref, cols_ref,
    q_ref, o_ref, lse_ref,
    vec_v, lat_v, wq_v, wkv_v, hid_v, sems,
):
    place = place_of()
    odd = place & 1
    last = lax.axis_size("sp") * lax.axis_size("tp") - 1
    copy = pltpu.make_async_copy
    own = [
        copy(vec_ref, vec_v, sems.at[0]),
        copy(lat_ref, lat_v.at[pl.ds(128, 256)], sems.at[1]),
    ]
    halo = [
        copy(one_ref, lat_v.at[pl.ds((1 - odd) * 384, 128)], sems.at[2]),
        copy(two_ref, lat_v.at[pl.ds(odd * 384, 128)], sems.at[3]),
    ]
    weights = [
        copy(wk_ref, wkv_v.at[:, pl.ds(0, 256)], sems.at[4]),
        copy(wv_ref, wkv_v.at[:, pl.ds(256, 256)], sems.at[5]),
        copy(wq_ref.at[:, pl.ds(0, 512)], wq_v.at[0], sems.at[6]),
        copy(wq_ref.at[:, pl.ds(512, 512)], wq_v.at[1], sems.at[7]),
    ]
    for c in own + halo:
        c.start()
    swap = swap_matrix()
    cos = jnp.concatenate([colc_ref[...] + rowc_ref[r : r + 1, :] for r in range(8)], axis=0)
    sin = jnp.concatenate([cols_ref[...] + rows_ref[r : r + 1, :] for r in range(8)], axis=0)
    for c in own:
        c.wait()
    for c in weights:
        c.start()
    mult, shift = vec_v[0:1, :], vec_v[1:2, :]
    for r in (1, 2):
        rows = slice(r * 128, r * 128 + 128)
        hid_v[rows, :] = normed(lat_v[rows, :], mult, shift)
    for c in halo:
        c.wait()
    for r in (0, 3):
        rows = slice(r * 128, r * 128 + 128)
        hid_v[rows, :] = normed(lat_v[rows, :], mult, shift)
    for c in weights[:2]:
        c.wait()
    kv = dot(hid_v[...], wkv_v[...]).astype(BF16)
    keys = rotated(kv[:, 0:256], cos, sin, swap).astype(BF16)
    kt = dot_nt(identity(), keys).astype(BF16)
    ones = jnp.ones((512, 128), BF16)
    low_own = iota((256, 128), 1) < HEAD_DIM
    low = iota((128, 128), 1) < HEAD_DIM
    row, col = iota((128, 128), 0), iota((128, 128), 1)
    from_low = jnp.where(col >= row, 0.0, NEG_BIG)
    from_high = jnp.where(col <= row, 0.0, NEG_BIG)
    bias = (
        (from_low + jnp.where(place > 0, 0.0, NEG_BIG), from_high),
        (from_low, from_high + jnp.where(place < last, 0.0, NEG_BIG)),
    )
    for c in weights[2:]:
        c.wait()
    slabs = []
    for a in range(2):
        q = dot(hid_v[128:384, :], wq_v[a]).astype(BF16)
        plain, turned = [], []
        for h in range(2):
            part = q[:, h * 256 : h * 256 + 256]
            plain.append(part.astype(F32))
            turned.append(rotated(part, cos[128:384], sin[128:384], swap))
        for p in range(2):
            piece = slice(p * 128, p * 128 + 128)
            at = a * 512 + p * 256
            one, two = paired(plain[0][:, piece], plain[1][:, piece], low_own)
            q_ref[:, at : at + 128] = one
            q_ref[:, at + 128 : at + 256] = two
            slabs += paired(turned[0][:, piece], turned[1][:, piece], low_own)
    eighth = (iota((128, 128), 1) & 63) >> 3
    lse = [jnp.zeros((128, 128), F32) for _ in range(2)]
    for a in range(2):
        va = jnp.concatenate([kv[:, 256 + a * 128 : 384 + a * 128], ones], axis=1)
        for b in range(2):
            rows = slice(b * 128, b * 128 + 128)
            seen = slice(b * 128, b * 128 + 384)
            stacked = []
            for g in range(4):
                stacked += split_pair(slabs[a * 4 + g][rows], low)
            s = dot(jnp.concatenate(stacked, axis=0), kt[a * 128 : a * 128 + 128, seen])
            ps, ms = [], []
            for i in range(8):
                si = s[i * 128 : i * 128 + 128]
                s0, s1, s2 = si[:, 0:128] + bias[b][0], si[:, 128:256], si[:, 256:384] + bias[b][1]
                sink = sink_ref[(2 * a + i % 2) * 4 + i // 2] * LOG2E
                m = jnp.max(jnp.maximum(jnp.maximum(s0, s1), s2), axis=-1, keepdims=True)
                m = jnp.maximum(m * FACTOR, sink)
                p = [jnp.exp2(x * FACTOR - m).astype(BF16) for x in (s0, s1, s2)]
                ps.append(jnp.concatenate(p, axis=1))
                ms.append((jnp.broadcast_to(m, (128, 128)), sink))
            o = dot(jnp.concatenate(ps, axis=0), va[seen])
            for g in range(4):
                to = slice(a * 512 + g * 128, a * 512 + g * 128 + 128)
                x, y = o[g * 256 : g * 256 + 128], o[g * 256 + 128 : g * 256 + 256]
                (mx, sx), (my, sy) = ms[2 * g], ms[2 * g + 1]
                m = jnp.where(low, mx, my)
                l = jnp.where(low, x[:, 128:256], y[:, 128:256])
                l = l + jnp.exp2(jnp.where(low, sx, sy) - m)
                o_ref[rows, to] = jnp.where(low, x[:, 0:128], y[:, 0:128]) / l
                lse[b] = jnp.where(eighth == a * 4 + g, m + jnp.log2(l), lse[b])
    for b in range(2):
        lse_ref[b * 128 : b * 128 + 128, :] = lse[b]


def final_kernel(
    q_ref, kv_ref, o_ref, lse_ref, wo_ref, lat_ref, vec_ref, gain_ref, out_ref,
    wo_v, lat_v, vec_v, gain_v, mix_v, out_v, kt_v, va_v, even_v, odd_v, sems,
):
    copy = pltpu.make_async_copy
    pairs = [(lat_ref, lat_v), (vec_ref, vec_v), (gain_ref, gain_v)]
    for a in range(2):
        for g in range(4):
            for i in range(2):
                head = (2 * a + i) * 4 + g
                to = ((a * 4 + g) * 2 + i) * HEAD_DIM
                pairs.append((wo_ref.at[pl.ds(head * 64, 64)], wo_v.at[pl.ds(to, 64)]))
    ins = [copy(src, dst, sems.at[i]) for i, (src, dst) in enumerate(pairs)]
    for c in ins:
        c.start()
    low = iota((256, 128), 1) < HEAD_DIM
    eye = identity()
    keys = dot_nt(eye, kv_ref[:, 0:256]).astype(BF16)
    for a in range(2):
        kt_v[a] = keys[a * 128 : a * 128 + 128]
        va_v[a, :, 0:128] = kv_ref[:, 256 + a * 128 : 384 + a * 128]
        va_v[a, :, 128:256] = jnp.ones((1024, 128), BF16)

    def scores(i, s_ref):
        q = q_ref[:, pl.ds(pl.multiple_of(i * 128, 128), 128)]
        stacked = jnp.concatenate(split_pair(q, low), axis=0)
        s_ref[...] = dot(stacked, kt_v[i // 4])

    def attend(i, s_ref):
        s = s_ref[...]
        m = jnp.max(s, axis=-1, keepdims=True) * FACTOR
        o = dot(jnp.exp2(s * FACTOR - m).astype(BF16), va_v[i // 4])
        m = jnp.broadcast_to(m, (512, 128))
        mc = jnp.where(low, m[0:256], m[256:512])
        oc = jnp.where(low, o[0:256, 0:128], o[256:512, 0:128])
        lc = jnp.where(low, o[0:256, 128:256], o[256:512, 128:256])
        at = pl.ds(pl.multiple_of(i * 128, 128), 128)
        lse = pltpu.roll(lse_ref[...], (128 - 8 * i) & 127, 1)
        here = [jnp.broadcast_to(lse[:, c : c + 1], (256, 128)) for c in (0, 64)]
        ml = jnp.where(low, here[0], here[1])
        top = jnp.maximum(ml, mc)
        wl, wc = jnp.exp2(ml - top), jnp.exp2(mc - top)
        mix_v[:, at] = ((wl * o_ref[:, at] + wc * oc) / (wl + wc * lc)).astype(BF16)

    scores(0, even_v)

    def two(j, carry):
        i = 2 * j
        scores(i + 1, odd_v)
        attend(i, even_v)
        scores(i + 2, even_v)
        attend(i + 1, odd_v)
        return carry

    lax.fori_loop(0, 3, two, 0)
    for c in ins:
        c.wait()
    scores(7, odd_v)
    part = dot(mix_v[:, 0:768], wo_v[0:768])
    attend(6, even_v)
    attend(7, odd_v)
    scale = vec_v[2:3, :] * gain_v[...]
    outs = []
    for b in range(2):
        rows = slice(b * 128, b * 128 + 128)
        projected = part[rows] + dot(mix_v[rows, 768:1024], wo_v[768:1024])
        rs = lax.rsqrt(jnp.mean(projected * projected, axis=-1, keepdims=True) + EPSILON)
        out_v[rows, :] = (lat_v[rows, :].astype(F32) + projected * rs * scale).astype(BF16)
        there = pl.ds(b * 128, 128)
        outs.append(copy(out_v.at[there], out_ref.at[there], sems.at[len(ins) + b]))
        outs[b].start()
    for c in outs:
        c.wait()


KINDS = {"v": VM, "V": VM, "h": HB, "s": SM}
FIXED = {"V": VM, "h": HB}


def spec(kinds):
    return [pl.BlockSpec(memory_space=KINDS[k]) for k in kinds]


def call(kernel, ins, outs, scratch, copies, args, flops, limit):
    return pl.pallas_call(
        kernel,
        out_shape=[FIXED.get(k, jax.ShapeDtypeStruct)(s, d) for k, s, d in outs],
        in_specs=spec(ins),
        out_specs=spec([k for k, _, _ in outs]),
        scratch_shapes=[pltpu.VMEM(s, d) for s, d in scratch]
        + [pltpu.SemaphoreType.DMA((copies,))],
        compiler_params=pltpu.CompilerParams(vmem_limit_bytes=limit * 1024 * 1024),
        cost_estimate=pl.CostEstimate(flops=flops, bytes_accessed=0, transcendentals=0),
    )(
        *[
            pltpu.with_memory_space_constraint(x, FIXED[k]) if k in FIXED else x
            for k, x in zip(ins, args)
        ]
    )


def shards(
    latent, cond, ctx_rows, ctx_cond, mod_weight, norm_gain, out_gain,
    w_query, w_key, w_value, w_out, sink,
):
    sp_size = lax.axis_size("sp")
    count = sp_size * lax.axis_size("tp")
    both = ("sp", "tp")
    rows, width = latent.shape
    half = (WINDOW, width)
    wide = (rows, 1024)
    rest = (8, width)
    line = (1, width)
    square = (16, 128)
    small = w_key.shape

    parts, one, two = call(
        entry_kernel,
        "hhhh",
        [("h", (count, 8, 640), BF16), ("h", half, BF16), ("h", half, BF16)],
        [
            (square, BF16),
            (square, BF16),
            (mod_weight.shape, BF16),
            (latent.shape, BF16),
            ((count, 8, 640), BF16),
        ],
        7,
        (cond.reshape(square), ctx_cond.reshape(square), mod_weight, latent),
        10**6,
        8,
    )
    ng, wk_near, wv_near = call(
        prep_kernel,
        "hhhhh",
        [("V", (72, width), F32), ("V", small, BF16), ("V", small, BF16)],
        [(ctx_rows.shape, BF16), (line, F32)],
        4,
        (one, ctx_rows, norm_gain.reshape(line), w_key, w_value),
        2 * 10**9,
        4,
    )
    recv = lax.all_to_all(parts, both, 0, 0, tiled=True)
    swap_one = [(i, i ^ 1) for i in range(count)]
    swap_two = [(i, i + 1 if i % 2 else i - 1) for i in range(1, count - 1)]
    one = lax.ppermute(one, both, swap_one)
    two = lax.ppermute(two, both, swap_two)
    send, vecs = call(
        context_kernel,
        "vVVV",
        [("h", (sp_size, 64, 512), BF16), ("h", rest, F32)],
        [((64, 512), BF16), (rest, F32)],
        17,
        (recv, ng, wk_near, wv_near),
        10**6,
        6,
    )
    kv_ctx = lax.all_to_all(send, "sp", 0, 0, tiled=True).reshape(sp_size * 64, 512)

    lanes = np.arange(256) % 32
    freq = 10000.0 ** (-(lanes % 16) / 16.0)
    by_row = (lanes < 16).astype(np.float32)
    angle = np.arange(GRID_W)[:, None] * freq
    colc = jnp.asarray(np.cos(angle) * (1.0 - by_row), F32)
    cols = jnp.asarray(np.sin(angle) * (1.0 - by_row), F32)
    grid_row = place_of() * (rows // GRID_W) - WINDOW // GRID_W + jnp.arange(8, dtype=jnp.int32)
    angle = grid_row.astype(F32)[:, None] * jnp.asarray(freq, F32)[None, :]
    tables = (jnp.cos(angle) * by_row, jnp.sin(angle) * by_row, colc, cols)

    query, o, lse = call(
        local_kernel,
        "shhhhhhhvvvv",
        [("V", wide, BF16), ("V", wide, F32), ("V", (rows, 128), F32)],
        [
            (rest, F32),
            ((2 * rows, width), BF16),
            ((2, width, 512), BF16),
            ((width, 512), BF16),
            ((2 * rows, width), BF16),
        ],
        8,
        (sink, vecs, latent, one, two, w_query, w_key, w_value, *tables),
        10**10,
        26,
    )
    (updated,) = call(
        final_kernel,
        "VVVVhhhh",
        [("h", latent.shape, BF16)],
        [
            (w_out.shape, BF16),
            (latent.shape, BF16),
            (rest, F32),
            (line, F32),
            (wide, BF16),
            (latent.shape, BF16),
            ((2, 128, 1024), BF16),
            ((2, 1024, 256), BF16),
            ((512, 1024), F32),
            ((512, 1024), F32),
        ],
        21,
        (query, kv_ctx, o, lse, w_out, latent, vecs, out_gain.reshape(line)),
        10**10,
        28,
    )
    return updated


def solution(mesh):
    placed = (
        P(("dp", "sp", "tp"), None),
        P("dp"),
        P(("dp", "sp"), None),
        P(),
        P(None, "sp", "tp"),
        P(),
        P(),
        P(),
        P(),
        P(),
        P(),
        P(),
    )

    return jax.shard_map(
        shards, mesh=mesh, in_specs=placed, out_specs=P(("dp", "sp", "tp"), None), check_vma=False
    )
```
